512 devices in a mesh: sp: 32 (over z, core), tp: 16 (over y, x).
Axes of the slice: x: 4, y: 4, z: 16, core: 2. Of those that a mesh axis runs over, the one named last changes fastest.
Arguments:
- queries: bfloat16 [8192, 2048], P('sp', 'tp'), may hold values from -6 to 6
- keys: bfloat16 [8192, 1024], P('sp', 'tp'), may hold values from -6 to 6
- values: bfloat16 [8192, 1024], P('sp', 'tp'), may hold values from -6 to 6
- sink_logit: float32 [32], P('tp'), may hold values from -1 to 6
- out_weight: bfloat16 [2048, 2048], P(None, 'tp'), may hold values from -0.125 to 0.125
- residual: bfloat16 [8192, 2048], P(('sp', 'tp')), may hold values from -1.796875 to 1.796875
- norm_gain: float32 [2048], replicated, may hold values from 0.1 to 1.9
- routes: int32 [8192, 2], P(('sp', 'tp')), may hold values from 0 to 31, all different within a row; in each aligned block of 16 rows (0 to 15, 16 to 31, ...) at most 2 rows name the same one
- route_weights: float32 [8192, 2], P(('sp', 'tp')), may hold values from 0.2 to 1
- gate_weight: bfloat16 [32, 2048, 5120], P('sp', None, 'tp'), may hold values from -0.125 to 0.125
- up_weight: bfloat16 [32, 2048, 5120], P('sp', None, 'tp'), may hold values from -0.125 to 0.125
- down_weight: bfloat16 [32, 5120, 2048], P('sp', 'tp'), may hold values from -0.078125 to 0.078125
Outputs:
- mixed: bfloat16 [8192, 2048], P(('sp', 'tp'))
The draws below stay inside these ranges and needn't reach their ends.
Inputs may be any that keep to these rules, and one draw needn't show every extreme that they name: `routes`: each row names two different experts. Among the rows of one device no expert is named more than 2 times, and in every draw some expert is named exactly 2 times by the rows of some device.
All inputs are finite; a program needn't handle non-finite values.
Results may differ from the reference program's by a relative error of at most 0.018.
Values may be sent and summed in bfloat16 or wider, within the bound.
No kernel may reach another device: no remote copies, remote signals or barrier semaphores. Data moves between devices by JAX's collectives and lax.ppermute only.
A program may use at most 64 MiB of HBM per device.

```python
import math
import jax
import jax.numpy as jnp
import numpy as np
from jax import lax

D = 2048
FF = 5120
HEADS = 32
KV_HEADS = 16
HEAD = 64
WINDOW = 128
TOK_DEV = 16
TOKENS = 8192
EXPERTS = 32
CAP = 2
N_SP = 32
N_TP = 16


def draw_queries(key, part):
    own_key = jax.random.fold_in(key, 17)
    drawn = jnp.clip(jax.random.normal(own_key, (TOKENS, HEADS * HEAD), jnp.float32), -6.0, 6.0)
    return drawn.astype(jnp.bfloat16)


def draw_keys(key, part):
    own_key = jax.random.fold_in(key, 29)
    drawn = jnp.clip(jax.random.normal(own_key, (TOKENS, KV_HEADS * HEAD), jnp.float32), -6.0, 6.0)
    return drawn.astype(jnp.bfloat16)


def shard_levels(stream_key, dims, cuts, smallest, top_value):
    level = 1.0
    for position, shards_of in cuts:
        steps = jax.random.uniform(jax.random.fold_in(jax.random.fold_in(stream_key, 6), position), (shards_of,), jnp.float32, smallest / len(cuts), top_value / len(cuts))
        level = level * jnp.repeat(jnp.exp(steps), dims[position] // shards_of).reshape((-1,) + (1,) * (len(dims) - 1 - position))
    return level


def deal_out(rng, own, number, rows, amount, top, limit, lean):
    order = jax.random.permutation(rng, amount)
    packed, ordinary = portions_of(amount, rows * top, limit, lean, True), portions_of(amount, rows * top, limit, lean, False)
    places = jnp.arange(amount)

    def named(tallies, rotation):
        used = int((tallies > 0).sum())
        fixed = max(1, used // 4)
        moved = fixed + (places - fixed + rotation * (used - fixed)) % max(1, amount - fixed)
        return jnp.zeros((amount,), jnp.int32).at[order[jnp.where(places < fixed, places, moved)]].set(jnp.asarray(tallies, jnp.int32))

    tallies = jnp.where(number % 4 == 0, named(packed, number // 4), named(ordinary, number - number // 4 - 1))
    mixed = jax.random.permutation(jax.random.fold_in(own, 3), amount)
    donor, taker = mixed[0:amount // 2 * 2:2], mixed[1:amount // 2 * 2:2]
    slack = jnp.minimum(tallies[donor] - 1, limit - tallies[taker]) // 2
    slack = jnp.where((donor == order[0]) | (taker == order[0]) | (tallies[taker] == 0), 0, jnp.maximum(slack, 0))
    moved = jax.random.randint(jax.random.fold_in(own, 4), (amount // 2,), 0, 1 << 20) % (slack + 1)
    tallies = tallies.at[donor].add(-moved).at[taker].add(moved)
    members = jnp.searchsorted(jnp.cumsum(tallies), jnp.arange(rows * top), side="right").astype(jnp.int32)
    listing = members.reshape(top, rows).T
    listing = listing[jax.random.permutation(jax.random.fold_in(own, 1), rows)]
    rotation = jax.random.randint(jax.random.fold_in(own, 2), (rows, 1), 0, top)
    return jnp.take_along_axis(listing, (jnp.arange(top)[None, :] + rotation) % top, axis=1)


def portions_of(amount, total, most, lean, full):
    loads = [(1 << 20) // math.isqrt(rank ** lean) + 1 for rank in range(1, amount + 1)]
    largest = most if full else min(most, max(-(-total // amount), total * loads[0] // sum(loads)))
    least = 1 if total - largest >= amount - 1 else 0
    counts, surplus = [largest] + [least] * (amount - 1), total - largest - least * (amount - 1)
    while surplus > 0:
        movable = [i for i in range(1, amount) if counts[i] < largest] or [i for i in range(1, amount) if counts[i] < most]
        pool, remaining = sum([loads[i] for i in movable]), surplus
        for i in movable:
            more = min(most - counts[i], max(1, remaining * loads[i] // pool), surplus)
            counts[i] = counts[i] + more
            surplus = surplus - more
    return np.array(counts)


def scatter_about(stream_key, extent, width, bound, shards=(), held_as=jnp.bfloat16):
    array = width * jax.random.normal(stream_key, extent, jnp.float32)
    if shards:
        array = array * shard_levels(stream_key, extent, shards, -0.22, 0.18)
    return jnp.clip(array, -bound, bound).astype(held_as)


def setup_inputs(seed: int = 0) -> dict:
    key_of = jax.random.split(jax.random.key(seed), 13)
    queries = draw_queries(jax.random.fold_in(key_of[12], 71), 0)
    keys = draw_keys(jax.random.fold_in(key_of[12], 71), 0)
    values = scatter_about(key_of[2], (TOKENS, KV_HEADS * HEAD), 1.0, 6.0, ((0, 32), (1, 16)))
    sink_logit = jnp.clip(-1.0 + 7.0 * jax.random.uniform(key_of[3], (HEADS,), jnp.float32) ** shard_levels(key_of[3], (HEADS,), ((0, 16),), -0.2, 0.2), -1.0, 6.0)
    out_weight = scatter_about(key_of[4], (HEADS * HEAD, D), (HEADS * HEAD) ** -0.5, 0.125, ((1, 16),))
    residual = scatter_about(key_of[5], (TOKENS, D), 0.3, 1.796875, ((0, 512),))
    norm_gain = jnp.clip(1.0 + 0.18 * jax.random.normal(key_of[6], (D,), jnp.float32), 0.1, 1.9)
    routes_keys = jax.random.split(jax.random.fold_in(key_of[7], 1), TOKENS // TOK_DEV)
    routes_turns = jax.random.permutation(jax.random.fold_in(key_of[7], 3), TOKENS // TOK_DEV)
    routes = jax.vmap(lambda own, number: deal_out(jax.random.fold_in(key_of[7], 2), own, number, TOK_DEV, EXPERTS, 2, CAP, 1))(routes_keys, routes_turns).reshape((TOKENS, 2))
    route_weights = jnp.clip(0.2 + 0.8 * jax.random.uniform(key_of[8], (TOKENS, 2), jnp.float32) ** shard_levels(key_of[8], (TOKENS, 2), ((0, 512),), -0.2, 0.2), 0.2, 1.0)
    gate_weight = scatter_about(key_of[9], (EXPERTS, D, FF), D ** -0.5, 0.125, ((0, 32), (2, 16)))
    up_weight = scatter_about(key_of[10], (EXPERTS, D, FF), D ** -0.5, 0.125, ((0, 32), (2, 16)))
    down_weight = scatter_about(key_of[11], (EXPERTS, FF, D), FF ** -0.5, 0.078125, ((0, 32), (1, 16)))
    return {"queries": queries, "keys": keys, "values": values, "sink_logit": sink_logit, "out_weight": out_weight, "residual": residual, "norm_gain": norm_gain, "routes": routes, "route_weights": route_weights, "gate_weight": gate_weight, "up_weight": up_weight, "down_weight": down_weight}


EPS = 1e-06
NEGATIVE = -1e+30

def make_band(tensor):
    length = tensor.shape[0]
    blocks = length // WINDOW
    padded = jnp.pad(tensor, ((WINDOW, WINDOW), (0, 0)))
    pieces = [padded[offset * WINDOW:offset * WINDOW + length].reshape(blocks, WINDOW, -1) for offset in range(3)]
    return jnp.concatenate(pieces, axis=1)

def attend(queries, keys, values, sink_logit):
    tokens = queries.shape[0]
    blocks = tokens // WINDOW
    repeat = HEADS // KV_HEADS
    scale = HEAD ** (-0.5)
    near = jnp.abs(jnp.arange(WINDOW)[:, None] + WINDOW - jnp.arange(3 * WINDOW)[None, :]) <= WINDOW
    key_pos = (jnp.arange(blocks)[:, None] - 1) * WINDOW + jnp.arange(3 * WINDOW)[None, :]
    inside = (key_pos >= 0) & (key_pos < tokens)
    valid = near[None, None, :, :] & inside[:, None, None, :]
    query_groups = queries.reshape(tokens, KV_HEADS, repeat, HEAD).transpose(1, 0, 2, 3)
    key_groups = keys.reshape(tokens, KV_HEADS, HEAD).transpose(1, 0, 2)
    value_groups = values.reshape(tokens, KV_HEADS, HEAD).transpose(1, 0, 2)
    sink_groups = sink_logit.reshape(KV_HEADS, repeat)

    def one_group(inputs):
        query_rows, key_rows, value_rows, sinks = inputs
        query_blocks = query_rows.reshape(blocks, WINDOW, repeat, HEAD).astype(jnp.float32)
        key_band = make_band(key_rows).astype(jnp.float32)
        value_band = make_band(value_rows).astype(jnp.float32)
        scores = jnp.einsum('nqrd,nkd->nrqk', query_blocks, key_band) * scale
        sink = sinks.astype(jnp.float32)[None, :, None, None]
        masked = jnp.where(valid, scores, NEGATIVE)
        top = jnp.maximum(lax.optimization_barrier(jnp.max(masked, axis=-1, keepdims=True)), sink)
        probs = jnp.exp(masked - top)
        denom = lax.optimization_barrier(jnp.sum(probs, axis=-1, keepdims=True)) + jnp.exp(sink - top)
        weights = (probs / denom).astype(jnp.bfloat16)
        output = jnp.einsum('nrqk,nkd->nqrd', weights.astype(jnp.float32), value_band)
        return output.astype(jnp.bfloat16).reshape(tokens, repeat * HEAD)
    outputs = lax.map(one_group, (query_groups, key_groups, value_groups, sink_groups))
    return outputs.transpose(1, 0, 2).reshape(tokens, HEADS * HEAD)

def one_expert(inputs):
    rows, gate_matrix, up_matrix, down_matrix = inputs
    gate = jnp.dot(rows, gate_matrix, preferred_element_type=jnp.float32)
    upward = jnp.dot(rows, up_matrix, preferred_element_type=jnp.float32)
    hidden = (jax.nn.silu(gate) * upward).astype(jnp.bfloat16)
    block_width = FF // N_TP
    shares = jnp.einsum('rjf,jfd->jrd', hidden.reshape(-1, N_TP, block_width).astype(jnp.float32), down_matrix.reshape(N_TP, block_width, D).astype(jnp.float32))
    return lax.optimization_barrier(jnp.sum(shares.astype(jnp.bfloat16).astype(jnp.float32), axis=0)).astype(jnp.bfloat16)

def reference(queries, keys, values, sink_logit, out_weight, residual, norm_gain, routes, route_weights, gate_weight, up_weight, down_weight):
    attention = attend(queries, keys, values, sink_logit)
    projected = jnp.dot(attention, out_weight, preferred_element_type=jnp.float32).astype(jnp.bfloat16)
    hidden_state = residual.astype(jnp.float32) + projected.astype(jnp.float32)
    inverse = lax.rsqrt(lax.optimization_barrier(jnp.mean(hidden_state * hidden_state, axis=-1, keepdims=True)) + EPS)
    normed = (hidden_state * inverse * norm_gain).astype(jnp.bfloat16)
    devices = N_SP * N_TP
    expert_ids = routes.reshape(devices, 2 * TOK_DEV).astype(jnp.int32)
    onehot = (expert_ids[..., None] == jnp.arange(EXPERTS, dtype=jnp.int32)).astype(jnp.int32)
    earlier = jnp.cumsum(onehot, axis=1) - onehot
    rank = lax.optimization_barrier(jnp.sum(earlier * onehot, axis=-1))
    slots = (jnp.arange(devices, dtype=jnp.int32)[:, None] * CAP + rank).reshape(-1).astype(jnp.int32)
    flat_ids = expert_ids.reshape(-1)
    pair_rows = jnp.repeat(normed, 2, axis=0)
    buffer = jnp.zeros((EXPERTS, devices * CAP, D), jnp.bfloat16).at[flat_ids, slots].set(pair_rows)
    expert_out = lax.map(one_expert, (buffer, gate_weight, up_weight, down_weight))
    picked = expert_out[flat_ids, slots].reshape(TOKENS, 2, D).astype(jnp.float32)
    mixture = lax.optimization_barrier(jnp.sum(route_weights[..., None] * picked, axis=1))
    return (hidden_state + mixture).astype(jnp.bfloat16)
```

```python
import jax
import jax.numpy as jnp
from jax import lax
from jax.sharding import PartitionSpec as P

HEADS = 32
KV_HEADS = 16
HEAD = 64
WINDOW = 128

EPS = 1e-06
NEGATIVE = -1e30


def halo(block, width):
    count = lax.axis_size("sp")
    forward = [(i, i + 1) for i in range(count - 1)]
    backward = [(target, source) for source, target in forward]
    low = lax.ppermute(block[-width:], "sp", forward)
    high = lax.ppermute(block[:width], "sp", backward)
    return jnp.concatenate([low, block, high], axis=0)


def make_band(extended, length):
    blocks = length // WINDOW
    pieces = [
        lax.slice_in_dim(extended, offset * WINDOW, offset * WINDOW + length, axis=0).reshape(
            blocks, WINDOW, -1
        )
        for offset in range(3)
    ]
    return jnp.concatenate(pieces, axis=1)


def attend_local(queries, keys, values, sink_logit):
    length = queries.shape[0]
    groups = keys.shape[1] // HEAD
    repeat = HEADS // KV_HEADS
    blocks = length // WINDOW
    joined = jnp.concatenate([keys, values], axis=1)
    extended = halo(joined, WINDOW)
    banded = make_band(extended, length)
    key_band = banded[..., : groups * HEAD].reshape(blocks, 3 * WINDOW, groups, HEAD)
    value_band = banded[..., groups * HEAD :].reshape(blocks, 3 * WINDOW, groups, HEAD)
    query_blocks = queries.reshape(blocks, WINDOW, groups, repeat, HEAD)
    scores = jnp.einsum(
        "nqgrd,nkgd->ngrqk", query_blocks, key_band, preferred_element_type=jnp.float32
    ) * HEAD ** (-0.5)
    near = jnp.abs(jnp.arange(WINDOW)[:, None] + WINDOW - jnp.arange(3 * WINDOW)[None, :]) <= WINDOW
    first_token = lax.axis_index("sp") * length
    key_pos = (
        first_token + (jnp.arange(blocks)[:, None] - 1) * WINDOW + jnp.arange(3 * WINDOW)[None, :]
    )
    inside = (key_pos >= 0) & (key_pos < length * lax.axis_size("sp"))
    valid = near[None, None, None, :, :] & inside[:, None, None, None, :]
    sinks = sink_logit.reshape(1, groups, repeat, 1, 1)
    masked = jnp.where(valid, scores, NEGATIVE)
    top = jnp.maximum(jnp.max(masked, axis=-1, keepdims=True), sinks)
    probs = jnp.exp(masked - top)
    denom = jnp.sum(probs, axis=-1, keepdims=True) + jnp.exp(sinks - top)
    weights = (probs / denom).astype(jnp.bfloat16)
    output = jnp.einsum(
        "ngrqk,nkgd->nqgrd", weights, value_band, preferred_element_type=jnp.float32
    )
    return output.astype(jnp.bfloat16).reshape(length, groups * repeat * HEAD)


def exchange(value, axis, groups=None):
    return lax.all_to_all(
        value, axis, split_axis=0, concat_axis=0, tiled=True, axis_index_groups=groups
    )


def local(
    queries,
    keys,
    values,
    sink_logit,
    out_weight,
    residual,
    norm_gain,
    routes,
    route_weights,
    gate_weight,
    up_weight,
    down_weight,
):
    n_sp, n_tp = lax.axis_size("sp"), lax.axis_size("tp")
    planes = n_sp // 2
    pairs = n_tp // 2
    tok_rows, width = residual.shape
    cols = width // n_tp
    length = queries.shape[0]
    parity = lax.axis_index("tp") % 2
    same_core = [[plane * 2 + core for plane in range(planes)] for core in range(2)]
    same_parity = [[pair * 2 + side for pair in range(pairs)] for side in range(2)]

    to_server = []
    for plane in range(planes):
        for core in range(2):
            for member in range(n_tp):
                source = (plane * 2 + core) * n_tp + member
                if member % 2 == core:
                    to_server.append((source, source))
                else:
                    to_server.append((source, (plane * 2 + 1 - core) * n_tp + (member ^ 1)))
    swap_core = [(s, s ^ 1) for s in range(n_sp)]
    swap_pair = [(t, t ^ 1) for t in range(n_tp)]
    gate_up = jnp.concatenate(
        [
            gate_weight[0, :, :256],
            up_weight[0, :, :256],
            gate_weight[0, :, 256:],
            up_weight[0, :, 256:],
        ],
        axis=1,
    )
    out_other = lax.ppermute(out_weight, "tp", swap_pair)
    down_one = lax.ppermute(down_weight[0], ("sp", "tp"), to_server)
    gate_up_one = lax.ppermute(gate_up, ("sp", "tp"), to_server)
    down_two = lax.ppermute(down_one, "sp", swap_core)
    gate_up_two = lax.ppermute(gate_up_one, "sp", swap_core)

    expert_ids = routes.reshape(-1)
    onehot = (expert_ids[:, None] == jnp.arange(n_sp, dtype=jnp.int32)[None, :]).astype(jnp.int32)
    earlier = jnp.cumsum(onehot, axis=0) - onehot
    rank = jnp.sum(earlier * onehot, axis=1)
    slots = (expert_ids * 2 + rank).reshape(tok_rows, 2)

    attention = attend_local(queries, keys, values, sink_logit)

    residual_pieces = residual.reshape(tok_rows, pairs, 2, cols).transpose(1, 2, 0, 3)
    residual_pieces = jnp.repeat(residual_pieces.reshape(pairs, 2 * tok_rows, cols), 2, axis=0)
    slot_rows = jnp.pad(slots.astype(jnp.bfloat16), ((0, 0), (0, cols - 2)))
    message = jnp.concatenate(
        [
            jnp.broadcast_to(attention, (n_tp, *attention.shape)),
            residual_pieces,
            jnp.broadcast_to(slot_rows, (n_tp, *slot_rows.shape)),
        ],
        axis=1,
    )
    arrived = exchange(message, "tp")
    attended = arrived[:, :length].transpose(1, 0, 2).reshape(length, width)
    residual_cols = (
        arrived[:, length : length + 2 * tok_rows]
        .reshape(n_tp, 2, tok_rows, cols)
        .transpose(0, 2, 1, 3)
        .reshape(length, 2 * cols)
    )
    slot_all = arrived[:, length + 2 * tok_rows :, :2].reshape(length, 2).astype(jnp.int32)

    own = jnp.dot(attended, out_weight, preferred_element_type=jnp.float32).astype(jnp.bfloat16)
    other = jnp.dot(attended, out_other, preferred_element_type=jnp.float32).astype(jnp.bfloat16)
    projected = jnp.concatenate(
        [jnp.where(parity == 0, own, other), jnp.where(parity == 0, other, own)], axis=1
    )
    hidden_cols = (residual_cols.astype(jnp.float32) + projected.astype(jnp.float32)).astype(
        jnp.bfloat16
    )
    wanted = (2 * jnp.arange(planes)[:, None] + parity) * 2 + jnp.arange(2)[None, :]
    named = jnp.any(slot_all[None, None] == wanted[:, :, None, None], axis=-1)
    mine = (jnp.arange(length) // tok_rows)[None, :] == jnp.arange(n_tp)[:, None]
    placing = (named[:, None] & mine[None, :, None]).astype(jnp.bfloat16)
    sending = jnp.dot(
        placing.reshape(planes * n_tp * 2, length), hidden_cols, preferred_element_type=jnp.float32
    ).astype(jnp.bfloat16)

    dispatched = exchange(sending.reshape(planes, n_tp * 2, 2 * cols), "sp", same_core)
    rows = planes * n_tp * 2
    block = dispatched.reshape(planes, n_tp, 2, 2 * cols).transpose(1, 2, 0, 3)
    block = block.reshape(rows, 2 * cols)
    gathered = exchange(jnp.broadcast_to(block, (pairs, *block.shape)), "tp", same_parity)
    flat = gathered.transpose(1, 0, 2).reshape(rows, width).astype(jnp.float32)
    inverse = lax.rsqrt(jnp.mean(flat * flat, axis=-1, keepdims=True) + EPS)
    normed = (flat * inverse * norm_gain).astype(jnp.bfloat16)

    def hidden_of(weights):
        both = jnp.dot(normed, weights, preferred_element_type=jnp.float32)
        gate = jnp.concatenate([both[:, :256], both[:, 512:576]], axis=1)
        upward = jnp.concatenate([both[:, 256:512], both[:, 576:]], axis=1)
        return (jax.nn.silu(gate) * upward).astype(jnp.bfloat16)

    share = jnp.dot(hidden_of(gate_up_one), down_one, preferred_element_type=jnp.float32)
    share = share + jnp.dot(hidden_of(gate_up_two), down_two, preferred_element_type=jnp.float32)

    pieces = share.astype(jnp.bfloat16).reshape(n_tp, 2 * planes, n_tp, cols).transpose(0, 2, 1, 3)
    pieces = pieces.reshape(n_tp, n_tp * 2 * planes, cols)
    pieces = jnp.concatenate([pieces, own.reshape(n_tp, tok_rows, cols)], axis=1)
    shares = exchange(pieces, "tp")
    main = shares[:, : n_tp * 2 * planes].astype(jnp.float32)
    main = main.reshape(pairs, 2, n_tp, 2, planes, cols).sum(axis=0).astype(jnp.bfloat16)
    own_rows = shares[:, n_tp * 2 * planes :].transpose(1, 0, 2).reshape(tok_rows, width)

    returning = main.transpose(3, 1, 0, 2, 4).reshape(planes, n_tp * 4, cols)
    returned = exchange(returning, "sp", same_core)
    returned = returned.reshape(planes, n_tp, 4, cols).transpose(0, 2, 1, 3).reshape(2 * n_sp, width)
    place = (slots[:, :, None] == jnp.arange(2 * n_sp)[None, None, :]).astype(jnp.bfloat16)
    first = jnp.dot(place[:, 0], returned, preferred_element_type=jnp.float32)
    second = jnp.dot(place[:, 1], returned, preferred_element_type=jnp.float32)
    mixture = route_weights[:, 0:1] * first + route_weights[:, 1:2] * second
    hidden_state = residual.astype(jnp.float32) + own_rows.astype(jnp.float32)
    return (hidden_state + mixture).astype(jnp.bfloat16)


def solution(mesh):
    in_specs = (
        P("sp", "tp"),
        P("sp", "tp"),
        P("sp", "tp"),
        P("tp"),
        P(None, "tp"),
        P(("sp", "tp"), None),
        P(),
        P(("sp", "tp"), None),
        P(("sp", "tp"), None),
        P("sp", None, "tp"),
        P("sp", None, "tp"),
        P("sp", "tp", None),
    )
    out_specs = P(("sp", "tp"), None)
    return jax.shard_map(local, mesh=mesh, in_specs=in_specs, out_specs=out_specs, check_vma=False)
```

```python
import jax
import jax.numpy as jnp
from jax import lax
from jax.experimental import pallas as pl
from jax.experimental.pallas import tpu as pltpu
from jax.sharding import PartitionSpec as P


HEADS = 32
KV_HEADS = 16
HEAD = 64
WINDOW = 128

EPS = 1e-06
NEGATIVE = -1e30


def halo(block, width):
    count = lax.axis_size("sp")
    forward = [(i, i + 1) for i in range(count - 1)]
    backward = [(target, source) for source, target in forward]
    low = lax.ppermute(block[-width:], "sp", forward)
    high = lax.ppermute(block[:width], "sp", backward)
    return jnp.concatenate([low, block, high], axis=0)


def make_band(extended, length):
    blocks = length // WINDOW
    pieces = [
        lax.slice_in_dim(extended, offset * WINDOW, offset * WINDOW + length, axis=0).reshape(
            blocks, WINDOW, -1
        )
        for offset in range(3)
    ]
    return jnp.concatenate(pieces, axis=1)


def attend_local(queries, keys, values, sink_logit):
    length = queries.shape[0]
    groups = keys.shape[1] // HEAD
    repeat = HEADS // KV_HEADS
    blocks = length // WINDOW
    joined = jnp.concatenate([keys, values], axis=1)
    extended = halo(joined, WINDOW)
    banded = make_band(extended, length)
    key_band = banded[..., : groups * HEAD].reshape(blocks, 3 * WINDOW, groups, HEAD)
    value_band = banded[..., groups * HEAD :].reshape(blocks, 3 * WINDOW, groups, HEAD)
    query_blocks = queries.reshape(blocks, WINDOW, groups, repeat, HEAD)
    scores = jnp.einsum(
        "nqgrd,nkgd->ngrqk", query_blocks, key_band, preferred_element_type=jnp.float32
    ) * HEAD ** (-0.5)
    near = jnp.abs(jnp.arange(WINDOW)[:, None] + WINDOW - jnp.arange(3 * WINDOW)[None, :]) <= WINDOW
    first_token = lax.axis_index("sp") * length
    key_pos = (
        first_token + (jnp.arange(blocks)[:, None] - 1) * WINDOW + jnp.arange(3 * WINDOW)[None, :]
    )
    inside = (key_pos >= 0) & (key_pos < length * lax.axis_size("sp"))
    valid = near[None, None, None, :, :] & inside[:, None, None, None, :]
    sinks = sink_logit.reshape(1, groups, repeat, 1, 1)
    masked = jnp.where(valid, scores, NEGATIVE)
    top = jnp.maximum(jnp.max(masked, axis=-1, keepdims=True), sinks)
    probs = jnp.exp(masked - top)
    denom = jnp.sum(probs, axis=-1, keepdims=True) + jnp.exp(sinks - top)
    weights = (probs / denom).astype(jnp.bfloat16)
    output = jnp.einsum(
        "ngrqk,nkgd->nqgrd", weights, value_band, preferred_element_type=jnp.float32
    )
    return output.astype(jnp.bfloat16).reshape(length, groups * repeat * HEAD)


def exchange(value, axis, groups=None):
    return lax.all_to_all(
        value, axis, split_axis=0, concat_axis=0, tiled=True, axis_index_groups=groups
    )


def expert_kernel(
    serves,
    gathered,
    own,
    gain,
    gate_own,
    up_own,
    down_own,
    gate_one,
    up_one,
    down_one,
    gate_two,
    up_two,
    down_two,
    out,
    gate,
    up,
    down,
    normed,
    sems,
):
    half = gate_own.shape[0]
    width = gate_own.shape[1]
    pairs, rows, piece = gathered.shape
    members = out.shape[0]
    each = rows // members
    tiles = width // 128
    lower = [
        pltpu.make_async_copy(source, target.at[pl.ds(0, half)], sems.at[i])
        for i, (source, target) in enumerate(((gate_one, gate), (up_one, up), (down_one, down)))
    ]
    for copy in lower:
        copy.start()

    def upper(sources):
        return [
            pltpu.make_async_copy(source, target.at[pl.ds(half, half)], sems.at[3 + i])
            for i, (source, target) in enumerate(zip(sources, (gate, up, down)))
        ]

    @pl.when(serves[0] == 1)
    def _():
        for copy in upper((gate_own, up_own, down_own)):
            copy.start()

    @pl.when(serves[0] != 1)
    def _():
        for copy in upper((gate_two, up_two, down_two)):
            copy.start()

    total = jnp.zeros((rows, 1), jnp.float32)
    for k in range(pairs):
        part = gathered[k].astype(jnp.float32)
        total = total + jnp.sum(part * part, axis=-1, keepdims=True)
    inverse = lax.rsqrt(total * (1.0 / width) + EPS)
    for k in range(pairs):
        part = gathered[k].astype(jnp.float32)
        scaled = part * inverse * gain[:, k * piece : (k + 1) * piece]
        normed[:, k * piece : (k + 1) * piece] = scaled.astype(jnp.bfloat16)
    for t in range(members):
        out[t, each * tiles :, :] = own[t * 16 : (t + 1) * 16, :]
    others = upper((gate_two, up_two, down_two))
    for copy in (lower[0], others[0], lower[1], others[1]):
        copy.wait()
    contract = (((1,), (1,)), ((), ()))
    hidden = []
    for start, size in ((0, 256), (256, 256), (512, 128)):
        g = lax.dot_general(
            normed[...], gate[pl.ds(start, size), :], contract, preferred_element_type=jnp.float32
        )
        u = lax.dot_general(
            normed[...], up[pl.ds(start, size), :], contract, preferred_element_type=jnp.float32
        )
        hidden.append((g / (1.0 + jnp.exp(-g)) * u).astype(jnp.bfloat16))
    hidden = jnp.concatenate(hidden, axis=1)
    lower[2].wait()
    others[2].wait()
    for chunk in range(width // 256):
        share = jnp.dot(
            hidden, down[:, pl.ds(chunk * 256, 256)], preferred_element_type=jnp.float32
        ).astype(jnp.bfloat16)
        for t in range(members):
            for side in range(2):
                tile = chunk * 2 + side
                out[t, tile * each : (tile + 1) * each, :] = share[
                    t * each : (t + 1) * each, side * 128 : (side + 1) * 128
                ]


def run_expert(serves, gathered, own, norm_gain, owned, first, second):
    pairs, rows, _ = gathered.shape
    half, width = owned[0].shape
    members = 2 * pairs
    vmem = pl.BlockSpec(memory_space=pltpu.VMEM)
    anywhere = pl.BlockSpec(memory_space=pl.ANY)
    return pl.pallas_call(
        expert_kernel,
        out_shape=jax.ShapeDtypeStruct(
            (members, rows // members * (width // 128) + 16, 128), jnp.bfloat16
        ),
        in_specs=[pl.BlockSpec(memory_space=pltpu.SMEM), vmem, vmem, vmem] + [anywhere] * 9,
        out_specs=vmem,
        scratch_shapes=[pltpu.VMEM((2 * half, width), jnp.bfloat16) for _ in range(3)]
        + [pltpu.VMEM((rows, width), jnp.bfloat16), pltpu.SemaphoreType.DMA((6,))],
        cost_estimate=pl.CostEstimate(
            flops=12 * rows * half * width,
            bytes_accessed=12 * half * width + 4 * rows * width,
            transcendentals=2 * rows * half,
        ),
        compiler_params=pltpu.CompilerParams(vmem_limit_bytes=28 * 2**20),
        name="expert",
    )(serves, gathered, own, norm_gain.reshape(1, -1), *owned, *first, *second)


def sum_kernel(shares, out, acc):
    members, rows, _ = shares.shape
    planes = out.shape[0]
    tiles = (rows - 16) // (2 * planes)
    for side in range(2):
        for block in range(2):
            lo, size = block * (rows - 16) // 2, (rows - 16) // 2
            total = shares[side, pl.ds(lo, size), :].astype(jnp.float32)
            for k in range(1, members // 2):
                total = total + shares[2 * k + side, pl.ds(lo, size), :].astype(jnp.float32)
            acc[pl.ds(lo, size), :] = total
        for rank in range(2):
            for plane in range(planes):
                rows_of = acc[pl.ds(rank * planes + plane, tiles, stride=2 * planes), :]
                at = (side * 2 + rank) * tiles
                out[plane, at : at + tiles, :] = rows_of.astype(jnp.bfloat16)


def sum_shares(shares, planes):
    members, rows, lanes = shares.shape
    tiles = (rows - 16) // (2 * planes)
    vmem = pl.BlockSpec(memory_space=pltpu.VMEM)
    return pl.pallas_call(
        sum_kernel,
        out_shape=jax.ShapeDtypeStruct((planes, 4 * tiles, lanes), jnp.bfloat16),
        in_specs=[vmem],
        out_specs=vmem,
        scratch_shapes=[pltpu.VMEM((rows - 16, lanes), jnp.float32)],
        cost_estimate=pl.CostEstimate(
            flops=members * rows * lanes, bytes_accessed=2 * members * rows * lanes, transcendentals=0
        ),
        compiler_params=pltpu.CompilerParams(vmem_limit_bytes=8 * 2**20),
        name="shares",
    )(shares)


def local(
    queries,
    keys,
    values,
    sink_logit,
    out_weight,
    residual,
    norm_gain,
    routes,
    route_weights,
    gate_weight,
    up_weight,
    down_weight,
):
    n_sp, n_tp = lax.axis_size("sp"), lax.axis_size("tp")
    planes = n_sp // 2
    pairs = n_tp // 2
    tok_rows, width = residual.shape
    cols = width // n_tp
    length = queries.shape[0]
    parity = lax.axis_index("tp") % 2
    same_core = [[plane * 2 + core for plane in range(planes)] for core in range(2)]
    same_parity = [[pair * 2 + side for pair in range(pairs)] for side in range(2)]

    swap_pair = [(t, t ^ 1) for t in range(n_tp)]
    first_moves, second_moves = [], []
    for plane in range(planes):
        for core in range(2):
            for member in range(n_tp):
                source = (plane * 2 + core) * n_tp + member
                across = (plane * 2 + 1 - core) * n_tp + member
                if member % 2 == core:
                    first_moves.append((source, across))
                    second_moves.append((source, across))
                else:
                    first_moves.append((source, source ^ 1))
    serves = (lax.axis_index("sp") % 2 == parity).astype(jnp.int32).reshape(1)
    gate_own, up_own, down_own = gate_weight[0].T, up_weight[0].T, down_weight[0]
    out_other = lax.ppermute(out_weight, "tp", swap_pair)
    gate_one = lax.ppermute(gate_own, ("sp", "tp"), first_moves)
    up_one = lax.ppermute(up_own, ("sp", "tp"), first_moves)
    down_one = lax.ppermute(down_own, ("sp", "tp"), first_moves)
    gate_two = lax.ppermute(gate_one, ("sp", "tp"), second_moves)
    up_two = lax.ppermute(up_one, ("sp", "tp"), second_moves)
    down_two = lax.ppermute(down_one, ("sp", "tp"), second_moves)

    expert_ids = routes.reshape(-1)
    onehot = (expert_ids[:, None] == jnp.arange(n_sp, dtype=jnp.int32)[None, :]).astype(jnp.int32)
    earlier = jnp.cumsum(onehot, axis=0) - onehot
    rank = jnp.sum(earlier * onehot, axis=1)
    slots = (expert_ids * 2 + rank).reshape(tok_rows, 2)

    attention = attend_local(queries, keys, values, sink_logit)

    residual_pieces = residual.reshape(tok_rows, pairs, 2, cols).transpose(1, 2, 0, 3)
    residual_pieces = jnp.repeat(residual_pieces.reshape(pairs, 2 * tok_rows, cols), 2, axis=0)
    slot_rows = jnp.pad(slots.astype(jnp.bfloat16), ((0, 0), (0, cols - 2)))
    message = jnp.concatenate(
        [
            jnp.broadcast_to(attention, (n_tp, *attention.shape)),
            residual_pieces,
            jnp.broadcast_to(slot_rows, (n_tp, *slot_rows.shape)),
        ],
        axis=1,
    )
    arrived = exchange(message, "tp")
    attended = arrived[:, :length].transpose(1, 0, 2).reshape(length, width)
    residual_cols = (
        arrived[:, length : length + 2 * tok_rows]
        .reshape(n_tp, 2, tok_rows, cols)
        .transpose(0, 2, 1, 3)
        .reshape(length, 2 * cols)
    )
    slot_all = arrived[:, length + 2 * tok_rows :, :2].reshape(length, 2).astype(jnp.int32)

    own = jnp.dot(attended, out_weight, preferred_element_type=jnp.float32).astype(jnp.bfloat16)
    other = jnp.dot(attended, out_other, preferred_element_type=jnp.float32).astype(jnp.bfloat16)
    projected = jnp.concatenate(
        [jnp.where(parity == 0, own, other), jnp.where(parity == 0, other, own)], axis=1
    )
    hidden_cols = (residual_cols.astype(jnp.float32) + projected.astype(jnp.float32)).astype(
        jnp.bfloat16
    )
    wanted = (2 * jnp.arange(planes)[:, None] + parity) * 2 + jnp.arange(2)[None, :]
    named = jnp.any(slot_all[None, None] == wanted[:, :, None, None], axis=-1)
    mine = (jnp.arange(length) // tok_rows)[None, :] == jnp.arange(n_tp)[:, None]
    placing = (named[:, None] & mine[None, :, None]).astype(jnp.bfloat16)
    sending = jnp.dot(
        placing.reshape(planes * n_tp * 2, length), hidden_cols, preferred_element_type=jnp.float32
    ).astype(jnp.bfloat16)

    dispatched = exchange(sending.reshape(planes, n_tp * 2, 2 * cols), "sp", same_core)
    rows = planes * n_tp * 2
    block = dispatched.reshape(planes, n_tp, 2, 2 * cols).transpose(1, 2, 0, 3)
    block = block.reshape(rows, 2 * cols)
    gathered = exchange(jnp.broadcast_to(block, (pairs, *block.shape)), "tp", same_parity)
    pieces = run_expert(
        serves,
        gathered,
        own,
        norm_gain,
        (gate_own, up_own, down_own),
        (gate_one, up_one, down_one),
        (gate_two, up_two, down_two),
    )

    shares = exchange(pieces, "tp")
    own_rows = shares[:, 2 * n_tp * planes :].transpose(1, 0, 2).reshape(tok_rows, width)
    returning = sum_shares(shares, planes)

    returned = exchange(returning, "sp", same_core)
    returned = returned.reshape(planes * 4, width)
    place = (slots[:, :, None] == jnp.arange(2 * n_sp)[None, None, :]).astype(jnp.bfloat16)
    first = jnp.dot(place[:, 0], returned, preferred_element_type=jnp.float32)
    second = jnp.dot(place[:, 1], returned, preferred_element_type=jnp.float32)
    mixture = route_weights[:, 0:1] * first + route_weights[:, 1:2] * second
    hidden_state = residual.astype(jnp.float32) + own_rows.astype(jnp.float32)
    return (hidden_state + mixture).astype(jnp.bfloat16)


def solution(mesh):
    in_specs = (
        P("sp", "tp"),
        P("sp", "tp"),
        P("sp", "tp"),
        P("tp"),
        P(None, "tp"),
        P(("sp", "tp"), None),
        P(),
        P(("sp", "tp"), None),
        P(("sp", "tp"), None),
        P("sp", None, "tp"),
        P("sp", None, "tp"),
        P("sp", "tp", None),
    )
    out_specs = P(("sp", "tp"), None)

    return jax.shard_map(local, mesh=mesh, in_specs=in_specs, out_specs=out_specs, check_vma=False)
```

```python
import jax
import jax.numpy as jnp
from jax import lax
from jax.experimental import pallas as pl
from jax.experimental.pallas import tpu as pltpu
from jax.sharding import PartitionSpec as P


HEAD = 64
WINDOW = 128

EPS = 1e-06
NEGATIVE = -1e30


VMEM = pl.BlockSpec(memory_space=pltpu.VMEM)
SMEM = pl.BlockSpec(memory_space=pltpu.SMEM)
ANYWHERE = pl.BlockSpec(memory_space=pl.ANY)


def attend_kernel(place, sink, queries, low, own, high, residual, slots, out):
    members = out.shape[0]
    length, both = queries.shape
    tok_rows = residual.shape[0]
    total = place[1] * length
    band = jnp.concatenate([low[...], own[...], high[...]], axis=1)
    row = lax.broadcasted_iota(jnp.int32, (WINDOW, 3 * WINDOW), 0)
    col = lax.broadcasted_iota(jnp.int32, (WINDOW, 3 * WINDOW), 1)
    near = jnp.abs(row + WINDOW - col) <= WINDOW
    for block in range(length // WINDOW):
        position = place[0] * length + (block - 1) * WINDOW + col
        valid = near & (position >= 0) & (position < total)
        keys = band[:HEAD, block * WINDOW : (block + 3) * WINDOW]
        values = band[HEAD:, block * WINDOW : (block + 3) * WINDOW]
        heads = []
        for head in range(both // HEAD):
            asked = queries[block * WINDOW : (block + 1) * WINDOW, head * HEAD : (head + 1) * HEAD]
            scores = jnp.dot(asked, keys, preferred_element_type=jnp.float32) * HEAD ** (-0.5)
            masked = jnp.where(valid, scores, NEGATIVE)
            top = jnp.maximum(jnp.max(masked, axis=-1, keepdims=True), sink[head])
            probs = jnp.exp(masked - top)
            denom = jnp.sum(probs, axis=-1, keepdims=True) + jnp.exp(sink[head] - top)
            weights = (probs / denom).astype(jnp.bfloat16)
            heads.append(
                lax.dot_general(
                    weights, values, (((1,), (1,)), ((), ())), preferred_element_type=jnp.float32
                )
            )
        attended = jnp.concatenate(heads, axis=1).astype(jnp.bfloat16)
        for t in range(members):
            out[t, block * WINDOW : (block + 1) * WINDOW, :] = attended
    for t in range(members):
        out[t, length : length + tok_rows, :] = residual[:, t * 128 : (t + 1) * 128]
        out[t, length + tok_rows :, :] = slots[...]


def run_attention(place, sink, queries, low, own, high, residual, slots, members):
    length, both = queries.shape
    tok_rows = residual.shape[0]
    return pl.pallas_call(
        attend_kernel,
        out_shape=jax.ShapeDtypeStruct((members, length + 2 * tok_rows, 128), jnp.bfloat16),
        in_specs=[SMEM, SMEM] + [VMEM] * 6,
        out_specs=VMEM,
        cost_estimate=pl.CostEstimate(
            flops=4 * length * both * 3 * WINDOW,
            bytes_accessed=4 * members * length * 128,
            transcendentals=6 * length * WINDOW,
        ),
        compiler_params=pltpu.CompilerParams(vmem_limit_bytes=10 * 2**20),
        name="attend",
    )(place, sink, queries, low, own, high, residual, slots)


def project_kernel(arrived, weight, projected, sending):
    members = arrived.shape[0]
    length = projected.shape[0]
    tok_rows = length // members
    planes, per_plane, lanes = sending.shape
    total = jnp.zeros((length, lanes), jnp.float32)
    for k in range(members // 2):
        part = jnp.concatenate(
            [arrived[2 * k, :length, :], arrived[2 * k + 1, :length, :]], axis=1
        )
        total = total + jnp.dot(
            part, weight[k * 256 : (k + 1) * 256, :], preferred_element_type=jnp.float32
        )
    rounded = total.astype(jnp.bfloat16)
    projected[...] = rounded
    base = jnp.concatenate(
        [arrived[t, length : length + tok_rows, :] for t in range(members)], axis=0
    )
    hidden = (base.astype(jnp.float32) + rounded.astype(jnp.float32)).astype(jnp.bfloat16)
    slots = jnp.concatenate([arrived[t, length + tok_rows :, :] for t in range(members)], axis=0)
    slots = slots.astype(jnp.float32)
    lines = planes * per_plane
    place = lax.broadcasted_iota(jnp.int32, (1, lines), 1)
    named = place // per_plane * 4 + place // (per_plane // 2) % 2 * 2 + place % 2
    wanted = (named + place // 2 % members * (4 * planes)).astype(jnp.float32)
    device = lax.broadcasted_iota(jnp.int32, (length, 1), 0) // tok_rows * (4 * planes)
    device = device.astype(jnp.float32)
    taken = (slots[:, 0:1] + device == wanted) | (slots[:, 1:2] + device == wanted)
    placing = jnp.where(taken, 1.0, 0.0).astype(jnp.bfloat16)
    rows = lax.dot_general(
        placing, hidden, (((0,), (0,)), ((), ())), preferred_element_type=jnp.float32
    ).astype(jnp.bfloat16)
    for plane in range(planes):
        sending[plane] = rows[plane * per_plane : (plane + 1) * per_plane, :]


def project(arrived, weight, planes, length):
    members = arrived.shape[0]
    width, lanes = weight.shape
    return pl.pallas_call(
        project_kernel,
        out_shape=(
            jax.ShapeDtypeStruct((length, lanes), jnp.bfloat16),
            jax.ShapeDtypeStruct((planes, 4 * members, lanes), jnp.bfloat16),
        ),
        in_specs=[VMEM, VMEM],
        out_specs=(VMEM, VMEM),
        cost_estimate=pl.CostEstimate(
            flops=2 * length * width * lanes,
            bytes_accessed=4 * width * lanes + 2 * members * length * lanes,
            transcendentals=0,
        ),
        compiler_params=pltpu.CompilerParams(vmem_limit_bytes=12 * 2**20),
        name="project",
    )(arrived, weight)


def spread_kernel(dispatched, out, rows):
    planes, lines, _ = dispatched.shape
    members = out.shape[0]
    for plane in range(planes):
        rows[plane * lines : (plane + 1) * lines, :] = dispatched[plane].astype(jnp.float32)
    for line in range(lines):
        side, at = line // (lines // 2), line % (lines // 2)
        group = rows[pl.ds(line, planes, stride=lines), :].astype(jnp.bfloat16)
        for k in range(members // 2):
            out[2 * k + side, at * planes : (at + 1) * planes, :] = group


def spread(dispatched, members):
    planes, lines, lanes = dispatched.shape
    return pl.pallas_call(
        spread_kernel,
        out_shape=jax.ShapeDtypeStruct((members, planes * lines // 2, lanes), jnp.bfloat16),
        in_specs=[VMEM],
        out_specs=VMEM,
        scratch_shapes=[pltpu.VMEM((planes * lines, lanes), jnp.float32)],
        cost_estimate=pl.CostEstimate(
            flops=planes * lines * lanes,
            bytes_accessed=members * planes * lines * lanes,
            transcendentals=0,
        ),
        compiler_params=pltpu.CompilerParams(vmem_limit_bytes=8 * 2**20),
        name="spread",
    )(dispatched)


def exchange(value, axis, groups=None):
    return lax.all_to_all(
        value, axis, split_axis=0, concat_axis=0, tiled=True, axis_index_groups=groups
    )


def expert_kernel(
    serves,
    gathered,
    own,
    gain,
    gate_own,
    up_own,
    down_own,
    gate_one,
    up_one,
    down_one,
    gate_two,
    up_two,
    down_two,
    out,
    gate,
    up,
    down,
    normed,
    sems,
):
    half = gate_own.shape[0]
    width = gate_own.shape[1]
    pairs, rows, piece = gathered.shape
    members = out.shape[0]
    each = rows // members
    tiles = width // 128
    lower = [
        pltpu.make_async_copy(source, target.at[pl.ds(0, half)], sems.at[i])
        for i, (source, target) in enumerate(((gate_one, gate), (up_one, up), (down_one, down)))
    ]
    for copy in lower:
        copy.start()

    def upper(sources):
        return [
            pltpu.make_async_copy(source, target.at[pl.ds(half, half)], sems.at[3 + i])
            for i, (source, target) in enumerate(zip(sources, (gate, up, down)))
        ]

    @pl.when(serves[0] == 1)
    def _():
        for copy in upper((gate_own, up_own, down_own)):
            copy.start()

    @pl.when(serves[0] != 1)
    def _():
        for copy in upper((gate_two, up_two, down_two)):
            copy.start()

    total = jnp.zeros((rows, 1), jnp.float32)
    for k in range(pairs):
        part = gathered[k].astype(jnp.float32)
        total = total + jnp.sum(part * part, axis=-1, keepdims=True)
    inverse = lax.rsqrt(total * (1.0 / width) + EPS)
    for k in range(pairs):
        part = gathered[k].astype(jnp.float32)
        scaled = part * inverse * gain[:, k * piece : (k + 1) * piece]
        normed[:, k * piece : (k + 1) * piece] = scaled.astype(jnp.bfloat16)
    for t in range(members):
        out[t, each * tiles :, :] = own[t * 16 : (t + 1) * 16, :]
    others = upper((gate_two, up_two, down_two))
    for copy in (lower[0], others[0], lower[1], others[1]):
        copy.wait()
    contract = (((1,), (1,)), ((), ()))
    hidden = []
    for start, size in ((0, 256), (256, 256), (512, 128)):
        g = lax.dot_general(
            normed[...], gate[pl.ds(start, size), :], contract, preferred_element_type=jnp.float32
        )
        u = lax.dot_general(
            normed[...], up[pl.ds(start, size), :], contract, preferred_element_type=jnp.float32
        )
        hidden.append((g / (1.0 + jnp.exp(-g)) * u).astype(jnp.bfloat16))
    hidden = jnp.concatenate(hidden, axis=1)
    lower[2].wait()
    others[2].wait()
    for chunk in range(width // 256):
        share = jnp.dot(
            hidden, down[:, pl.ds(chunk * 256, 256)], preferred_element_type=jnp.float32
        ).astype(jnp.bfloat16)
        for t in range(members):
            for side in range(2):
                tile = chunk * 2 + side
                out[t, tile * each : (tile + 1) * each, :] = share[
                    t * each : (t + 1) * each, side * 128 : (side + 1) * 128
                ]


def run_expert(serves, gathered, own, norm_gain, owned, first, second):
    pairs, rows, _ = gathered.shape
    half, width = owned[0].shape
    members = pairs
    return pl.pallas_call(
        expert_kernel,
        out_shape=jax.ShapeDtypeStruct(
            (members, rows // members * (width // 128) + 16, 128), jnp.bfloat16
        ),
        in_specs=[SMEM, VMEM, VMEM, VMEM] + [ANYWHERE] * 9,
        out_specs=VMEM,
        scratch_shapes=[pltpu.VMEM((2 * half, width), jnp.bfloat16) for _ in range(3)]
        + [pltpu.VMEM((rows, width), jnp.bfloat16), pltpu.SemaphoreType.DMA((6,))],
        cost_estimate=pl.CostEstimate(
            flops=12 * rows * half * width,
            bytes_accessed=12 * half * width + 4 * rows * width,
            transcendentals=2 * rows * half,
        ),
        compiler_params=pltpu.CompilerParams(vmem_limit_bytes=28 * 2**20),
        name="expert",
    )(serves, gathered, own, norm_gain.reshape(1, -1), *owned, *first, *second)


def sum_kernel(shares, out, acc):
    members, rows, _ = shares.shape
    planes = out.shape[0]
    tiles = (rows - 16) // (2 * planes)
    for side in range(2):
        for block in range(2):
            lo, size = block * (rows - 16) // 2, (rows - 16) // 2
            total = shares[side, pl.ds(lo, size), :].astype(jnp.float32)
            for k in range(1, members // 2):
                total = total + shares[2 * k + side, pl.ds(lo, size), :].astype(jnp.float32)
            acc[pl.ds(lo, size), :] = total
        for rank in range(2):
            for plane in range(planes):
                rows_of = acc[pl.ds(rank * planes + plane, tiles, stride=2 * planes), :]
                at = (side * 2 + rank) * tiles
                out[plane, at : at + tiles, :] = rows_of.astype(jnp.bfloat16)


def sum_shares(shares, planes):
    members, rows, lanes = shares.shape
    tiles = (rows - 16) // (2 * planes)
    return pl.pallas_call(
        sum_kernel,
        out_shape=jax.ShapeDtypeStruct((planes, 4 * tiles, lanes), jnp.bfloat16),
        in_specs=[VMEM],
        out_specs=VMEM,
        scratch_shapes=[pltpu.VMEM((rows - 16, lanes), jnp.float32)],
        cost_estimate=pl.CostEstimate(
            flops=members * rows * lanes, bytes_accessed=2 * members * rows * lanes, transcendentals=0
        ),
        compiler_params=pltpu.CompilerParams(vmem_limit_bytes=8 * 2**20),
        name="shares",
    )(shares)


def local(
    queries,
    keys,
    values,
    sink_logit,
    out_weight,
    residual,
    norm_gain,
    routes,
    route_weights,
    gate_weight,
    up_weight,
    down_weight,
):
    n_sp, n_tp = lax.axis_size("sp"), lax.axis_size("tp")
    planes = n_sp // 2
    tok_rows, width = residual.shape
    cols = width // n_tp
    length = queries.shape[0]
    parity = lax.axis_index("tp") % 2
    same_core = [[plane * 2 + core for plane in range(planes)] for core in range(2)]

    first_moves, second_moves = [], []
    for plane in range(planes):
        for core in range(2):
            for member in range(n_tp):
                source = (plane * 2 + core) * n_tp + member
                across = (plane * 2 + 1 - core) * n_tp + member
                if member % 2 == core:
                    first_moves.append((source, across))
                    second_moves.append((source, across))
                else:
                    first_moves.append((source, source ^ 1))
    serves = (lax.axis_index("sp") % 2 == parity).astype(jnp.int32).reshape(1)
    gate_own, up_own, down_own = gate_weight[0].T, up_weight[0].T, down_weight[0]
    gate_one = lax.ppermute(gate_own, ("sp", "tp"), first_moves)
    up_one = lax.ppermute(up_own, ("sp", "tp"), first_moves)
    down_one = lax.ppermute(down_own, ("sp", "tp"), first_moves)
    gate_two = lax.ppermute(gate_one, ("sp", "tp"), second_moves)
    up_two = lax.ppermute(up_one, ("sp", "tp"), second_moves)
    down_two = lax.ppermute(down_one, ("sp", "tp"), second_moves)

    expert_ids = routes.reshape(-1)
    count = expert_ids.shape[0]
    before = jnp.arange(count)[None, :] < jnp.arange(count)[:, None]
    same = (expert_ids[:, None] == expert_ids[None, :]) & before
    rank = jnp.sum(same.astype(jnp.int32), axis=1)
    slots = (expert_ids * 2 + rank).reshape(tok_rows, 2)
    slot_rows = jnp.pad(slots.astype(jnp.bfloat16), ((0, 0), (0, cols - 2)))

    joined = jnp.concatenate([keys.T, values.T], axis=0)
    forward = [(i, i + 1) for i in range(n_sp - 1)]
    backward = [(i + 1, i) for i in range(n_sp - 1)]
    low = lax.ppermute(joined[:, length - WINDOW :], "sp", forward)
    high = lax.ppermute(joined[:, :WINDOW], "sp", backward)
    where = jnp.stack([lax.axis_index("sp"), jnp.int32(n_sp)]).astype(jnp.int32)
    message = run_attention(
        where, sink_logit, queries, low, joined, high, residual, slot_rows, n_tp
    )

    arrived = exchange(message, "tp")
    own, sending = project(arrived, out_weight, planes, length)

    dispatched = exchange(sending, "sp", same_core)
    to_servers = spread(dispatched, n_tp)
    gathered = exchange(to_servers, "tp")
    pieces = run_expert(
        serves,
        gathered,
        own,
        norm_gain,
        (gate_own, up_own, down_own),
        (gate_one, up_one, down_one),
        (gate_two, up_two, down_two),
    )

    shares = exchange(pieces, "tp")
    own_rows = shares[:, 2 * n_tp * planes :].transpose(1, 0, 2).reshape(tok_rows, width)
    returning = sum_shares(shares, planes)

    returned = exchange(returning, "sp", same_core)
    returned = returned.reshape(planes * 4, width)
    place = (slots[:, :, None] == jnp.arange(2 * n_sp)[None, None, :]).astype(jnp.bfloat16)
    first = jnp.dot(place[:, 0], returned, preferred_element_type=jnp.float32)
    second = jnp.dot(place[:, 1], returned, preferred_element_type=jnp.float32)
    mixture = route_weights[:, 0:1] * first + route_weights[:, 1:2] * second
    hidden_state = residual.astype(jnp.float32) + own_rows.astype(jnp.float32)
    return (hidden_state + mixture).astype(jnp.bfloat16)


def solution(mesh):
    in_specs = (
        P("sp", "tp"),
        P("sp", "tp"),
        P("sp", "tp"),
        P("tp"),
        P(None, "tp"),
        P(("sp", "tp"), None),
        P(),
        P(("sp", "tp"), None),
        P(("sp", "tp"), None),
        P("sp", None, "tp"),
        P("sp", None, "tp"),
        P("sp", "tp", None),
    )
    out_specs = P(("sp", "tp"), None)

    return jax.shard_map(local, mesh=mesh, in_specs=in_specs, out_specs=out_specs, check_vma=False)
```

```python
import jax
import jax.numpy as jnp
from jax import lax
from jax.experimental import pallas as pl
from jax.experimental.pallas import tpu as pltpu
from jax.sharding import PartitionSpec as P


HEAD = 64
WINDOW = 128

EPS = 1e-06
NEGATIVE = -1e30


VMEM = pl.BlockSpec(memory_space=pltpu.VMEM)
SMEM = pl.BlockSpec(memory_space=pltpu.SMEM)
ANYWHERE = pl.BlockSpec(memory_space=pltpu.HBM)


def in_hbm(values):
    return [pltpu.with_memory_space_constraint(value, pltpu.HBM) for value in values]


def served_side(member):
    return (member + member // 4) % 2


def prep_kernel(
    keys, values, queries, residual, sink, routes, low, high, own, asked, base, sinks, slots,
    named, sems,
):
    head, length = keys.shape
    copies = [
        pltpu.make_async_copy(source, target, sems.at[i])
        for i, (source, target) in enumerate(
            (
                (keys, own.at[pl.ds(0, head)]),
                (values, own.at[pl.ds(head, head)]),
                (queries, asked),
                (residual, base),
                (sink, sinks),
                (routes, named),
            )
        )
    ]
    for copy in copies:
        copy.start()
    for copy in copies:
        copy.wait()
    low[...] = own[:, length - WINDOW :]
    high[...] = own[:, :WINDOW]
    ways, count = named.shape
    flat = named[...].astype(jnp.float32)
    row = lax.broadcasted_iota(jnp.int32, (count, count), 0)
    col = lax.broadcasted_iota(jnp.int32, (count, count), 1)
    eye = jnp.where(row == col, 1.0, 0.0)
    upright = lax.dot_general(
        eye, flat, (((1,), (1,)), ((), ())), preferred_element_type=jnp.float32
    )
    lane = lax.broadcasted_iota(jnp.int32, slots.shape, 1)
    result = jnp.zeros(slots.shape, jnp.float32)
    for way in range(ways):
        mine = upright[:, way : way + 1]
        rank = jnp.zeros((count, 1), jnp.float32)
        for other in range(ways):
            same = (flat[other : other + 1, :] == mine) & (col < row)
            rank = rank + jnp.sum(jnp.where(same, 1.0, 0.0), axis=1, keepdims=True)
        result = jnp.where(lane == way, mine * 2.0 + rank, result)
    slots[...] = result.astype(jnp.bfloat16)


def prepare(keys, values, queries, residual, sink, routes):
    head, length = keys.shape
    tok_rows = residual.shape[0]
    bf16 = jnp.bfloat16
    return pl.pallas_call(
        prep_kernel,
        out_shape=(
            jax.ShapeDtypeStruct((2 * head, WINDOW), bf16),
            jax.ShapeDtypeStruct((2 * head, WINDOW), bf16),
            jax.ShapeDtypeStruct((2 * head, length), bf16),
            jax.ShapeDtypeStruct(queries.shape, bf16),
            jax.ShapeDtypeStruct(residual.shape, bf16),
            jax.ShapeDtypeStruct(sink.shape, jnp.float32),
            jax.ShapeDtypeStruct((tok_rows, 128), bf16),
        ),
        in_specs=[ANYWHERE] * 6,
        out_specs=(VMEM,) * 7,
        scratch_shapes=[pltpu.VMEM(routes.shape, jnp.int32), pltpu.SemaphoreType.DMA((6,))],
        compiler_params=pltpu.CompilerParams(vmem_limit_bytes=4 * 2**20),
        name="prepare",
    )(*in_hbm((keys, values, queries, residual, sink, routes)))


def attend_kernel(place, sink, queries, low, own, high, residual, slots, out):
    members = out.shape[0]
    length, both = queries.shape
    tok_rows = residual.shape[0]
    total = place[1] * length
    band = jnp.concatenate([low[...], own[...], high[...]], axis=1)
    row = lax.broadcasted_iota(jnp.int32, (WINDOW, 3 * WINDOW), 0)
    col = lax.broadcasted_iota(jnp.int32, (WINDOW, 3 * WINDOW), 1)
    near = jnp.abs(row + WINDOW - col) <= WINDOW
    for block in range(length // WINDOW):
        position = place[0] * length + (block - 1) * WINDOW + col
        valid = near & (position >= 0) & (position < total)
        keys = band[:HEAD, block * WINDOW : (block + 3) * WINDOW]
        values = band[HEAD:, block * WINDOW : (block + 3) * WINDOW]
        heads = []
        for head in range(both // HEAD):
            asked = queries[block * WINDOW : (block + 1) * WINDOW, head * HEAD : (head + 1) * HEAD]
            scores = jnp.dot(asked, keys, preferred_element_type=jnp.float32) * HEAD ** (-0.5)
            masked = jnp.where(valid, scores, NEGATIVE)
            bound = sink[:, head : head + 1]
            top = jnp.maximum(jnp.max(masked, axis=-1, keepdims=True), bound)
            probs = jnp.exp(masked - top)
            denom = jnp.sum(probs, axis=-1, keepdims=True) + jnp.exp(bound - top)
            weights = (probs / denom).astype(jnp.bfloat16)
            heads.append(
                lax.dot_general(
                    weights, values, (((1,), (1,)), ((), ())), preferred_element_type=jnp.float32
                )
            )
        attended = jnp.concatenate(heads, axis=1).astype(jnp.bfloat16)
        for t in range(members):
            out[t, block * WINDOW : (block + 1) * WINDOW, :] = attended
    for t in range(members):
        out[t, length : length + tok_rows, :] = residual[:, t * 128 : (t + 1) * 128]
        out[t, length + tok_rows :, :] = slots[...]


def run_attention(place, sink, queries, low, own, high, residual, slots, members):
    length, both = queries.shape
    tok_rows = residual.shape[0]
    return pl.pallas_call(
        attend_kernel,
        out_shape=jax.ShapeDtypeStruct((members, length + 2 * tok_rows, 128), jnp.bfloat16),
        in_specs=[SMEM] + [VMEM] * 7,
        out_specs=VMEM,
        cost_estimate=pl.CostEstimate(
            flops=4 * length * both * 3 * WINDOW,
            bytes_accessed=4 * members * length * 128,
            transcendentals=6 * length * WINDOW,
        ),
        compiler_params=pltpu.CompilerParams(vmem_limit_bytes=10 * 2**20),
        name="attend",
    )(place, sink, queries, low, own, high, residual, slots)


def project_kernel(arrived, weight, projected, sending):
    members = arrived.shape[0]
    length = projected.shape[0]
    tok_rows = length // members
    planes, per_plane, lanes = sending.shape
    total = jnp.zeros((length, lanes), jnp.float32)
    for k in range(members // 2):
        part = jnp.concatenate(
            [arrived[2 * k, :length, :], arrived[2 * k + 1, :length, :]], axis=1
        )
        total = total + jnp.dot(
            part, weight[k * 256 : (k + 1) * 256, :], preferred_element_type=jnp.float32
        )
    rounded = total.astype(jnp.bfloat16)
    projected[...] = rounded
    base = jnp.concatenate(
        [arrived[t, length : length + tok_rows, :] for t in range(members)], axis=0
    )
    hidden = (base.astype(jnp.float32) + rounded.astype(jnp.float32)).astype(jnp.bfloat16)
    slots = jnp.concatenate([arrived[t, length + tok_rows :, :] for t in range(members)], axis=0)
    slots = slots.astype(jnp.float32)
    lines = planes * per_plane
    place = lax.broadcasted_iota(jnp.int32, (1, lines), 1)
    named = place // per_plane * 4 + place // (per_plane // 2) % 2 * 2 + place % 2
    wanted = (named + place // 2 % members * (4 * planes)).astype(jnp.float32)
    device = lax.broadcasted_iota(jnp.int32, (length, 1), 0) // tok_rows * (4 * planes)
    device = device.astype(jnp.float32)
    taken = (slots[:, 0:1] + device == wanted) | (slots[:, 1:2] + device == wanted)
    placing = jnp.where(taken, 1.0, 0.0).astype(jnp.bfloat16)
    rows = lax.dot_general(
        placing, hidden, (((0,), (0,)), ((), ())), preferred_element_type=jnp.float32
    ).astype(jnp.bfloat16)
    for plane in range(planes):
        sending[plane] = rows[plane * per_plane : (plane + 1) * per_plane, :]


def project(arrived, weight, planes, length):
    members = arrived.shape[0]
    width, lanes = weight.shape
    return pl.pallas_call(
        project_kernel,
        out_shape=(
            jax.ShapeDtypeStruct((length, lanes), jnp.bfloat16),
            jax.ShapeDtypeStruct((planes, 4 * members, lanes), jnp.bfloat16),
        ),
        in_specs=[VMEM, VMEM],
        out_specs=(VMEM, VMEM),
        cost_estimate=pl.CostEstimate(
            flops=2 * length * width * lanes,
            bytes_accessed=4 * width * lanes + 2 * members * length * lanes,
            transcendentals=0,
        ),
        compiler_params=pltpu.CompilerParams(vmem_limit_bytes=12 * 2**20),
        name="project",
    )(arrived, weight)


def spread_kernel(dispatched, out, rows, block, sems):
    planes, lines, _ = dispatched.shape
    members = out.shape[0]
    for plane in range(planes):
        rows[plane * lines : (plane + 1) * lines, :] = dispatched[plane].astype(jnp.float32)
    copies = [
        pltpu.make_async_copy(block.at[served_side(t)], out.at[t], sems.at[t])
        for t in range(members)
    ]
    for side in range(2):
        for at in range(lines // 2):
            group = rows[pl.ds(side * (lines // 2) + at, planes, stride=lines), :]
            block[side, at * planes : (at + 1) * planes, :] = group.astype(jnp.bfloat16)
        for t in range(members):
            if served_side(t) == side:
                copies[t].start()
    for copy in copies:
        copy.wait()


def spread(dispatched, members):
    planes, lines, lanes = dispatched.shape
    return pl.pallas_call(
        spread_kernel,
        out_shape=pltpu.HBM((members, planes * lines // 2, lanes), jnp.bfloat16),
        in_specs=[VMEM],
        out_specs=ANYWHERE,
        scratch_shapes=[
            pltpu.VMEM((planes * lines, lanes), jnp.float32),
            pltpu.VMEM((2, planes * lines // 2, lanes), jnp.bfloat16),
            pltpu.SemaphoreType.DMA((members,)),
        ],
        cost_estimate=pl.CostEstimate(
            flops=planes * lines * lanes,
            bytes_accessed=members * planes * lines * lanes,
            transcendentals=0,
        ),
        compiler_params=pltpu.CompilerParams(vmem_limit_bytes=8 * 2**20),
        name="spread",
    )(dispatched)


def exchange(value, axis, groups=None):
    return lax.all_to_all(
        value, axis, split_axis=0, concat_axis=0, tiled=True, axis_index_groups=groups
    )


def expert_kernel(
    serves, gathered, own, gain,
    gate_own, up_own, down_own,
    gate_x, up_x, down_x, gate_y, up_y, down_y,
    gate_fx, up_fx, down_fx, gate_fy, up_fy, down_fy,
    out, gate, up, down, normed, sems,
):
    half, width = gate_own.shape
    part = half // 2
    pairs, rows, piece = gathered.shape
    members = out.shape[0]
    each = rows // members
    tiles = width // 128
    targets = (gate, up, down)

    def placed(sources, start, size, base):
        return [
            pltpu.make_async_copy(source, target.at[pl.ds(start, size)], sems.at[base + i])
            for i, (source, target) in enumerate(zip(sources, targets))
        ]

    received_x = placed((gate_x, up_x, down_x), 0, part, 0)
    received_y = placed((gate_y, up_y, down_y), part, part, 3)
    held = placed((gate_own, up_own, down_own), half, half, 6)
    forwarded_x = placed((gate_fx, up_fx, down_fx), half, part, 6)
    forwarded_y = placed((gate_fy, up_fy, down_fy), half + part, part, 6)
    for copy in received_x + received_y:
        copy.start()

    @pl.when(serves[0] == 1)
    def _():
        for copy in held:
            copy.start()

    @pl.when(serves[0] != 1)
    def _():
        for copy in forwarded_x + forwarded_y:
            copy.start()

    total = jnp.zeros((rows, 1), jnp.float32)
    for k in range(pairs):
        block = gathered[k].astype(jnp.float32)
        total = total + jnp.sum(block * block, axis=-1, keepdims=True)
    inverse = lax.rsqrt(total * (1.0 / width) + EPS)
    for k in range(pairs):
        block = gathered[k].astype(jnp.float32)
        scaled = block * inverse * gain[:, k * piece : (k + 1) * piece]
        normed[:, k * piece : (k + 1) * piece] = scaled.astype(jnp.bfloat16)
    for t in range(members):
        out[t, each * tiles :, :] = own[t * 16 : (t + 1) * 16, :]
    for i in range(2):
        for copy in (received_x[i], received_y[i], held[i]):
            copy.wait()
    contract = (((1,), (1,)), ((), ()))
    hidden = []
    for start, size in ((0, 256), (256, 256), (512, 128)):
        g = lax.dot_general(
            normed[...], gate[pl.ds(start, size), :], contract, preferred_element_type=jnp.float32
        )
        u = lax.dot_general(
            normed[...], up[pl.ds(start, size), :], contract, preferred_element_type=jnp.float32
        )
        hidden.append((g / (1.0 + jnp.exp(-g)) * u).astype(jnp.bfloat16))
    hidden = jnp.concatenate(hidden, axis=1)
    for copy in (received_x[2], received_y[2], held[2]):
        copy.wait()
    for chunk in range(width // 256):
        share = jnp.dot(
            hidden, down[:, pl.ds(chunk * 256, 256)], preferred_element_type=jnp.float32
        ).astype(jnp.bfloat16)
        for t in range(members):
            for side in range(2):
                tile = chunk * 2 + side
                out[t, tile * each : (tile + 1) * each, :] = share[
                    t * each : (t + 1) * each, side * 128 : (side + 1) * 128
                ]


def run_expert(serves, gathered, own, norm_gain, owned, moved):
    pairs, rows, _ = gathered.shape
    half, width = owned[0].shape
    members = pairs
    return pl.pallas_call(
        expert_kernel,
        out_shape=jax.ShapeDtypeStruct(
            (members, rows // members * (width // 128) + 16, 128), jnp.bfloat16
        ),
        in_specs=[SMEM, VMEM, VMEM, VMEM] + [ANYWHERE] * 15,
        out_specs=VMEM,
        scratch_shapes=[pltpu.VMEM((2 * half, width), jnp.bfloat16) for _ in range(3)]
        + [pltpu.VMEM((rows, width), jnp.bfloat16), pltpu.SemaphoreType.DMA((9,))],
        cost_estimate=pl.CostEstimate(
            flops=12 * rows * half * width,
            bytes_accessed=12 * half * width + 4 * rows * width,
            transcendentals=2 * rows * half,
        ),
        compiler_params=pltpu.CompilerParams(vmem_limit_bytes=28 * 2**20),
        name="expert",
    )(serves, gathered, own, norm_gain.reshape(1, -1), *in_hbm(owned), *in_hbm(moved))


def sum_kernel(shares, out, acc):
    members, rows, lanes = shares.shape
    planes = out.shape[0]
    tiles = (rows - 16) // (2 * planes)
    for side in range(2):
        for block in range(2):
            lo, size = block * (rows - 16) // 2, (rows - 16) // 2
            total = jnp.zeros((size, lanes), jnp.float32)
            for t in range(members):
                if served_side(t) == side:
                    total = total + shares[t, pl.ds(lo, size), :].astype(jnp.float32)
            acc[pl.ds(lo, size), :] = total
        for rank in range(2):
            for plane in range(planes):
                rows_of = acc[pl.ds(rank * planes + plane, tiles, stride=2 * planes), :]
                at = (side * 2 + rank) * tiles
                out[plane, at : at + tiles, :] = rows_of.astype(jnp.bfloat16)


def sum_shares(shares, planes):
    members, rows, lanes = shares.shape
    tiles = (rows - 16) // (2 * planes)
    return pl.pallas_call(
        sum_kernel,
        out_shape=jax.ShapeDtypeStruct((planes, 4 * tiles, lanes), jnp.bfloat16),
        in_specs=[VMEM],
        out_specs=VMEM,
        scratch_shapes=[pltpu.VMEM((rows - 16, lanes), jnp.float32)],
        cost_estimate=pl.CostEstimate(
            flops=members * rows * lanes, bytes_accessed=2 * members * rows * lanes, transcendentals=0
        ),
        compiler_params=pltpu.CompilerParams(vmem_limit_bytes=8 * 2**20),
        name="shares",
    )(shares)


def local(
    queries,
    keys,
    values,
    sink_logit,
    out_weight,
    residual,
    norm_gain,
    routes,
    route_weights,
    gate_weight,
    up_weight,
    down_weight,
):
    n_sp, n_tp = lax.axis_size("sp"), lax.axis_size("tp")
    planes = n_sp // 2
    tok_rows, width = residual.shape
    length = queries.shape[0]
    same_core = [[plane * 2 + core for plane in range(planes)] for core in range(2)]

    moves_x, moves_y, passes = [], [], []
    for plane in range(planes):
        for core in range(2):
            for member in range(n_tp):
                source = (plane * 2 + core) * n_tp + member
                across = (plane * 2 + 1 - core) * n_tp + member
                if served_side(member) == core:
                    for moves in (moves_x, moves_y, passes):
                        moves.append((source, across))
                else:
                    moves_x.append((source, source ^ 1))
                    moves_y.append((source, source ^ 4))
    core_index = lax.axis_index("sp") % 2
    serves = (core_index == served_side(lax.axis_index("tp"))).astype(jnp.int32).reshape(1)
    owned = (gate_weight[0].T, up_weight[0].T, down_weight[0])
    part = owned[0].shape[0] // 2
    received, forwarded = [], []
    for direction, moves in (("x", moves_x), ("y", moves_y)):
        lo = 0 if direction == "x" else part
        for weight in owned:
            piece = weight[lo : lo + part]
            received.append(lax.ppermute(piece, ("sp", "tp"), moves))
            forwarded.append(lax.ppermute(received[-1], ("sp", "tp"), passes))

    low, high, joined, asked, base, sinks, slot_rows = prepare(
        keys.T, values.T, queries, residual, sink_logit.reshape(1, -1), routes.T
    )
    forward = [(i, i + 1) for i in range(n_sp - 1)]
    backward = [(i + 1, i) for i in range(n_sp - 1)]
    low = lax.ppermute(low, "sp", forward)
    high = lax.ppermute(high, "sp", backward)
    where = jnp.stack([lax.axis_index("sp"), jnp.int32(n_sp)]).astype(jnp.int32)
    message = run_attention(where, sinks, asked, low, joined, high, base, slot_rows, n_tp)

    arrived = exchange(message, "tp")
    own, sending = project(arrived, out_weight, planes, length)

    dispatched = exchange(sending, "sp", same_core)
    to_servers = spread(dispatched, n_tp)
    gathered = exchange(to_servers, "tp")
    pieces = run_expert(serves, gathered, own, norm_gain, owned, (*received, *forwarded))

    shares = exchange(pieces, "tp")
    own_rows = shares[:, 2 * n_tp * planes :].transpose(1, 0, 2).reshape(tok_rows, width)
    returning = sum_shares(shares, planes)

    returned = exchange(returning, "sp", same_core)
    returned = returned.reshape(planes * 4, width)
    slots = slot_rows[:, :2].astype(jnp.int32)
    place = (slots[:, :, None] == jnp.arange(2 * n_sp)[None, None, :]).astype(jnp.bfloat16)
    first = jnp.dot(place[:, 0], returned, preferred_element_type=jnp.float32)
    second = jnp.dot(place[:, 1], returned, preferred_element_type=jnp.float32)
    mixture = route_weights[:, 0:1] * first + route_weights[:, 1:2] * second
    hidden_state = residual.astype(jnp.float32) + own_rows.astype(jnp.float32)
    return (hidden_state + mixture).astype(jnp.bfloat16)


def solution(mesh):
    in_specs = (
        P("sp", "tp"),
        P("sp", "tp"),
        P("sp", "tp"),
        P("tp"),
        P(None, "tp"),
        P(("sp", "tp"), None),
        P(),
        P(("sp", "tp"), None),
        P(("sp", "tp"), None),
        P("sp", None, "tp"),
        P("sp", None, "tp"),
        P("sp", "tp", None),
    )
    out_specs = P(("sp", "tp"), None)

    return jax.shard_map(local, mesh=mesh, in_specs=in_specs, out_specs=out_specs, check_vma=False)
```

```python
import jax
import jax.numpy as jnp
from jax import lax
from jax.experimental import pallas as pl
from jax.experimental.pallas import tpu as pltpu
from jax.sharding import PartitionSpec as P


HEAD = 64
WINDOW = 128

EPS = 1e-06
NEGATIVE = -1e30


VMEM = pl.BlockSpec(memory_space=pltpu.VMEM)
SMEM = pl.BlockSpec(memory_space=pltpu.SMEM)
ANYWHERE = pl.BlockSpec(memory_space=pltpu.HBM)


def in_hbm(values):
    return [pltpu.with_memory_space_constraint(value, pltpu.HBM) for value in values]


def served_side(member):
    return (member + member // 4) % 2


def prep_kernel(
    keys, values, queries, residual, sink, routes, low, high, own, asked, base, sinks, slots,
    named, sems,
):
    head, length = keys.shape
    copies = [
        pltpu.make_async_copy(source, target, sems.at[i])
        for i, (source, target) in enumerate(
            (
                (keys, own.at[pl.ds(0, head)]),
                (values, own.at[pl.ds(head, head)]),
                (queries, asked),
                (residual, base),
                (sink, sinks),
                (routes, named),
            )
        )
    ]
    for copy in copies:
        copy.start()
    for copy in copies:
        copy.wait()
    low[...] = own[:, length - WINDOW :]
    high[...] = own[:, :WINDOW]
    ways, count = named.shape
    flat = named[...].astype(jnp.float32)
    row = lax.broadcasted_iota(jnp.int32, (count, count), 0)
    col = lax.broadcasted_iota(jnp.int32, (count, count), 1)
    eye = jnp.where(row == col, 1.0, 0.0)
    upright = lax.dot_general(
        eye, flat, (((1,), (1,)), ((), ())), preferred_element_type=jnp.float32
    )
    lane = lax.broadcasted_iota(jnp.int32, slots.shape, 1)
    result = jnp.zeros(slots.shape, jnp.float32)
    for way in range(ways):
        mine = upright[:, way : way + 1]
        rank = jnp.zeros((count, 1), jnp.float32)
        for other in range(ways):
            same = (flat[other : other + 1, :] == mine) & (col < row)
            rank = rank + jnp.sum(jnp.where(same, 1.0, 0.0), axis=1, keepdims=True)
        result = jnp.where(lane == way, mine * 2.0 + rank, result)
    slots[...] = result.astype(jnp.bfloat16)


def prepare(keys, values, queries, residual, sink, routes):
    head, length = keys.shape
    tok_rows = residual.shape[0]
    bf16 = jnp.bfloat16
    return pl.pallas_call(
        prep_kernel,
        out_shape=(
            jax.ShapeDtypeStruct((2 * head, WINDOW), bf16),
            jax.ShapeDtypeStruct((2 * head, WINDOW), bf16),
            jax.ShapeDtypeStruct((2 * head, length), bf16),
            jax.ShapeDtypeStruct(queries.shape, bf16),
            jax.ShapeDtypeStruct(residual.shape, bf16),
            jax.ShapeDtypeStruct(sink.shape, jnp.float32),
            jax.ShapeDtypeStruct((tok_rows, 128), bf16),
        ),
        in_specs=[ANYWHERE] * 6,
        out_specs=(VMEM,) * 7,
        scratch_shapes=[pltpu.VMEM(routes.shape, jnp.int32), pltpu.SemaphoreType.DMA((6,))],
        compiler_params=pltpu.CompilerParams(vmem_limit_bytes=4 * 2**20),
        name="prepare",
    )(*in_hbm((keys, values, queries, residual, sink, routes)))


def attend_kernel(place, sink, queries, low, own, high, residual, slots, out):
    members = out.shape[0]
    length, both = queries.shape
    tok_rows = residual.shape[0]
    total = place[1] * length
    band = jnp.concatenate([low[...], own[...], high[...]], axis=1)
    row = lax.broadcasted_iota(jnp.int32, (WINDOW, 3 * WINDOW), 0)
    col = lax.broadcasted_iota(jnp.int32, (WINDOW, 3 * WINDOW), 1)
    near = jnp.abs(row + WINDOW - col) <= WINDOW
    for block in range(length // WINDOW):
        position = place[0] * length + (block - 1) * WINDOW + col
        valid = near & (position >= 0) & (position < total)
        keys = band[:HEAD, block * WINDOW : (block + 3) * WINDOW]
        values = band[HEAD:, block * WINDOW : (block + 3) * WINDOW]
        heads = []
        for head in range(both // HEAD):
            asked = queries[block * WINDOW : (block + 1) * WINDOW, head * HEAD : (head + 1) * HEAD]
            scores = jnp.dot(asked, keys, preferred_element_type=jnp.float32) * HEAD ** (-0.5)
            masked = jnp.where(valid, scores, NEGATIVE)
            bound = sink[:, head : head + 1]
            top = jnp.maximum(jnp.max(masked, axis=-1, keepdims=True), bound)
            probs = jnp.exp(masked - top)
            denom = jnp.sum(probs, axis=-1, keepdims=True) + jnp.exp(bound - top)
            weights = (probs / denom).astype(jnp.bfloat16)
            heads.append(
                lax.dot_general(
                    weights, values, (((1,), (1,)), ((), ())), preferred_element_type=jnp.float32
                )
            )
        attended = jnp.concatenate(heads, axis=1).astype(jnp.bfloat16)
        for t in range(members):
            out[t, block * WINDOW : (block + 1) * WINDOW, :] = attended
    for t in range(members):
        out[t, length : length + tok_rows, :] = residual[:, t * 128 : (t + 1) * 128]
        out[t, length + tok_rows :, :] = slots[...]


def run_attention(place, sink, queries, low, own, high, residual, slots, members):
    length, both = queries.shape
    tok_rows = residual.shape[0]
    return pl.pallas_call(
        attend_kernel,
        out_shape=jax.ShapeDtypeStruct((members, length + 2 * tok_rows, 128), jnp.bfloat16),
        in_specs=[SMEM] + [VMEM] * 7,
        out_specs=VMEM,
        cost_estimate=pl.CostEstimate(
            flops=4 * length * both * 3 * WINDOW,
            bytes_accessed=4 * members * length * 128,
            transcendentals=6 * length * WINDOW,
        ),
        compiler_params=pltpu.CompilerParams(vmem_limit_bytes=10 * 2**20),
        name="attend",
    )(place, sink, queries, low, own, high, residual, slots)


def project_kernel(arrived, weight, projected, sending):
    members = arrived.shape[0]
    length = projected.shape[0]
    tok_rows = length // members
    planes, per_plane, lanes = sending.shape
    total = jnp.zeros((length, lanes), jnp.float32)
    for k in range(members // 2):
        part = jnp.concatenate(
            [arrived[2 * k, :length, :], arrived[2 * k + 1, :length, :]], axis=1
        )
        total = total + jnp.dot(
            part, weight[k * 256 : (k + 1) * 256, :], preferred_element_type=jnp.float32
        )
    rounded = total.astype(jnp.bfloat16)
    projected[...] = rounded
    base = jnp.concatenate(
        [arrived[t, length : length + tok_rows, :] for t in range(members)], axis=0
    )
    hidden = (base.astype(jnp.float32) + rounded.astype(jnp.float32)).astype(jnp.bfloat16)
    slots = jnp.concatenate([arrived[t, length + tok_rows :, :] for t in range(members)], axis=0)
    slots = slots.astype(jnp.float32)
    lines = planes * per_plane
    place = lax.broadcasted_iota(jnp.int32, (1, lines), 1)
    named = place // per_plane * 4 + place // (per_plane // 2) % 2 * 2 + place % 2
    wanted = (named + place // 2 % members * (4 * planes)).astype(jnp.float32)
    device = lax.broadcasted_iota(jnp.int32, (length, 1), 0) // tok_rows * (4 * planes)
    device = device.astype(jnp.float32)
    taken = (slots[:, 0:1] + device == wanted) | (slots[:, 1:2] + device == wanted)
    placing = jnp.where(taken, 1.0, 0.0).astype(jnp.bfloat16)
    rows = lax.dot_general(
        placing, hidden, (((0,), (0,)), ((), ())), preferred_element_type=jnp.float32
    ).astype(jnp.bfloat16)
    for plane in range(planes):
        sending[plane] = rows[plane * per_plane : (plane + 1) * per_plane, :]


def project(arrived, weight, planes, length):
    members = arrived.shape[0]
    width, lanes = weight.shape
    return pl.pallas_call(
        project_kernel,
        out_shape=(
            jax.ShapeDtypeStruct((length, lanes), jnp.bfloat16),
            jax.ShapeDtypeStruct((planes, 4 * members, lanes), jnp.bfloat16),
        ),
        in_specs=[VMEM, VMEM],
        out_specs=(VMEM, VMEM),
        cost_estimate=pl.CostEstimate(
            flops=2 * length * width * lanes,
            bytes_accessed=4 * width * lanes + 2 * members * length * lanes,
            transcendentals=0,
        ),
        compiler_params=pltpu.CompilerParams(vmem_limit_bytes=12 * 2**20),
        name="project",
    )(arrived, weight)


def spread_kernel(dispatched, out, rows, block, sems):
    planes, lines, _ = dispatched.shape
    members = out.shape[0]
    for plane in range(planes):
        rows[plane * lines : (plane + 1) * lines, :] = dispatched[plane].astype(jnp.float32)
    copies = [
        pltpu.make_async_copy(block.at[served_side(t)], out.at[t], sems.at[t])
        for t in range(members)
    ]
    for side in range(2):
        for at in range(lines // 2):
            group = rows[pl.ds(side * (lines // 2) + at, planes, stride=lines), :]
            block[side, at * planes : (at + 1) * planes, :] = group.astype(jnp.bfloat16)
        for t in range(members):
            if served_side(t) == side:
                copies[t].start()
    for copy in copies:
        copy.wait()


def spread(dispatched, members):
    planes, lines, lanes = dispatched.shape
    return pl.pallas_call(
        spread_kernel,
        out_shape=pltpu.HBM((members, planes * lines // 2, lanes), jnp.bfloat16),
        in_specs=[VMEM],
        out_specs=ANYWHERE,
        scratch_shapes=[
            pltpu.VMEM((planes * lines, lanes), jnp.float32),
            pltpu.VMEM((2, planes * lines // 2, lanes), jnp.bfloat16),
            pltpu.SemaphoreType.DMA((members,)),
        ],
        cost_estimate=pl.CostEstimate(
            flops=planes * lines * lanes,
            bytes_accessed=members * planes * lines * lanes,
            transcendentals=0,
        ),
        compiler_params=pltpu.CompilerParams(vmem_limit_bytes=8 * 2**20),
        name="spread",
    )(dispatched)


def exchange(value, axis, groups=None):
    return lax.all_to_all(
        value, axis, split_axis=0, concat_axis=0, tiled=True, axis_index_groups=groups
    )


def pack_kernel(gate, up, down, *rest):
    outs, sems = rest[:-1], rest[-1]
    part = gate.shape[0] // len(outs)
    copies = [
        pltpu.make_async_copy(
            source.at[pl.ds(k * part, part)], out.at[pl.ds(i * part, part)], sems.at[k * 3 + i]
        )
        for k, out in enumerate(outs)
        for i, source in enumerate((gate, up, down))
    ]
    for copy in copies:
        copy.start()
    for copy in copies:
        copy.wait()


def pack(owned, ways):
    half, width = owned[0].shape
    return pl.pallas_call(
        pack_kernel,
        out_shape=tuple(pltpu.HBM((3 * half // ways, width), jnp.bfloat16) for _ in range(ways)),
        in_specs=[ANYWHERE] * 3,
        out_specs=(ANYWHERE,) * ways,
        scratch_shapes=[pltpu.SemaphoreType.DMA((3 * ways,))],
        cost_estimate=pl.CostEstimate(
            flops=half * width, bytes_accessed=12 * half * width, transcendentals=0
        ),
        compiler_params=pltpu.CompilerParams(vmem_limit_bytes=2 * 2**20),
        name="pack",
    )(*in_hbm(owned))


def expert_kernel(
    serves, gathered, own, gain, gate_own, up_own, down_own,
    got_0, got_1, got_2, got_3, fwd_0, fwd_1, fwd_2, fwd_3,
    out, gate, up, down, normed, sems,
):
    half, width = gate_own.shape
    part = half // 4
    pairs, rows, piece = gathered.shape
    members = out.shape[0]
    each = rows // members
    tiles = width // 128
    targets = (gate, up, down)

    def placed(packed, start, base):
        return [
            pltpu.make_async_copy(
                packed.at[pl.ds(i * part, part)], target.at[pl.ds(start, part)], sems.at[base + i]
            )
            for i, target in enumerate(targets)
        ]

    received = [
        placed(packed, k * part, 3 * k) for k, packed in enumerate((got_0, got_1, got_2, got_3))
    ]
    forwarded = [
        placed(packed, half + k * part, 12) for k, packed in enumerate((fwd_0, fwd_1, fwd_2, fwd_3))
    ]
    held = [
        pltpu.make_async_copy(source, target.at[pl.ds(half, half)], sems.at[12 + i])
        for i, (source, target) in enumerate(zip((gate_own, up_own, down_own), targets))
    ]
    for i in range(3):
        for copies in received:
            copies[i].start()

    @pl.when(serves[0] == 1)
    def _():
        for copy in held:
            copy.start()

    @pl.when(serves[0] != 1)
    def _():
        for i in range(3):
            for copies in forwarded:
                copies[i].start()

    total = jnp.zeros((rows, 1), jnp.float32)
    for k in range(pairs):
        block = gathered[k].astype(jnp.float32)
        total = total + jnp.sum(block * block, axis=-1, keepdims=True)
    inverse = lax.rsqrt(total * (1.0 / width) + EPS)
    for k in range(pairs):
        block = gathered[k].astype(jnp.float32)
        scaled = block * inverse * gain[:, k * piece : (k + 1) * piece]
        normed[:, k * piece : (k + 1) * piece] = scaled.astype(jnp.bfloat16)
    for t in range(members):
        out[t, each * tiles :, :] = own[t * 16 : (t + 1) * 16, :]
    for i in range(2):
        for copy in (*(copies[i] for copies in received), held[i]):
            copy.wait()
    contract = (((1,), (1,)), ((), ()))
    hidden = []
    for start, size in ((0, 256), (256, 256), (512, 128)):
        g = lax.dot_general(
            normed[...], gate[pl.ds(start, size), :], contract, preferred_element_type=jnp.float32
        )
        u = lax.dot_general(
            normed[...], up[pl.ds(start, size), :], contract, preferred_element_type=jnp.float32
        )
        hidden.append((g / (1.0 + jnp.exp(-g)) * u).astype(jnp.bfloat16))
    hidden = jnp.concatenate(hidden, axis=1)
    for copy in (*(copies[2] for copies in received), held[2]):
        copy.wait()
    for chunk in range(width // 256):
        share = jnp.dot(
            hidden, down[:, pl.ds(chunk * 256, 256)], preferred_element_type=jnp.float32
        ).astype(jnp.bfloat16)
        for t in range(members):
            for side in range(2):
                tile = chunk * 2 + side
                out[t, tile * each : (tile + 1) * each, :] = share[
                    t * each : (t + 1) * each, side * 128 : (side + 1) * 128
                ]


def run_expert(serves, gathered, own, norm_gain, owned, moved):
    pairs, rows, _ = gathered.shape
    half, width = owned[0].shape
    members = pairs
    return pl.pallas_call(
        expert_kernel,
        out_shape=jax.ShapeDtypeStruct(
            (members, rows // members * (width // 128) + 16, 128), jnp.bfloat16
        ),
        in_specs=[SMEM, VMEM, VMEM, VMEM] + [ANYWHERE] * 11,
        out_specs=VMEM,
        scratch_shapes=[pltpu.VMEM((2 * half, width), jnp.bfloat16) for _ in range(3)]
        + [pltpu.VMEM((rows, width), jnp.bfloat16), pltpu.SemaphoreType.DMA((15,))],
        cost_estimate=pl.CostEstimate(
            flops=12 * rows * half * width,
            bytes_accessed=12 * half * width + 4 * rows * width,
            transcendentals=2 * rows * half,
        ),
        compiler_params=pltpu.CompilerParams(vmem_limit_bytes=28 * 2**20),
        name="expert",
    )(serves, gathered, own, norm_gain.reshape(1, -1), *in_hbm(owned), *in_hbm(moved))


def sum_kernel(shares, out, acc):
    members, rows, lanes = shares.shape
    planes = out.shape[0]
    tiles = (rows - 16) // (2 * planes)
    for side in range(2):
        for block in range(2):
            lo, size = block * (rows - 16) // 2, (rows - 16) // 2
            total = jnp.zeros((size, lanes), jnp.float32)
            for t in range(members):
                if served_side(t) == side:
                    total = total + shares[t, pl.ds(lo, size), :].astype(jnp.float32)
            acc[pl.ds(lo, size), :] = total
        for rank in range(2):
            for plane in range(planes):
                rows_of = acc[pl.ds(rank * planes + plane, tiles, stride=2 * planes), :]
                at = (side * 2 + rank) * tiles
                out[plane, at : at + tiles, :] = rows_of.astype(jnp.bfloat16)


def sum_shares(shares, planes):
    members, rows, lanes = shares.shape
    tiles = (rows - 16) // (2 * planes)
    return pl.pallas_call(
        sum_kernel,
        out_shape=jax.ShapeDtypeStruct((planes, 4 * tiles, lanes), jnp.bfloat16),
        in_specs=[VMEM],
        out_specs=VMEM,
        scratch_shapes=[pltpu.VMEM((rows - 16, lanes), jnp.float32)],
        cost_estimate=pl.CostEstimate(
            flops=members * rows * lanes, bytes_accessed=2 * members * rows * lanes, transcendentals=0
        ),
        compiler_params=pltpu.CompilerParams(vmem_limit_bytes=8 * 2**20),
        name="shares",
    )(shares)


def local(
    queries,
    keys,
    values,
    sink_logit,
    out_weight,
    residual,
    norm_gain,
    routes,
    route_weights,
    gate_weight,
    up_weight,
    down_weight,
):
    n_sp, n_tp = lax.axis_size("sp"), lax.axis_size("tp")
    planes = n_sp // 2
    tok_rows, width = residual.shape
    length = queries.shape[0]
    same_core = [[plane * 2 + core for plane in range(planes)] for core in range(2)]

    steps = ((0, 1), (0, 3), (1, 0), (3, 0))
    moves, passes = [[] for _ in steps], []
    for plane in range(planes):
        for core in range(2):
            for member in range(n_tp):
                source = (plane * 2 + core) * n_tp + member
                across = (plane * 2 + 1 - core) * n_tp + member
                if served_side(member) == core:
                    for way in moves:
                        way.append((source, across))
                    passes.append((source, across))
                else:
                    for way, (dy, dx) in zip(moves, steps):
                        other = (member // 4 + dy) % 4 * 4 + (member % 4 + dx) % 4
                        way.append((source, source - member + other))
    core_index = lax.axis_index("sp") % 2
    serves = (core_index == served_side(lax.axis_index("tp"))).astype(jnp.int32).reshape(1)
    owned = (gate_weight[0].T, up_weight[0].T, down_weight[0])
    received, forwarded = [], []
    packed = pack(owned, len(steps))
    for k, way in enumerate(moves):
        received.append(lax.ppermute(packed[k], ("sp", "tp"), way))
        forwarded.append(lax.ppermute(received[-1], ("sp", "tp"), passes))

    low, high, joined, asked, base, sinks, slot_rows = prepare(
        keys.T, values.T, queries, residual, sink_logit.reshape(1, -1), routes.T
    )
    forward = [(i, i + 1) for i in range(n_sp - 1)]
    backward = [(i + 1, i) for i in range(n_sp - 1)]
    low = lax.ppermute(low, "sp", forward)
    high = lax.ppermute(high, "sp", backward)
    where = jnp.stack([lax.axis_index("sp"), jnp.int32(n_sp)]).astype(jnp.int32)
    message = run_attention(where, sinks, asked, low, joined, high, base, slot_rows, n_tp)

    arrived = exchange(message, "tp")
    own, sending = project(arrived, out_weight, planes, length)

    dispatched = exchange(sending, "sp", same_core)
    to_servers = spread(dispatched, n_tp)
    gathered = exchange(to_servers, "tp")
    pieces = run_expert(serves, gathered, own, norm_gain, owned, (*received, *forwarded))

    shares = exchange(pieces, "tp")
    own_rows = shares[:, 2 * n_tp * planes :].transpose(1, 0, 2).reshape(tok_rows, width)
    returning = sum_shares(shares, planes)

    returned = exchange(returning, "sp", same_core)
    returned = returned.reshape(planes * 4, width)
    slots = slot_rows[:, :2].astype(jnp.int32)
    place = (slots[:, :, None] == jnp.arange(2 * n_sp)[None, None, :]).astype(jnp.bfloat16)
    first = jnp.dot(place[:, 0], returned, preferred_element_type=jnp.float32)
    second = jnp.dot(place[:, 1], returned, preferred_element_type=jnp.float32)
    mixture = route_weights[:, 0:1] * first + route_weights[:, 1:2] * second
    hidden_state = residual.astype(jnp.float32) + own_rows.astype(jnp.float32)
    return (hidden_state + mixture).astype(jnp.bfloat16)


def solution(mesh):
    in_specs = (
        P("sp", "tp"),
        P("sp", "tp"),
        P("sp", "tp"),
        P("tp"),
        P(None, "tp"),
        P(("sp", "tp"), None),
        P(),
        P(("sp", "tp"), None),
        P(("sp", "tp"), None),
        P("sp", None, "tp"),
        P("sp", None, "tp"),
        P("sp", "tp", None),
    )
    out_specs = P(("sp", "tp"), None)

    return jax.shard_map(local, mesh=mesh, in_specs=in_specs, out_specs=out_specs, check_vma=False)
```

```python
import jax
import jax.numpy as jnp
from jax import lax
from jax.experimental import pallas as pl
from jax.experimental.pallas import tpu as pltpu
from jax.sharding import PartitionSpec as P


HEAD = 64
WINDOW = 128

EPS = 1e-06
NEGATIVE = -1e30


VMEM = pl.BlockSpec(memory_space=pltpu.VMEM)
SMEM = pl.BlockSpec(memory_space=pltpu.SMEM)
ANYWHERE = pl.BlockSpec(memory_space=pltpu.HBM)


def in_hbm(values):
    return [pltpu.with_memory_space_constraint(value, pltpu.HBM) for value in values]


def served_side(member):
    return (member + member // 4) % 2


def prep_kernel(
    keys, values, queries, residual, sink, routes, low, high, own, asked, base, sinks, slots,
    named, sems,
):
    head, length = keys.shape
    copies = [
        pltpu.make_async_copy(source, target, sems.at[i])
        for i, (source, target) in enumerate(
            (
                (keys, own.at[pl.ds(0, head)]),
                (values, own.at[pl.ds(head, head)]),
                (queries, asked),
                (residual, base),
                (sink, sinks),
                (routes, named),
            )
        )
    ]
    for copy in copies:
        copy.start()
    for copy in copies:
        copy.wait()
    low[...] = own[:, length - WINDOW :]
    high[...] = own[:, :WINDOW]
    ways, count = named.shape
    flat = named[...].astype(jnp.float32)
    row = lax.broadcasted_iota(jnp.int32, (count, count), 0)
    col = lax.broadcasted_iota(jnp.int32, (count, count), 1)
    eye = jnp.where(row == col, 1.0, 0.0)
    upright = lax.dot_general(
        eye, flat, (((1,), (1,)), ((), ())), preferred_element_type=jnp.float32
    )
    lane = lax.broadcasted_iota(jnp.int32, slots.shape, 1)
    result = jnp.zeros(slots.shape, jnp.float32)
    for way in range(ways):
        mine = upright[:, way : way + 1]
        rank = jnp.zeros((count, 1), jnp.float32)
        for other in range(ways):
            same = (flat[other : other + 1, :] == mine) & (col < row)
            rank = rank + jnp.sum(jnp.where(same, 1.0, 0.0), axis=1, keepdims=True)
        result = jnp.where(lane == way, mine * 2.0 + rank, result)
    slots[...] = result.astype(jnp.bfloat16)


def prepare(keys, values, queries, residual, sink, routes):
    head, length = keys.shape
    tok_rows = residual.shape[0]
    bf16 = jnp.bfloat16
    return pl.pallas_call(
        prep_kernel,
        out_shape=(
            jax.ShapeDtypeStruct((2 * head, WINDOW), bf16),
            jax.ShapeDtypeStruct((2 * head, WINDOW), bf16),
            jax.ShapeDtypeStruct((2 * head, length), bf16),
            jax.ShapeDtypeStruct(queries.shape, bf16),
            jax.ShapeDtypeStruct(residual.shape, bf16),
            jax.ShapeDtypeStruct(sink.shape, jnp.float32),
            jax.ShapeDtypeStruct((tok_rows, 128), bf16),
        ),
        in_specs=[ANYWHERE] * 6,
        out_specs=(VMEM,) * 7,
        scratch_shapes=[pltpu.VMEM(routes.shape, jnp.int32), pltpu.SemaphoreType.DMA((6,))],
        compiler_params=pltpu.CompilerParams(vmem_limit_bytes=4 * 2**20),
        name="prepare",
    )(*in_hbm((keys, values, queries, residual, sink, routes)))


def attend_kernel(place, sink, queries, low, own, high, residual, slots, out):
    members = out.shape[0]
    length, both = queries.shape
    tok_rows = residual.shape[0]
    total = place[1] * length
    band = jnp.concatenate([low[...], own[...], high[...]], axis=1)
    row = lax.broadcasted_iota(jnp.int32, (WINDOW, 3 * WINDOW), 0)
    col = lax.broadcasted_iota(jnp.int32, (WINDOW, 3 * WINDOW), 1)
    near = jnp.abs(row + WINDOW - col) <= WINDOW
    for block in range(length // WINDOW):
        position = place[0] * length + (block - 1) * WINDOW + col
        valid = near & (position >= 0) & (position < total)
        keys = band[:HEAD, block * WINDOW : (block + 3) * WINDOW]
        values = band[HEAD:, block * WINDOW : (block + 3) * WINDOW]
        heads = []
        for head in range(both // HEAD):
            asked = queries[block * WINDOW : (block + 1) * WINDOW, head * HEAD : (head + 1) * HEAD]
            scores = jnp.dot(asked, keys, preferred_element_type=jnp.float32) * HEAD ** (-0.5)
            masked = jnp.where(valid, scores, NEGATIVE)
            bound = sink[:, head : head + 1]
            top = jnp.maximum(jnp.max(masked, axis=-1, keepdims=True), bound)
            probs = jnp.exp(masked - top)
            denom = jnp.sum(probs, axis=-1, keepdims=True) + jnp.exp(bound - top)
            weights = (probs / denom).astype(jnp.bfloat16)
            heads.append(
                lax.dot_general(
                    weights, values, (((1,), (1,)), ((), ())), preferred_element_type=jnp.float32
                )
            )
        attended = jnp.concatenate(heads, axis=1).astype(jnp.bfloat16)
        for t in range(members):
            out[t, block * WINDOW : (block + 1) * WINDOW, :] = attended
    for t in range(members):
        out[t, length : length + tok_rows, :] = residual[:, t * 128 : (t + 1) * 128]
        out[t, length + tok_rows :, :] = slots[...]


def run_attention(place, sink, queries, low, own, high, residual, slots, members):
    length, both = queries.shape
    tok_rows = residual.shape[0]
    return pl.pallas_call(
        attend_kernel,
        out_shape=jax.ShapeDtypeStruct((members, length + 2 * tok_rows, 128), jnp.bfloat16),
        in_specs=[SMEM] + [VMEM] * 7,
        out_specs=VMEM,
        cost_estimate=pl.CostEstimate(
            flops=4 * length * both * 3 * WINDOW,
            bytes_accessed=4 * members * length * 128,
            transcendentals=6 * length * WINDOW,
        ),
        compiler_params=pltpu.CompilerParams(vmem_limit_bytes=10 * 2**20),
        name="attend",
    )(place, sink, queries, low, own, high, residual, slots)


def project_kernel(arrived, weight, projected, sending):
    members = arrived.shape[0]
    length = projected.shape[0]
    tok_rows = length // members
    planes, per_plane, lanes = sending.shape
    total = jnp.zeros((length, lanes), jnp.float32)
    for k in range(members // 2):
        part = jnp.concatenate(
            [arrived[2 * k, :length, :], arrived[2 * k + 1, :length, :]], axis=1
        )
        total = total + jnp.dot(
            part, weight[k * 256 : (k + 1) * 256, :], preferred_element_type=jnp.float32
        )
    rounded = total.astype(jnp.bfloat16)
    projected[...] = rounded
    base = jnp.concatenate(
        [arrived[t, length : length + tok_rows, :] for t in range(members)], axis=0
    )
    hidden = (base.astype(jnp.float32) + rounded.astype(jnp.float32)).astype(jnp.bfloat16)
    slots = jnp.concatenate([arrived[t, length + tok_rows :, :] for t in range(members)], axis=0)
    slots = slots.astype(jnp.float32)
    lines = planes * per_plane
    place = lax.broadcasted_iota(jnp.int32, (1, lines), 1)
    named = place // per_plane * 4 + place // (per_plane // 2) % 2 * 2 + place % 2
    wanted = (named + place // 2 % members * (4 * planes)).astype(jnp.float32)
    device = lax.broadcasted_iota(jnp.int32, (length, 1), 0) // tok_rows * (4 * planes)
    device = device.astype(jnp.float32)
    taken = (slots[:, 0:1] + device == wanted) | (slots[:, 1:2] + device == wanted)
    placing = jnp.where(taken, 1.0, 0.0).astype(jnp.bfloat16)
    rows = lax.dot_general(
        placing, hidden, (((0,), (0,)), ((), ())), preferred_element_type=jnp.float32
    ).astype(jnp.bfloat16)
    for plane in range(planes):
        sending[plane] = rows[plane * per_plane : (plane + 1) * per_plane, :]


def project(arrived, weight, planes, length):
    members = arrived.shape[0]
    width, lanes = weight.shape
    return pl.pallas_call(
        project_kernel,
        out_shape=(
            jax.ShapeDtypeStruct((length, lanes), jnp.bfloat16),
            jax.ShapeDtypeStruct((planes, 4 * members, lanes), jnp.bfloat16),
        ),
        in_specs=[VMEM, VMEM],
        out_specs=(VMEM, VMEM),
        cost_estimate=pl.CostEstimate(
            flops=2 * length * width * lanes,
            bytes_accessed=4 * width * lanes + 2 * members * length * lanes,
            transcendentals=0,
        ),
        compiler_params=pltpu.CompilerParams(vmem_limit_bytes=12 * 2**20),
        name="project",
    )(arrived, weight)


def spread_kernel(dispatched, out, rows, block, sems):
    planes, lines, _ = dispatched.shape
    members = out.shape[0]
    for plane in range(planes):
        rows[plane * lines : (plane + 1) * lines, :] = dispatched[plane].astype(jnp.float32)
    copies = [
        pltpu.make_async_copy(block.at[served_side(t)], out.at[t], sems.at[t])
        for t in range(members)
    ]
    for side in range(2):
        for at in range(lines // 2):
            group = rows[pl.ds(side * (lines // 2) + at, planes, stride=lines), :]
            block[side, at * planes : (at + 1) * planes, :] = group.astype(jnp.bfloat16)
        for t in range(members):
            if served_side(t) == side:
                copies[t].start()
    for copy in copies:
        copy.wait()


def spread(dispatched, members):
    planes, lines, lanes = dispatched.shape
    return pl.pallas_call(
        spread_kernel,
        out_shape=pltpu.HBM((members, planes * lines // 2, lanes), jnp.bfloat16),
        in_specs=[VMEM],
        out_specs=ANYWHERE,
        scratch_shapes=[
            pltpu.VMEM((planes * lines, lanes), jnp.float32),
            pltpu.VMEM((2, planes * lines // 2, lanes), jnp.bfloat16),
            pltpu.SemaphoreType.DMA((members,)),
        ],
        cost_estimate=pl.CostEstimate(
            flops=planes * lines * lanes,
            bytes_accessed=members * planes * lines * lanes,
            transcendentals=0,
        ),
        compiler_params=pltpu.CompilerParams(vmem_limit_bytes=8 * 2**20),
        name="spread",
    )(dispatched)


def exchange(value, axis, groups=None):
    return lax.all_to_all(
        value, axis, split_axis=0, concat_axis=0, tiled=True, axis_index_groups=groups
    )


def pack_kernel(gate, up, down, *rest):
    outs, sems = rest[:-1], rest[-1]
    part = gate.shape[0] // len(outs)
    copies = [
        pltpu.make_async_copy(
            source.at[pl.ds(k * part, part)], out.at[pl.ds(i * part, part)], sems.at[k * 3 + i]
        )
        for k, out in enumerate(outs)
        for i, source in enumerate((gate, up, down))
    ]
    for copy in copies:
        copy.start()
    for copy in copies:
        copy.wait()


def pack(owned, ways):
    half, width = owned[0].shape
    return pl.pallas_call(
        pack_kernel,
        out_shape=tuple(
            jax.ShapeDtypeStruct((3 * half // ways, width), jnp.bfloat16) for _ in range(ways)
        ),
        in_specs=[ANYWHERE] * 3,
        out_specs=(VMEM,) * ways,
        scratch_shapes=[pltpu.SemaphoreType.DMA((3 * ways,))],
        cost_estimate=pl.CostEstimate(
            flops=half * width, bytes_accessed=12 * half * width, transcendentals=0
        ),
        compiler_params=pltpu.CompilerParams(vmem_limit_bytes=8 * 2**20),
        name="pack",
    )(*in_hbm(owned))


def expert_kernel(
    serves, gathered, own, gain, gate_own, up_own, down_own,
    got_0, got_1, got_2, got_3, fwd_0, fwd_1, fwd_2, fwd_3,
    out, gate, up, down, normed, sems,
):
    half, width = gate_own.shape
    part = half // 4
    pairs, rows, piece = gathered.shape
    members = out.shape[0]
    each = rows // members
    tiles = width // 128
    targets = (gate, up, down)

    def placed(packed, start, base):
        return [
            pltpu.make_async_copy(
                packed.at[pl.ds(i * part, part)], target.at[pl.ds(start, part)], sems.at[base + i]
            )
            for i, target in enumerate(targets)
        ]

    received = [
        placed(packed, k * part, 3 * k) for k, packed in enumerate((got_0, got_1, got_2, got_3))
    ]
    forwarded = [
        placed(packed, half + k * part, 12) for k, packed in enumerate((fwd_0, fwd_1, fwd_2, fwd_3))
    ]
    held = [
        pltpu.make_async_copy(source, target.at[pl.ds(half, half)], sems.at[12 + i])
        for i, (source, target) in enumerate(zip((gate_own, up_own, down_own), targets))
    ]
    for i in range(3):
        for copies in received:
            copies[i].start()

    @pl.when(serves[0] == 1)
    def _():
        for copy in held:
            copy.start()

    @pl.when(serves[0] != 1)
    def _():
        for i in range(3):
            for copies in forwarded:
                copies[i].start()

    total = jnp.zeros((rows, 1), jnp.float32)
    for k in range(pairs):
        block = gathered[k].astype(jnp.float32)
        total = total + jnp.sum(block * block, axis=-1, keepdims=True)
    inverse = lax.rsqrt(total * (1.0 / width) + EPS)
    for k in range(pairs):
        block = gathered[k].astype(jnp.float32)
        scaled = block * inverse * gain[:, k * piece : (k + 1) * piece]
        normed[:, k * piece : (k + 1) * piece] = scaled.astype(jnp.bfloat16)
    for t in range(members):
        out[t, each * tiles :, :] = own[t * 16 : (t + 1) * 16, :]
    for i in range(2):
        for copy in (*(copies[i] for copies in received), held[i]):
            copy.wait()
    contract = (((1,), (1,)), ((), ()))
    hidden = []
    for start, size in ((0, 256), (256, 256), (512, 128)):
        g = lax.dot_general(
            normed[...], gate[pl.ds(start, size), :], contract, preferred_element_type=jnp.float32
        )
        u = lax.dot_general(
            normed[...], up[pl.ds(start, size), :], contract, preferred_element_type=jnp.float32
        )
        hidden.append((g / (1.0 + jnp.exp(-g)) * u).astype(jnp.bfloat16))
    hidden = jnp.concatenate(hidden, axis=1)
    for copy in (*(copies[2] for copies in received), held[2]):
        copy.wait()
    for chunk in range(width // 256):
        share = jnp.dot(
            hidden, down[:, pl.ds(chunk * 256, 256)], preferred_element_type=jnp.float32
        ).astype(jnp.bfloat16)
        for t in range(members):
            for side in range(2):
                tile = chunk * 2 + side
                out[t, tile * each : (tile + 1) * each, :] = share[
                    t * each : (t + 1) * each, side * 128 : (side + 1) * 128
                ]


def run_expert(serves, gathered, own, norm_gain, owned, moved):
    pairs, rows, _ = gathered.shape
    half, width = owned[0].shape
    members = pairs
    return pl.pallas_call(
        expert_kernel,
        out_shape=jax.ShapeDtypeStruct(
            (members, rows // members * (width // 128) + 16, 128), jnp.bfloat16
        ),
        in_specs=[SMEM, VMEM, VMEM, VMEM] + [ANYWHERE] * 11,
        out_specs=VMEM,
        scratch_shapes=[pltpu.VMEM((2 * half, width), jnp.bfloat16) for _ in range(3)]
        + [pltpu.VMEM((rows, width), jnp.bfloat16), pltpu.SemaphoreType.DMA((15,))],
        cost_estimate=pl.CostEstimate(
            flops=12 * rows * half * width,
            bytes_accessed=12 * half * width + 4 * rows * width,
            transcendentals=2 * rows * half,
        ),
        compiler_params=pltpu.CompilerParams(vmem_limit_bytes=28 * 2**20),
        name="expert",
    )(serves, gathered, own, norm_gain.reshape(1, -1), *in_hbm(owned), *in_hbm(moved))


def sum_kernel(shares, out, acc):
    members, rows, lanes = shares.shape
    planes = out.shape[0]
    tiles = (rows - 16) // (2 * planes)
    for side in range(2):
        for block in range(2):
            lo, size = block * (rows - 16) // 2, (rows - 16) // 2
            total = jnp.zeros((size, lanes), jnp.float32)
            for t in range(members):
                if served_side(t) == side:
                    total = total + shares[t, pl.ds(lo, size), :].astype(jnp.float32)
            acc[pl.ds(lo, size), :] = total
        for rank in range(2):
            for plane in range(planes):
                rows_of = acc[pl.ds(rank * planes + plane, tiles, stride=2 * planes), :]
                at = (side * 2 + rank) * tiles
                out[plane, at : at + tiles, :] = rows_of.astype(jnp.bfloat16)


def sum_shares(shares, planes):
    members, rows, lanes = shares.shape
    tiles = (rows - 16) // (2 * planes)
    return pl.pallas_call(
        sum_kernel,
        out_shape=jax.ShapeDtypeStruct((planes, 4 * tiles, lanes), jnp.bfloat16),
        in_specs=[VMEM],
        out_specs=VMEM,
        scratch_shapes=[pltpu.VMEM((rows - 16, lanes), jnp.float32)],
        cost_estimate=pl.CostEstimate(
            flops=members * rows * lanes, bytes_accessed=2 * members * rows * lanes, transcendentals=0
        ),
        compiler_params=pltpu.CompilerParams(vmem_limit_bytes=8 * 2**20),
        name="shares",
    )(shares)


def local(
    queries,
    keys,
    values,
    sink_logit,
    out_weight,
    residual,
    norm_gain,
    routes,
    route_weights,
    gate_weight,
    up_weight,
    down_weight,
):
    n_sp, n_tp = lax.axis_size("sp"), lax.axis_size("tp")
    planes = n_sp // 2
    tok_rows, width = residual.shape
    length = queries.shape[0]
    same_core = [[plane * 2 + core for plane in range(planes)] for core in range(2)]

    steps = ((0, 1), (0, 3), (1, 0), (3, 0))
    moves, passes = [[] for _ in steps], []
    for plane in range(planes):
        for core in range(2):
            for member in range(n_tp):
                source = (plane * 2 + core) * n_tp + member
                across = (plane * 2 + 1 - core) * n_tp + member
                if served_side(member) == core:
                    for way in moves:
                        way.append((source, across))
                    passes.append((source, across))
                else:
                    for way, (dy, dx) in zip(moves, steps):
                        other = (member // 4 + dy) % 4 * 4 + (member % 4 + dx) % 4
                        way.append((source, source - member + other))
    core_index = lax.axis_index("sp") % 2
    serves = (core_index == served_side(lax.axis_index("tp"))).astype(jnp.int32).reshape(1)
    owned = (gate_weight[0].T, up_weight[0].T, down_weight[0])
    received, forwarded = [], []
    packed = pack(owned, len(steps))
    for k, way in enumerate(moves):
        received.append(lax.ppermute(packed[k], ("sp", "tp"), way))
        forwarded.append(lax.ppermute(received[-1], ("sp", "tp"), passes))

    low, high, joined, asked, base, sinks, slot_rows = prepare(
        keys.T, values.T, queries, residual, sink_logit.reshape(1, -1), routes.T
    )
    forward = [(i, i + 1) for i in range(n_sp - 1)]
    backward = [(i + 1, i) for i in range(n_sp - 1)]
    low = lax.ppermute(low, "sp", forward)
    high = lax.ppermute(high, "sp", backward)
    where = jnp.stack([lax.axis_index("sp"), jnp.int32(n_sp)]).astype(jnp.int32)
    message = run_attention(where, sinks, asked, low, joined, high, base, slot_rows, n_tp)

    arrived = exchange(message, "tp")
    own, sending = project(arrived, out_weight, planes, length)

    dispatched = exchange(sending, "sp", same_core)
    to_servers = spread(dispatched, n_tp)
    gathered = exchange(to_servers, "tp")
    pieces = run_expert(serves, gathered, own, norm_gain, owned, (*received, *forwarded))

    shares = exchange(pieces, "tp")
    own_rows = shares[:, 2 * n_tp * planes :].transpose(1, 0, 2).reshape(tok_rows, width)
    returning = sum_shares(shares, planes)

    returned = exchange(returning, "sp", same_core)
    returned = returned.reshape(planes * 4, width)
    slots = slot_rows[:, :2].astype(jnp.int32)
    place = (slots[:, :, None] == jnp.arange(2 * n_sp)[None, None, :]).astype(jnp.bfloat16)
    first = jnp.dot(place[:, 0], returned, preferred_element_type=jnp.float32)
    second = jnp.dot(place[:, 1], returned, preferred_element_type=jnp.float32)
    mixture = route_weights[:, 0:1] * first + route_weights[:, 1:2] * second
    hidden_state = residual.astype(jnp.float32) + own_rows.astype(jnp.float32)
    return (hidden_state + mixture).astype(jnp.bfloat16)


def solution(mesh):
    in_specs = (
        P("sp", "tp"),
        P("sp", "tp"),
        P("sp", "tp"),
        P("tp"),
        P(None, "tp"),
        P(("sp", "tp"), None),
        P(),
        P(("sp", "tp"), None),
        P(("sp", "tp"), None),
        P("sp", None, "tp"),
        P("sp", None, "tp"),
        P("sp", "tp", None),
    )
    out_specs = P(("sp", "tp"), None)

    return jax.shard_map(local, mesh=mesh, in_specs=in_specs, out_specs=out_specs, check_vma=False)
```

```python
import jax
import jax.numpy as jnp
from jax import lax
from jax.experimental import pallas as pl
from jax.experimental.pallas import tpu as pltpu
from jax.sharding import PartitionSpec as P


HEAD = 64
WINDOW = 128

EPS = 1e-06
NEGATIVE = -1e30


VMEM = pl.BlockSpec(memory_space=pltpu.VMEM)
SMEM = pl.BlockSpec(memory_space=pltpu.SMEM)
ANYWHERE = pl.BlockSpec(memory_space=pltpu.HBM)


def in_hbm(values):
    return [pltpu.with_memory_space_constraint(value, pltpu.HBM) for value in values]


def served_side(member):
    return (member + member // 4) % 2


def served_rank(member):
    return member // 4 % 2


def prep_kernel(
    keys, values, queries, residual, sink, routes, low, high, own, asked, base, sinks, slots,
    named, sems,
):
    head, length = keys.shape
    copies = [
        pltpu.make_async_copy(source, target, sems.at[i])
        for i, (source, target) in enumerate(
            (
                (keys, own.at[pl.ds(0, head)]),
                (values, own.at[pl.ds(head, head)]),
                (queries, asked),
                (residual, base),
                (sink, sinks),
                (routes, named),
            )
        )
    ]
    for copy in copies:
        copy.start()
    for copy in copies:
        copy.wait()
    low[...] = own[:, length - WINDOW :]
    high[...] = own[:, :WINDOW]
    ways, count = named.shape
    flat = named[...].astype(jnp.float32)
    row = lax.broadcasted_iota(jnp.int32, (count, count), 0)
    col = lax.broadcasted_iota(jnp.int32, (count, count), 1)
    eye = jnp.where(row == col, 1.0, 0.0)
    upright = lax.dot_general(
        eye, flat, (((1,), (1,)), ((), ())), preferred_element_type=jnp.float32
    )
    lane = lax.broadcasted_iota(jnp.int32, slots.shape, 1)
    result = jnp.zeros(slots.shape, jnp.float32)
    for way in range(ways):
        mine = upright[:, way : way + 1]
        rank = jnp.zeros((count, 1), jnp.float32)
        for other in range(ways):
            same = (flat[other : other + 1, :] == mine) & (col < row)
            rank = rank + jnp.sum(jnp.where(same, 1.0, 0.0), axis=1, keepdims=True)
        result = jnp.where(lane == way, mine * 2.0 + rank, result)
    slots[...] = result.astype(jnp.bfloat16)


def prepare(keys, values, queries, residual, sink, routes):
    head, length = keys.shape
    tok_rows = residual.shape[0]
    bf16 = jnp.bfloat16
    return pl.pallas_call(
        prep_kernel,
        out_shape=(
            jax.ShapeDtypeStruct((2 * head, WINDOW), bf16),
            jax.ShapeDtypeStruct((2 * head, WINDOW), bf16),
            jax.ShapeDtypeStruct((2 * head, length), bf16),
            jax.ShapeDtypeStruct(queries.shape, bf16),
            jax.ShapeDtypeStruct(residual.shape, bf16),
            jax.ShapeDtypeStruct(sink.shape, jnp.float32),
            jax.ShapeDtypeStruct((tok_rows, 128), bf16),
        ),
        in_specs=[ANYWHERE] * 6,
        out_specs=(VMEM,) * 7,
        scratch_shapes=[pltpu.VMEM(routes.shape, jnp.int32), pltpu.SemaphoreType.DMA((6,))],
        compiler_params=pltpu.CompilerParams(vmem_limit_bytes=4 * 2**20),
        name="prepare",
    )(*in_hbm((keys, values, queries, residual, sink, routes)))


def attend_kernel(place, sink, queries, low, own, high, residual, slots, out):
    members = out.shape[0]
    length, both = queries.shape
    tok_rows = residual.shape[0]
    total = place[1] * length
    band = jnp.concatenate([low[...], own[...], high[...]], axis=1)
    row = lax.broadcasted_iota(jnp.int32, (WINDOW, 3 * WINDOW), 0)
    col = lax.broadcasted_iota(jnp.int32, (WINDOW, 3 * WINDOW), 1)
    near = jnp.abs(row + WINDOW - col) <= WINDOW
    for block in range(length // WINDOW):
        position = place[0] * length + (block - 1) * WINDOW + col
        valid = near & (position >= 0) & (position < total)
        keys = band[:HEAD, block * WINDOW : (block + 3) * WINDOW]
        values = band[HEAD:, block * WINDOW : (block + 3) * WINDOW]
        heads = []
        for head in range(both // HEAD):
            asked = queries[block * WINDOW : (block + 1) * WINDOW, head * HEAD : (head + 1) * HEAD]
            scores = jnp.dot(asked, keys, preferred_element_type=jnp.float32) * HEAD ** (-0.5)
            masked = jnp.where(valid, scores, NEGATIVE)
            bound = sink[:, head : head + 1]
            top = jnp.maximum(jnp.max(masked, axis=-1, keepdims=True), bound)
            probs = jnp.exp(masked - top)
            denom = jnp.sum(probs, axis=-1, keepdims=True) + jnp.exp(bound - top)
            weights = (probs / denom).astype(jnp.bfloat16)
            heads.append(
                lax.dot_general(
                    weights, values, (((1,), (1,)), ((), ())), preferred_element_type=jnp.float32
                )
            )
        attended = jnp.concatenate(heads, axis=1).astype(jnp.bfloat16)
        for t in range(members):
            out[t, block * WINDOW : (block + 1) * WINDOW, :] = attended
    for t in range(members):
        out[t, length : length + tok_rows, :] = residual[:, t * 128 : (t + 1) * 128]
        out[t, length + tok_rows :, :] = slots[...]


def run_attention(place, sink, queries, low, own, high, residual, slots, members):
    length, both = queries.shape
    tok_rows = residual.shape[0]
    return pl.pallas_call(
        attend_kernel,
        out_shape=jax.ShapeDtypeStruct((members, length + 2 * tok_rows, 128), jnp.bfloat16),
        in_specs=[SMEM] + [VMEM] * 7,
        out_specs=VMEM,
        cost_estimate=pl.CostEstimate(
            flops=4 * length * both * 3 * WINDOW,
            bytes_accessed=4 * members * length * 128,
            transcendentals=6 * length * WINDOW,
        ),
        compiler_params=pltpu.CompilerParams(vmem_limit_bytes=10 * 2**20),
        name="attend",
    )(place, sink, queries, low, own, high, residual, slots)


def project_kernel(arrived, weight, projected, sending):
    members = arrived.shape[0]
    length = projected.shape[0]
    tok_rows = length // members
    planes, per_plane, lanes = sending.shape
    total = jnp.zeros((length, lanes), jnp.float32)
    for k in range(members // 2):
        part = jnp.concatenate(
            [arrived[2 * k, :length, :], arrived[2 * k + 1, :length, :]], axis=1
        )
        total = total + jnp.dot(
            part, weight[k * 256 : (k + 1) * 256, :], preferred_element_type=jnp.float32
        )
    rounded = total.astype(jnp.bfloat16)
    projected[...] = rounded
    base = jnp.concatenate(
        [arrived[t, length : length + tok_rows, :] for t in range(members)], axis=0
    )
    hidden = (base.astype(jnp.float32) + rounded.astype(jnp.float32)).astype(jnp.bfloat16)
    slots = jnp.concatenate([arrived[t, length + tok_rows :, :] for t in range(members)], axis=0)
    slots = slots.astype(jnp.float32)
    lines = planes * per_plane
    place = lax.broadcasted_iota(jnp.int32, (1, lines), 1)
    named = place // per_plane * 4 + place // (per_plane // 2) % 2 * 2 + place % 2
    wanted = (named + place // 2 % members * (4 * planes)).astype(jnp.float32)
    device = lax.broadcasted_iota(jnp.int32, (length, 1), 0) // tok_rows * (4 * planes)
    device = device.astype(jnp.float32)
    taken = (slots[:, 0:1] + device == wanted) | (slots[:, 1:2] + device == wanted)
    placing = jnp.where(taken, 1.0, 0.0).astype(jnp.bfloat16)
    rows = lax.dot_general(
        placing, hidden, (((0,), (0,)), ((), ())), preferred_element_type=jnp.float32
    ).astype(jnp.bfloat16)
    for plane in range(planes):
        sending[plane] = rows[plane * per_plane : (plane + 1) * per_plane, :]


def project(arrived, weight, planes, length):
    members = arrived.shape[0]
    width, lanes = weight.shape
    return pl.pallas_call(
        project_kernel,
        out_shape=(
            jax.ShapeDtypeStruct((length, lanes), jnp.bfloat16),
            jax.ShapeDtypeStruct((planes, 4 * members, lanes), jnp.bfloat16),
        ),
        in_specs=[VMEM, VMEM],
        out_specs=(VMEM, VMEM),
        cost_estimate=pl.CostEstimate(
            flops=2 * length * width * lanes,
            bytes_accessed=4 * width * lanes + 2 * members * length * lanes,
            transcendentals=0,
        ),
        compiler_params=pltpu.CompilerParams(vmem_limit_bytes=12 * 2**20),
        name="project",
    )(arrived, weight)


def spread_kernel(dispatched, out, rows, block, sems):
    planes, lines, _ = dispatched.shape
    members = out.shape[0]
    for plane in range(planes):
        rows[plane * lines : (plane + 1) * lines, :] = dispatched[plane].astype(jnp.float32)
    copies = [
        pltpu.make_async_copy(
            block.at[served_side(t) * 2 + served_rank(t)], out.at[t], sems.at[t]
        )
        for t in range(members)
    ]
    for side in range(2):
        for at in range(lines // 2):
            group = rows[pl.ds(side * (lines // 2) + at, planes, stride=lines), :]
            token, rank = at // 2, at % 2
            block[side * 2 + rank, token * planes : (token + 1) * planes, :] = group.astype(
                jnp.bfloat16
            )
        for t in range(members):
            if served_side(t) == side:
                copies[t].start()
    for copy in copies:
        copy.wait()


def spread(dispatched, members):
    planes, lines, lanes = dispatched.shape
    return pl.pallas_call(
        spread_kernel,
        out_shape=pltpu.HBM((members, planes * lines // 4, lanes), jnp.bfloat16),
        in_specs=[VMEM],
        out_specs=ANYWHERE,
        scratch_shapes=[
            pltpu.VMEM((planes * lines, lanes), jnp.float32),
            pltpu.VMEM((4, planes * lines // 4, lanes), jnp.bfloat16),
            pltpu.SemaphoreType.DMA((members,)),
        ],
        cost_estimate=pl.CostEstimate(
            flops=planes * lines * lanes,
            bytes_accessed=members * planes * lines * lanes,
            transcendentals=0,
        ),
        compiler_params=pltpu.CompilerParams(vmem_limit_bytes=8 * 2**20),
        name="spread",
    )(dispatched)


def exchange(value, axis, groups=None):
    return lax.all_to_all(
        value, axis, split_axis=0, concat_axis=0, tiled=True, axis_index_groups=groups
    )


def pack_kernel(gate, up, down, *rest):
    outs, sems = rest[:-1], rest[-1]
    part = gate.shape[0] // len(outs)
    copies = [
        pltpu.make_async_copy(
            source.at[pl.ds(k * part, part)], out.at[pl.ds(i * part, part)], sems.at[k * 3 + i]
        )
        for k, out in enumerate(outs)
        for i, source in enumerate((gate, up, down))
    ]
    for copy in copies:
        copy.start()
    for copy in copies:
        copy.wait()


def pack(owned, ways):
    half, width = owned[0].shape
    return pl.pallas_call(
        pack_kernel,
        out_shape=tuple(
            jax.ShapeDtypeStruct((3 * half // ways, width), jnp.bfloat16) for _ in range(ways)
        ),
        in_specs=[ANYWHERE] * 3,
        out_specs=(VMEM,) * ways,
        scratch_shapes=[pltpu.SemaphoreType.DMA((3 * ways,))],
        cost_estimate=pl.CostEstimate(
            flops=half * width, bytes_accessed=12 * half * width, transcendentals=0
        ),
        compiler_params=pltpu.CompilerParams(vmem_limit_bytes=8 * 2**20),
        name="pack",
    )(*in_hbm(owned))


def expert_kernel(
    serves, gathered, own, gain, gate_own, up_own, down_own,
    got_0, got_1, got_2, got_3, fwd_0, fwd_1, fwd_2, fwd_3,
    out, gate, up, down, normed, sems,
):
    half, width = gate_own.shape
    part = half // 2
    pairs, rows, piece = gathered.shape
    members = out.shape[0]
    each = rows // members
    tiles = width // 128
    targets = (gate, up, down)

    def placed(packed, start, base):
        return [
            pltpu.make_async_copy(
                packed.at[pl.ds(i * part, part)], target.at[pl.ds(start, part)], sems.at[base + i]
            )
            for i, target in enumerate(targets)
        ]

    received = [
        placed(packed, k * part, 3 * k) for k, packed in enumerate((got_0, got_1, got_2, got_3))
    ]
    received += [placed(fwd_0, 4 * part, 12), placed(fwd_1, 5 * part, 15)]
    forwarded = [placed(fwd_2, 6 * part, 18), placed(fwd_3, 7 * part, 18)]
    held = [
        pltpu.make_async_copy(source, target.at[pl.ds(3 * half, half)], sems.at[18 + i])
        for i, (source, target) in enumerate(zip((gate_own, up_own, down_own), targets))
    ]
    for copies in received:
        for copy in copies[:2]:
            copy.start()

    @pl.when(serves[0] == 1)
    def _():
        for copy in held:
            copy.start()

    @pl.when(serves[0] != 1)
    def _():
        for i in range(3):
            for copies in forwarded:
                copies[i].start()

    for copies in received:
        copies[2].start()

    total = jnp.zeros((rows, 1), jnp.float32)
    for k in range(pairs):
        block = gathered[k].astype(jnp.float32)
        total = total + jnp.sum(block * block, axis=-1, keepdims=True)
    inverse = lax.rsqrt(total * (1.0 / width) + EPS)
    for k in range(pairs):
        block = gathered[k].astype(jnp.float32)
        scaled = block * inverse * gain[:, k * piece : (k + 1) * piece]
        normed[:, k * piece : (k + 1) * piece] = scaled.astype(jnp.bfloat16)
    for t in range(members):
        out[t, each * tiles :, :] = own[t * 16 : (t + 1) * 16, :]
    contract = (((1,), (1,)), ((), ()))
    hidden = []
    arrived = 0
    for start in range(0, 4 * half, 256):
        size = 256
        while arrived < 6 and arrived * part < start + size:
            for copy in received[arrived][:2]:
                copy.wait()
            arrived += 1
        if arrived == 6 and start + size > 6 * part:
            for copy in held[:2]:
                copy.wait()
            arrived += 1
        g = lax.dot_general(
            normed[...], gate[pl.ds(start, size), :], contract, preferred_element_type=jnp.float32
        )
        u = lax.dot_general(
            normed[...], up[pl.ds(start, size), :], contract, preferred_element_type=jnp.float32
        )
        hidden.append((g / (1.0 + jnp.exp(-g)) * u).astype(jnp.bfloat16))
    hidden = jnp.concatenate(hidden, axis=1)
    for copy in (*(copies[2] for copies in received), held[2]):
        copy.wait()
    for chunk in range(width // 256):
        share = jnp.dot(
            hidden, down[:, pl.ds(chunk * 256, 256)], preferred_element_type=jnp.float32
        ).astype(jnp.bfloat16)
        for t in range(members):
            for side in range(2):
                tile = chunk * 2 + side
                out[t, tile * each : (tile + 1) * each, :] = share[
                    t * each : (t + 1) * each, side * 128 : (side + 1) * 128
                ]


def run_expert(serves, gathered, own, norm_gain, owned, moved):
    pairs, rows, _ = gathered.shape
    half, width = owned[0].shape
    members = pairs
    return pl.pallas_call(
        expert_kernel,
        out_shape=jax.ShapeDtypeStruct(
            (members, rows // members * (width // 128) + 16, 128), jnp.bfloat16
        ),
        in_specs=[SMEM, VMEM, VMEM, VMEM] + [ANYWHERE] * 11,
        out_specs=VMEM,
        scratch_shapes=[pltpu.VMEM((4 * half, width), jnp.bfloat16) for _ in range(3)]
        + [pltpu.VMEM((rows, width), jnp.bfloat16), pltpu.SemaphoreType.DMA((21,))],
        cost_estimate=pl.CostEstimate(
            flops=24 * rows * half * width,
            bytes_accessed=24 * half * width + 4 * rows * width,
            transcendentals=2 * rows * half,
        ),
        compiler_params=pltpu.CompilerParams(vmem_limit_bytes=28 * 2**20),
        name="expert",
    )(serves, gathered, own, norm_gain.reshape(1, -1), *in_hbm(owned), *in_hbm(moved))


def sum_kernel(shares, out, acc):
    members, rows, lanes = shares.shape
    planes = out.shape[0]
    tiles = (rows - 16) // planes
    for side in range(2):
        for rank in range(2):
            total = jnp.zeros((rows - 16, lanes), jnp.float32)
            for t in range(members):
                if served_side(t) == side and served_rank(t) == rank:
                    total = total + shares[t, pl.ds(0, rows - 16), :].astype(jnp.float32)
            acc[...] = total
            for plane in range(planes):
                rows_of = acc[pl.ds(plane, tiles, stride=planes), :]
                at = (side * 2 + rank) * tiles
                out[plane, at : at + tiles, :] = rows_of.astype(jnp.bfloat16)


def sum_shares(shares, planes):
    members, rows, lanes = shares.shape
    tiles = (rows - 16) // planes
    return pl.pallas_call(
        sum_kernel,
        out_shape=jax.ShapeDtypeStruct((planes, 4 * tiles, lanes), jnp.bfloat16),
        in_specs=[VMEM],
        out_specs=VMEM,
        scratch_shapes=[pltpu.VMEM((rows - 16, lanes), jnp.float32)],
        cost_estimate=pl.CostEstimate(
            flops=members * rows * lanes, bytes_accessed=2 * members * rows * lanes, transcendentals=0
        ),
        compiler_params=pltpu.CompilerParams(vmem_limit_bytes=8 * 2**20),
        name="shares",
    )(shares)


def local(
    queries,
    keys,
    values,
    sink_logit,
    out_weight,
    residual,
    norm_gain,
    routes,
    route_weights,
    gate_weight,
    up_weight,
    down_weight,
):
    n_sp, n_tp = lax.axis_size("sp"), lax.axis_size("tp")
    planes = n_sp // 2
    tok_rows, width = residual.shape
    length = queries.shape[0]
    same_core = [[plane * 2 + core for plane in range(planes)] for core in range(2)]

    steps = ((0, 1), (0, 3), (1, 0), (3, 0))
    diagonal = ((1, 1), (3, 3))
    moves, passes = [[] for _ in steps], [[] for _ in steps]
    for plane in range(planes):
        for core in range(2):
            for member in range(n_tp):
                base = (plane * 2 + core) * n_tp
                across = (plane * 2 + 1 - core) * n_tp
                y, x = member // 4, member % 4
                right = served_side(member) == core
                for k, (dy, dx) in enumerate(steps):
                    if right and k < 2:
                        dy, dx = diagonal[k]
                        target = across + (y + dy) % 4 * 4 + (x + dx) % 4
                    elif right:
                        target = across + member
                    else:
                        target = base + (y + dy) % 4 * 4 + (x + dx) % 4
                    moves[k].append((base + member, target))
                    if right or k < 2:
                        passes[k].append((base + member, across + member))
    core_index = lax.axis_index("sp") % 2
    serves = (core_index == served_side(lax.axis_index("tp"))).astype(jnp.int32).reshape(1)
    owned = (gate_weight[0].T, up_weight[0].T, down_weight[0])
    received, forwarded = [], []
    packed = pack(owned, 2)
    for k, way in enumerate(moves):
        received.append(lax.ppermute(packed[k % 2], ("sp", "tp"), way))
        forwarded.append(lax.ppermute(received[-1], ("sp", "tp"), passes[k]))

    low, high, joined, asked, base, sinks, slot_rows = prepare(
        keys.T, values.T, queries, residual, sink_logit.reshape(1, -1), routes.T
    )
    forward = [(i, i + 1) for i in range(n_sp - 1)]
    backward = [(i + 1, i) for i in range(n_sp - 1)]
    low = lax.ppermute(low, "sp", forward)
    high = lax.ppermute(high, "sp", backward)
    where = jnp.stack([lax.axis_index("sp"), jnp.int32(n_sp)]).astype(jnp.int32)
    message = run_attention(where, sinks, asked, low, joined, high, base, slot_rows, n_tp)

    arrived = exchange(message, "tp")
    own, sending = project(arrived, out_weight, planes, length)

    dispatched = exchange(sending, "sp", same_core)
    to_servers = spread(dispatched, n_tp)
    gathered = exchange(to_servers, "tp")
    pieces = run_expert(serves, gathered, own, norm_gain, owned, (*received, *forwarded))

    shares = exchange(pieces, "tp")
    own_rows = shares[:, n_tp * planes :].transpose(1, 0, 2).reshape(tok_rows, width)
    returning = sum_shares(shares, planes)

    returned = exchange(returning, "sp", same_core)
    returned = returned.reshape(planes * 4, width)
    slots = slot_rows[:, :2].astype(jnp.int32)
    place = (slots[:, :, None] == jnp.arange(2 * n_sp)[None, None, :]).astype(jnp.bfloat16)
    first = jnp.dot(place[:, 0], returned, preferred_element_type=jnp.float32)
    second = jnp.dot(place[:, 1], returned, preferred_element_type=jnp.float32)
    mixture = route_weights[:, 0:1] * first + route_weights[:, 1:2] * second
    hidden_state = residual.astype(jnp.float32) + own_rows.astype(jnp.float32)
    return (hidden_state + mixture).astype(jnp.bfloat16)


def solution(mesh):
    in_specs = (
        P("sp", "tp"),
        P("sp", "tp"),
        P("sp", "tp"),
        P("tp"),
        P(None, "tp"),
        P(("sp", "tp"), None),
        P(),
        P(("sp", "tp"), None),
        P(("sp", "tp"), None),
        P("sp", None, "tp"),
        P("sp", None, "tp"),
        P("sp", "tp", None),
    )
    out_specs = P(("sp", "tp"), None)

    return jax.shard_map(local, mesh=mesh, in_specs=in_specs, out_specs=out_specs, check_vma=False)
```

```python
import jax
import jax.numpy as jnp
from jax import lax
from jax.experimental import pallas as pl
from jax.experimental.pallas import tpu as pltpu
from jax.sharding import PartitionSpec as P


HEAD = 64
WINDOW = 128

EPS = 1e-06
NEGATIVE = -1e30


VMEM = pl.BlockSpec(memory_space=pltpu.VMEM)
SMEM = pl.BlockSpec(memory_space=pltpu.SMEM)
ANYWHERE = pl.BlockSpec(memory_space=pltpu.HBM)


def in_hbm(values):
    return [pltpu.with_memory_space_constraint(value, pltpu.HBM) for value in values]


def served_side(member):
    return (member + member // 4) % 2


def served_rank(member):
    return member // 4 % 2


def prep_kernel(
    keys, values, queries, residual, sink, routes, low, high, own, asked, base, sinks, slots,
    named, sems,
):
    head, length = keys.shape
    copies = [
        pltpu.make_async_copy(source, target, sems.at[i])
        for i, (source, target) in enumerate(
            (
                (keys, own.at[pl.ds(0, head)]),
                (values, own.at[pl.ds(head, head)]),
                (queries, asked),
                (residual, base),
                (sink, sinks),
                (routes, named),
            )
        )
    ]
    for copy in copies:
        copy.start()
    for copy in copies:
        copy.wait()
    low[...] = own[:, length - WINDOW :]
    high[...] = own[:, :WINDOW]
    ways, count = named.shape
    flat = named[...].astype(jnp.float32)
    row = lax.broadcasted_iota(jnp.int32, (count, count), 0)
    col = lax.broadcasted_iota(jnp.int32, (count, count), 1)
    eye = jnp.where(row == col, 1.0, 0.0)
    upright = lax.dot_general(
        eye, flat, (((1,), (1,)), ((), ())), preferred_element_type=jnp.float32
    )
    lane = lax.broadcasted_iota(jnp.int32, slots.shape, 1)
    result = jnp.zeros(slots.shape, jnp.float32)
    for way in range(ways):
        mine = upright[:, way : way + 1]
        rank = jnp.zeros((count, 1), jnp.float32)
        for other in range(ways):
            same = (flat[other : other + 1, :] == mine) & (col < row)
            rank = rank + jnp.sum(jnp.where(same, 1.0, 0.0), axis=1, keepdims=True)
        result = jnp.where(lane == way, mine * 2.0 + rank, result)
    slots[...] = result.astype(jnp.bfloat16)


def prepare(keys, values, queries, residual, sink, routes):
    head, length = keys.shape
    tok_rows = residual.shape[0]
    bf16 = jnp.bfloat16
    return pl.pallas_call(
        prep_kernel,
        out_shape=(
            jax.ShapeDtypeStruct((2 * head, WINDOW), bf16),
            jax.ShapeDtypeStruct((2 * head, WINDOW), bf16),
            jax.ShapeDtypeStruct((2 * head, length), bf16),
            jax.ShapeDtypeStruct(queries.shape, bf16),
            jax.ShapeDtypeStruct(residual.shape, bf16),
            jax.ShapeDtypeStruct(sink.shape, jnp.float32),
            jax.ShapeDtypeStruct((tok_rows, 128), bf16),
        ),
        in_specs=[ANYWHERE] * 6,
        out_specs=(VMEM,) * 7,
        scratch_shapes=[pltpu.VMEM(routes.shape, jnp.int32), pltpu.SemaphoreType.DMA((6,))],
        compiler_params=pltpu.CompilerParams(vmem_limit_bytes=4 * 2**20),
        name="prepare",
    )(*in_hbm((keys, values, queries, residual, sink, routes)))


def attend_kernel(place, sink, queries, low, own, high, residual, slots, out):
    members = out.shape[0]
    length, both = queries.shape
    tok_rows = residual.shape[0]
    total = place[1] * length
    band = jnp.concatenate([low[...], own[...], high[...]], axis=1)
    row = lax.broadcasted_iota(jnp.int32, (WINDOW, 3 * WINDOW), 0)
    col = lax.broadcasted_iota(jnp.int32, (WINDOW, 3 * WINDOW), 1)
    near = jnp.abs(row + WINDOW - col) <= WINDOW
    for block in range(length // WINDOW):
        position = place[0] * length + (block - 1) * WINDOW + col
        valid = near & (position >= 0) & (position < total)
        keys = band[:HEAD, block * WINDOW : (block + 3) * WINDOW]
        values = band[HEAD:, block * WINDOW : (block + 3) * WINDOW]
        heads = []
        for head in range(both // HEAD):
            asked = queries[block * WINDOW : (block + 1) * WINDOW, head * HEAD : (head + 1) * HEAD]
            scores = jnp.dot(asked, keys, preferred_element_type=jnp.float32) * HEAD ** (-0.5)
            masked = jnp.where(valid, scores, NEGATIVE)
            bound = sink[:, head : head + 1]
            top = jnp.maximum(jnp.max(masked, axis=-1, keepdims=True), bound)
            probs = jnp.exp(masked - top)
            denom = jnp.sum(probs, axis=-1, keepdims=True) + jnp.exp(bound - top)
            weights = (probs / denom).astype(jnp.bfloat16)
            heads.append(
                lax.dot_general(
                    weights, values, (((1,), (1,)), ((), ())), preferred_element_type=jnp.float32
                )
            )
        attended = jnp.concatenate(heads, axis=1).astype(jnp.bfloat16)
        for t in range(members):
            out[t, block * WINDOW : (block + 1) * WINDOW, :] = attended
    for t in range(members):
        out[t, length : length + tok_rows, :] = residual[:, t * 128 : (t + 1) * 128]
        out[t, length + tok_rows :, :] = slots[...]


def run_attention(place, sink, queries, low, own, high, residual, slots, members):
    length, both = queries.shape
    tok_rows = residual.shape[0]
    return pl.pallas_call(
        attend_kernel,
        out_shape=jax.ShapeDtypeStruct((members, length + 2 * tok_rows, 128), jnp.bfloat16),
        in_specs=[SMEM] + [VMEM] * 7,
        out_specs=VMEM,
        cost_estimate=pl.CostEstimate(
            flops=4 * length * both * 3 * WINDOW,
            bytes_accessed=4 * members * length * 128,
            transcendentals=6 * length * WINDOW,
        ),
        compiler_params=pltpu.CompilerParams(vmem_limit_bytes=10 * 2**20),
        name="attend",
    )(place, sink, queries, low, own, high, residual, slots)


def project_kernel(arrived, weight, projected, sending):
    members = arrived.shape[0]
    length = projected.shape[0]
    tok_rows = length // members
    planes, per_plane, lanes = sending.shape
    total = jnp.zeros((length, lanes), jnp.float32)
    for k in range(members // 2):
        part = jnp.concatenate(
            [arrived[2 * k, :length, :], arrived[2 * k + 1, :length, :]], axis=1
        )
        total = total + jnp.dot(
            part, weight[k * 256 : (k + 1) * 256, :], preferred_element_type=jnp.float32
        )
    rounded = total.astype(jnp.bfloat16)
    projected[...] = rounded
    base = jnp.concatenate(
        [arrived[t, length : length + tok_rows, :] for t in range(members)], axis=0
    )
    hidden = (base.astype(jnp.float32) + rounded.astype(jnp.float32)).astype(jnp.bfloat16)
    slots = jnp.concatenate([arrived[t, length + tok_rows :, :] for t in range(members)], axis=0)
    slots = slots.astype(jnp.float32)
    lines = planes * per_plane
    place = lax.broadcasted_iota(jnp.int32, (1, lines), 1)
    named = place // per_plane * 4 + place // (per_plane // 2) % 2 * 2 + place % 2
    wanted = (named + place // 2 % members * (4 * planes)).astype(jnp.float32)
    device = lax.broadcasted_iota(jnp.int32, (length, 1), 0) // tok_rows * (4 * planes)
    device = device.astype(jnp.float32)
    taken = (slots[:, 0:1] + device == wanted) | (slots[:, 1:2] + device == wanted)
    placing = jnp.where(taken, 1.0, 0.0).astype(jnp.bfloat16)
    rows = lax.dot_general(
        placing, hidden, (((0,), (0,)), ((), ())), preferred_element_type=jnp.float32
    ).astype(jnp.bfloat16)
    for plane in range(planes):
        sending[plane] = rows[plane * per_plane : (plane + 1) * per_plane, :]


def project(arrived, weight, planes, length):
    members = arrived.shape[0]
    width, lanes = weight.shape
    return pl.pallas_call(
        project_kernel,
        out_shape=(
            jax.ShapeDtypeStruct((length, lanes), jnp.bfloat16),
            jax.ShapeDtypeStruct((planes, 4 * members, lanes), jnp.bfloat16),
        ),
        in_specs=[VMEM, VMEM],
        out_specs=(VMEM, VMEM),
        cost_estimate=pl.CostEstimate(
            flops=2 * length * width * lanes,
            bytes_accessed=4 * width * lanes + 2 * members * length * lanes,
            transcendentals=0,
        ),
        compiler_params=pltpu.CompilerParams(vmem_limit_bytes=12 * 2**20),
        name="project",
    )(arrived, weight)


def spread_kernel(dispatched, out, rows, block, sems):
    planes, lines, _ = dispatched.shape
    members = out.shape[0]
    for plane in range(planes):
        rows[plane * lines : (plane + 1) * lines, :] = dispatched[plane].astype(jnp.float32)
    copies = [
        pltpu.make_async_copy(
            block.at[served_side(t) * 2 + served_rank(t)], out.at[t], sems.at[t]
        )
        for t in range(members)
    ]
    for side in range(2):
        for at in range(lines // 2):
            group = rows[pl.ds(side * (lines // 2) + at, planes, stride=lines), :]
            token, rank = at // 2, at % 2
            block[side * 2 + rank, token * planes : (token + 1) * planes, :] = group.astype(
                jnp.bfloat16
            )
        for t in range(members):
            if served_side(t) == side:
                copies[t].start()
    for copy in copies:
        copy.wait()


def spread(dispatched, members):
    planes, lines, lanes = dispatched.shape
    return pl.pallas_call(
        spread_kernel,
        out_shape=pltpu.HBM((members, planes * lines // 4, lanes), jnp.bfloat16),
        in_specs=[VMEM],
        out_specs=ANYWHERE,
        scratch_shapes=[
            pltpu.VMEM((planes * lines, lanes), jnp.float32),
            pltpu.VMEM((4, planes * lines // 4, lanes), jnp.bfloat16),
            pltpu.SemaphoreType.DMA((members,)),
        ],
        cost_estimate=pl.CostEstimate(
            flops=planes * lines * lanes,
            bytes_accessed=members * planes * lines * lanes,
            transcendentals=0,
        ),
        compiler_params=pltpu.CompilerParams(vmem_limit_bytes=8 * 2**20),
        name="spread",
    )(dispatched)


def exchange(value, axis, groups=None):
    return lax.all_to_all(
        value, axis, split_axis=0, concat_axis=0, tiled=True, axis_index_groups=groups
    )


def pack_kernel(gate, up, down, first, second, held, sems):
    half = gate.shape[0]
    part = half // 2
    sources, outs = (gate, up, down), (first, second)
    loads = [
        pltpu.make_async_copy(source, held.at[i], sems.at[i]) for i, source in enumerate(sources)
    ]
    for copy in loads:
        copy.start()
    stores = []
    for i, copy in enumerate(loads):
        copy.wait()
        for k, out in enumerate(outs):
            stores.append(
                pltpu.make_async_copy(
                    held.at[i, pl.ds(k * part, part)],
                    out.at[pl.ds(i * part, part)],
                    sems.at[3 + 2 * i + k],
                )
            )
            stores[-1].start()
    for copy in stores:
        copy.wait()


def pack(owned):
    half, width = owned[0].shape
    return pl.pallas_call(
        pack_kernel,
        out_shape=tuple(pltpu.HBM((3 * half // 2, width), jnp.bfloat16) for _ in range(2)),
        in_specs=[ANYWHERE] * 3,
        out_specs=(ANYWHERE,) * 2,
        scratch_shapes=[
            pltpu.VMEM((3, half, width), jnp.bfloat16), pltpu.SemaphoreType.DMA((9,)),
        ],
        cost_estimate=pl.CostEstimate(
            flops=half * width, bytes_accessed=12 * half * width, transcendentals=0
        ),
        compiler_params=pltpu.CompilerParams(vmem_limit_bytes=8 * 2**20),
        name="pack",
    )(*in_hbm(owned))


def expert_kernel(
    serves, gathered, own, gain, gate_own, up_own, down_own,
    got_0, got_1, got_2, got_3, fwd_0, fwd_1, fwd_2, fwd_3,
    out, gate, up, down, normed, sems,
):
    half, width = gate_own.shape
    part = half // 2
    pairs, rows, piece = gathered.shape
    members = out.shape[0]
    each = rows // members
    tiles = width // 128
    targets = (gate, up, down)

    def placed(packed, start, base):
        return [
            pltpu.make_async_copy(
                packed.at[pl.ds(i * part, part)], target.at[pl.ds(start, part)], sems.at[base + i]
            )
            for i, target in enumerate(targets)
        ]

    received = [
        placed(packed, k * part, 3 * k) for k, packed in enumerate((got_0, got_1, got_2, got_3))
    ]
    received += [placed(fwd_0, 4 * part, 12), placed(fwd_1, 5 * part, 15)]
    forwarded = [placed(fwd_2, 6 * part, 18), placed(fwd_3, 7 * part, 18)]
    held = [
        pltpu.make_async_copy(source, target.at[pl.ds(3 * half, half)], sems.at[18 + i])
        for i, (source, target) in enumerate(zip((gate_own, up_own, down_own), targets))
    ]
    for copies in received:
        for copy in copies[:2]:
            copy.start()

    @pl.when(serves[0] == 1)
    def _():
        for copy in held:
            copy.start()

    @pl.when(serves[0] != 1)
    def _():
        for i in range(3):
            for copies in forwarded:
                copies[i].start()

    for copies in received:
        copies[2].start()

    total = jnp.zeros((rows, 1), jnp.float32)
    for k in range(pairs):
        block = gathered[k].astype(jnp.float32)
        total = total + jnp.sum(block * block, axis=-1, keepdims=True)
    inverse = lax.rsqrt(total * (1.0 / width) + EPS)
    for k in range(pairs):
        block = gathered[k].astype(jnp.float32)
        scaled = block * inverse * gain[:, k * piece : (k + 1) * piece]
        normed[:, k * piece : (k + 1) * piece] = scaled.astype(jnp.bfloat16)
    for t in range(members):
        out[t, each * tiles :, :] = own[t * 16 : (t + 1) * 16, :]
    contract = (((1,), (1,)), ((), ()))
    hidden = []
    arrived = 0
    for start in range(0, 4 * half, 256):
        size = 256
        while arrived < 6 and arrived * part < start + size:
            for copy in received[arrived][:2]:
                copy.wait()
            arrived += 1
        if arrived == 6 and start + size > 6 * part:
            for copy in held[:2]:
                copy.wait()
            arrived += 1
        g = lax.dot_general(
            normed[...], gate[pl.ds(start, size), :], contract, preferred_element_type=jnp.float32
        )
        u = lax.dot_general(
            normed[...], up[pl.ds(start, size), :], contract, preferred_element_type=jnp.float32
        )
        hidden.append((g / (1.0 + jnp.exp(-g)) * u).astype(jnp.bfloat16))
    hidden = jnp.concatenate(hidden, axis=1)
    for copy in (*(copies[2] for copies in received), held[2]):
        copy.wait()
    for chunk in range(width // 256):
        share = jnp.dot(
            hidden, down[:, pl.ds(chunk * 256, 256)], preferred_element_type=jnp.float32
        ).astype(jnp.bfloat16)
        for t in range(members):
            for side in range(2):
                tile = chunk * 2 + side
                out[t, tile * each : (tile + 1) * each, :] = share[
                    t * each : (t + 1) * each, side * 128 : (side + 1) * 128
                ]


def run_expert(serves, gathered, own, norm_gain, owned, moved):
    pairs, rows, _ = gathered.shape
    half, width = owned[0].shape
    members = pairs
    return pl.pallas_call(
        expert_kernel,
        out_shape=jax.ShapeDtypeStruct(
            (members, rows // members * (width // 128) + 16, 128), jnp.bfloat16
        ),
        in_specs=[SMEM, VMEM, VMEM, VMEM] + [ANYWHERE] * 11,
        out_specs=VMEM,
        scratch_shapes=[pltpu.VMEM((4 * half, width), jnp.bfloat16) for _ in range(3)]
        + [pltpu.VMEM((rows, width), jnp.bfloat16), pltpu.SemaphoreType.DMA((21,))],
        cost_estimate=pl.CostEstimate(
            flops=24 * rows * half * width,
            bytes_accessed=24 * half * width + 4 * rows * width,
            transcendentals=2 * rows * half,
        ),
        compiler_params=pltpu.CompilerParams(vmem_limit_bytes=28 * 2**20),
        name="expert",
    )(serves, gathered, own, norm_gain.reshape(1, -1), *in_hbm(owned), *in_hbm(moved))


def sum_kernel(shares, out, acc):
    members, rows, lanes = shares.shape
    planes = out.shape[0]
    tiles = (rows - 16) // planes
    for side in range(2):
        for rank in range(2):
            total = jnp.zeros((rows - 16, lanes), jnp.float32)
            for t in range(members):
                if served_side(t) == side and served_rank(t) == rank:
                    total = total + shares[t, pl.ds(0, rows - 16), :].astype(jnp.float32)
            acc[...] = total
            for plane in range(planes):
                rows_of = acc[pl.ds(plane, tiles, stride=planes), :]
                at = (side * 2 + rank) * tiles
                out[plane, at : at + tiles, :] = rows_of.astype(jnp.bfloat16)


def sum_shares(shares, planes):
    members, rows, lanes = shares.shape
    tiles = (rows - 16) // planes
    return pl.pallas_call(
        sum_kernel,
        out_shape=jax.ShapeDtypeStruct((planes, 4 * tiles, lanes), jnp.bfloat16),
        in_specs=[VMEM],
        out_specs=VMEM,
        scratch_shapes=[pltpu.VMEM((rows - 16, lanes), jnp.float32)],
        cost_estimate=pl.CostEstimate(
            flops=members * rows * lanes, bytes_accessed=2 * members * rows * lanes, transcendentals=0
        ),
        compiler_params=pltpu.CompilerParams(vmem_limit_bytes=8 * 2**20),
        name="shares",
    )(shares)


def local(
    queries,
    keys,
    values,
    sink_logit,
    out_weight,
    residual,
    norm_gain,
    routes,
    route_weights,
    gate_weight,
    up_weight,
    down_weight,
):
    n_sp, n_tp = lax.axis_size("sp"), lax.axis_size("tp")
    planes = n_sp // 2
    tok_rows, width = residual.shape
    length = queries.shape[0]
    same_core = [[plane * 2 + core for plane in range(planes)] for core in range(2)]

    steps = ((0, 1), (0, 3), (1, 0), (3, 0))
    diagonal = ((1, 1), (3, 3))
    moves, passes = [[] for _ in steps], [[] for _ in steps]
    for plane in range(planes):
        for core in range(2):
            for member in range(n_tp):
                base = (plane * 2 + core) * n_tp
                across = (plane * 2 + 1 - core) * n_tp
                y, x = member // 4, member % 4
                right = served_side(member) == core
                for k, (dy, dx) in enumerate(steps):
                    if right and k < 2:
                        dy, dx = diagonal[k]
                        target = across + (y + dy) % 4 * 4 + (x + dx) % 4
                    elif right:
                        target = across + member
                    else:
                        target = base + (y + dy) % 4 * 4 + (x + dx) % 4
                    moves[k].append((base + member, target))
                    if right or k < 2:
                        passes[k].append((base + member, across + member))
    core_index = lax.axis_index("sp") % 2
    serves = (core_index == served_side(lax.axis_index("tp"))).astype(jnp.int32).reshape(1)
    owned = (gate_weight[0].T, up_weight[0].T, down_weight[0])
    received, forwarded = [], []
    packed = pack(owned)
    for k, way in enumerate(moves):
        received.append(lax.ppermute(packed[k % 2], ("sp", "tp"), way))
        forwarded.append(lax.ppermute(received[-1], ("sp", "tp"), passes[k]))

    low, high, joined, asked, base, sinks, slot_rows = prepare(
        keys.T, values.T, queries, residual, sink_logit.reshape(1, -1), routes.T
    )
    forward = [(i, i + 1) for i in range(n_sp - 1)]
    backward = [(i + 1, i) for i in range(n_sp - 1)]
    low = lax.ppermute(low, "sp", forward)
    high = lax.ppermute(high, "sp", backward)
    where = jnp.stack([lax.axis_index("sp"), jnp.int32(n_sp)]).astype(jnp.int32)
    message = run_attention(where, sinks, asked, low, joined, high, base, slot_rows, n_tp)

    arrived = exchange(message, "tp")
    own, sending = project(arrived, out_weight, planes, length)

    dispatched = exchange(sending, "sp", same_core)
    to_servers = spread(dispatched, n_tp)
    gathered = exchange(to_servers, "tp")
    pieces = run_expert(serves, gathered, own, norm_gain, owned, (*received, *forwarded))

    shares = exchange(pieces, "tp")
    own_rows = shares[:, n_tp * planes :].transpose(1, 0, 2).reshape(tok_rows, width)
    returning = sum_shares(shares, planes)

    returned = exchange(returning, "sp", same_core)
    returned = returned.reshape(planes * 4, width)
    slots = slot_rows[:, :2].astype(jnp.int32)
    place = (slots[:, :, None] == jnp.arange(2 * n_sp)[None, None, :]).astype(jnp.bfloat16)
    first = jnp.dot(place[:, 0], returned, preferred_element_type=jnp.float32)
    second = jnp.dot(place[:, 1], returned, preferred_element_type=jnp.float32)
    mixture = route_weights[:, 0:1] * first + route_weights[:, 1:2] * second
    hidden_state = residual.astype(jnp.float32) + own_rows.astype(jnp.float32)
    return (hidden_state + mixture).astype(jnp.bfloat16)


def solution(mesh):
    in_specs = (
        P("sp", "tp"),
        P("sp", "tp"),
        P("sp", "tp"),
        P("tp"),
        P(None, "tp"),
        P(("sp", "tp"), None),
        P(),
        P(("sp", "tp"), None),
        P(("sp", "tp"), None),
        P("sp", None, "tp"),
        P("sp", None, "tp"),
        P("sp", "tp", None),
    )
    out_specs = P(("sp", "tp"), None)

    return jax.shard_map(local, mesh=mesh, in_specs=in_specs, out_specs=out_specs, check_vma=False)
```

```python
import jax
import jax.numpy as jnp
from jax import lax
from jax.experimental import pallas as pl
from jax.experimental.pallas import tpu as pltpu
from jax.sharding import PartitionSpec as P


HEAD = 64
WINDOW = 128

EPS = 1e-06
NEGATIVE = -1e30


VMEM = pl.BlockSpec(memory_space=pltpu.VMEM)
SMEM = pl.BlockSpec(memory_space=pltpu.SMEM)
ANYWHERE = pl.BlockSpec(memory_space=pltpu.HBM)


def in_hbm(values):
    return [pltpu.with_memory_space_constraint(value, pltpu.HBM) for value in values]


def served_side(member):
    return (member + member // 4) % 2


def served_rank(member):
    return member // 4 % 2


def prep_kernel(
    keys, values, queries, residual, sink, routes, low, high, own, asked, base, sinks, slots,
    named, sems,
):
    head, length = keys.shape
    copies = [
        pltpu.make_async_copy(source, target, sems.at[i])
        for i, (source, target) in enumerate(
            (
                (keys, own.at[pl.ds(0, head)]),
                (values, own.at[pl.ds(head, head)]),
                (queries, asked),
                (residual, base),
                (sink, sinks),
                (routes, named),
            )
        )
    ]
    for copy in copies:
        copy.start()
    for copy in copies:
        copy.wait()
    low[...] = own[:, length - WINDOW :]
    high[...] = own[:, :WINDOW]
    ways, count = named.shape
    flat = named[...].astype(jnp.float32)
    row = lax.broadcasted_iota(jnp.int32, (count, count), 0)
    col = lax.broadcasted_iota(jnp.int32, (count, count), 1)
    eye = jnp.where(row == col, 1.0, 0.0)
    upright = lax.dot_general(
        eye, flat, (((1,), (1,)), ((), ())), preferred_element_type=jnp.float32
    )
    lane = lax.broadcasted_iota(jnp.int32, slots.shape, 1)
    result = jnp.zeros(slots.shape, jnp.float32)
    for way in range(ways):
        mine = upright[:, way : way + 1]
        rank = jnp.zeros((count, 1), jnp.float32)
        for other in range(ways):
            same = (flat[other : other + 1, :] == mine) & (col < row)
            rank = rank + jnp.sum(jnp.where(same, 1.0, 0.0), axis=1, keepdims=True)
        result = jnp.where(lane == way, mine * 2.0 + rank, result)
    slots[...] = result.astype(jnp.bfloat16)


def prepare(keys, values, queries, residual, sink, routes):
    head, length = keys.shape
    tok_rows = residual.shape[0]
    bf16 = jnp.bfloat16
    return pl.pallas_call(
        prep_kernel,
        out_shape=(
            jax.ShapeDtypeStruct((2 * head, WINDOW), bf16),
            jax.ShapeDtypeStruct((2 * head, WINDOW), bf16),
            jax.ShapeDtypeStruct((2 * head, length), bf16),
            jax.ShapeDtypeStruct(queries.shape, bf16),
            jax.ShapeDtypeStruct(residual.shape, bf16),
            jax.ShapeDtypeStruct(sink.shape, jnp.float32),
            jax.ShapeDtypeStruct((tok_rows, 128), bf16),
        ),
        in_specs=[ANYWHERE] * 6,
        out_specs=(VMEM,) * 7,
        scratch_shapes=[pltpu.VMEM(routes.shape, jnp.int32), pltpu.SemaphoreType.DMA((6,))],
        compiler_params=pltpu.CompilerParams(vmem_limit_bytes=4 * 2**20),
        name="prepare",
    )(*in_hbm((keys, values, queries, residual, sink, routes)))


def attend_kernel(place, sink, queries, low, own, high, residual, slots, out, held, rest, sems):
    members = out.shape[0]
    length, both = queries.shape
    tok_rows = residual.shape[0]
    total = place[1] * length
    copies = []

    def send(source, t, start, size):
        copies.append(
            pltpu.make_async_copy(
                source, out.at[t, pl.ds(start, size)], sems.at[len(copies)]
            )
        )
        copies[-1].start()

    for t in range(members):
        rest[t, :tok_rows, :] = residual[:, t * 128 : (t + 1) * 128]
        rest[t, tok_rows:, :] = slots[...]
    for t in range(members):
        send(rest.at[t], t, length, 2 * tok_rows)
    band = jnp.concatenate([low[...], own[...], high[...]], axis=1)
    row = lax.broadcasted_iota(jnp.int32, (WINDOW, 3 * WINDOW), 0)
    col = lax.broadcasted_iota(jnp.int32, (WINDOW, 3 * WINDOW), 1)
    near = jnp.abs(row + WINDOW - col) <= WINDOW
    for block in range(length // WINDOW):
        position = place[0] * length + (block - 1) * WINDOW + col
        valid = near & (position >= 0) & (position < total)
        keys = band[:HEAD, block * WINDOW : (block + 3) * WINDOW]
        values = band[HEAD:, block * WINDOW : (block + 3) * WINDOW]
        heads = []
        for head in range(both // HEAD):
            asked = queries[block * WINDOW : (block + 1) * WINDOW, head * HEAD : (head + 1) * HEAD]
            scores = jnp.dot(asked, keys, preferred_element_type=jnp.float32) * HEAD ** (-0.5)
            masked = jnp.where(valid, scores, NEGATIVE)
            bound = sink[:, head : head + 1]
            top = jnp.maximum(jnp.max(masked, axis=-1, keepdims=True), bound)
            probs = jnp.exp(masked - top)
            denom = jnp.sum(probs, axis=-1, keepdims=True) + jnp.exp(bound - top)
            weights = (probs / denom).astype(jnp.bfloat16)
            heads.append(
                lax.dot_general(
                    weights, values, (((1,), (1,)), ((), ())), preferred_element_type=jnp.float32
                )
            )
        attended = jnp.concatenate(heads, axis=1).astype(jnp.bfloat16)
        held[block * WINDOW : (block + 1) * WINDOW, :] = attended
        for t in range(members):
            send(held.at[pl.ds(block * WINDOW, WINDOW)], t, block * WINDOW, WINDOW)
    for copy in copies:
        copy.wait()


def run_attention(place, sink, queries, low, own, high, residual, slots, members):
    length, both = queries.shape
    tok_rows = residual.shape[0]
    return pl.pallas_call(
        attend_kernel,
        out_shape=pltpu.HBM((members, length + 2 * tok_rows, 128), jnp.bfloat16),
        in_specs=[SMEM] + [VMEM] * 7,
        out_specs=ANYWHERE,
        scratch_shapes=[
            pltpu.VMEM((length, 128), jnp.bfloat16),
            pltpu.VMEM((members, 2 * tok_rows, 128), jnp.bfloat16),
            pltpu.SemaphoreType.DMA((members * (1 + length // WINDOW),)),
        ],
        cost_estimate=pl.CostEstimate(
            flops=4 * length * both * 3 * WINDOW,
            bytes_accessed=4 * members * length * 128,
            transcendentals=6 * length * WINDOW,
        ),
        compiler_params=pltpu.CompilerParams(vmem_limit_bytes=10 * 2**20),
        name="attend",
    )(place, sink, queries, low, own, high, residual, slots)


def project_kernel(arrived, weight, projected, sending):
    members = arrived.shape[0]
    length = projected.shape[0]
    tok_rows = length // members
    planes, per_plane, lanes = sending.shape
    total = jnp.zeros((length, lanes), jnp.float32)
    for k in range(members // 2):
        part = jnp.concatenate(
            [arrived[2 * k, :length, :], arrived[2 * k + 1, :length, :]], axis=1
        )
        total = total + jnp.dot(
            part, weight[k * 256 : (k + 1) * 256, :], preferred_element_type=jnp.float32
        )
    rounded = total.astype(jnp.bfloat16)
    projected[...] = rounded
    base = jnp.concatenate(
        [arrived[t, length : length + tok_rows, :] for t in range(members)], axis=0
    )
    hidden = (base.astype(jnp.float32) + rounded.astype(jnp.float32)).astype(jnp.bfloat16)
    slots = jnp.concatenate([arrived[t, length + tok_rows :, :] for t in range(members)], axis=0)
    slots = slots.astype(jnp.float32)
    lines = planes * per_plane
    place = lax.broadcasted_iota(jnp.int32, (1, lines), 1)
    named = place // per_plane * 4 + place // (per_plane // 2) % 2 * 2 + place % 2
    wanted = (named + place // 2 % members * (4 * planes)).astype(jnp.float32)
    device = lax.broadcasted_iota(jnp.int32, (length, 1), 0) // tok_rows * (4 * planes)
    device = device.astype(jnp.float32)
    taken = (slots[:, 0:1] + device == wanted) | (slots[:, 1:2] + device == wanted)
    placing = jnp.where(taken, 1.0, 0.0).astype(jnp.bfloat16)
    rows = lax.dot_general(
        placing, hidden, (((0,), (0,)), ((), ())), preferred_element_type=jnp.float32
    ).astype(jnp.bfloat16)
    for plane in range(planes):
        sending[plane] = rows[plane * per_plane : (plane + 1) * per_plane, :]


def project(arrived, weight, planes, length):
    members = arrived.shape[0]
    width, lanes = weight.shape
    return pl.pallas_call(
        project_kernel,
        out_shape=(
            jax.ShapeDtypeStruct((length, lanes), jnp.bfloat16),
            jax.ShapeDtypeStruct((planes, 4 * members, lanes), jnp.bfloat16),
        ),
        in_specs=[VMEM, VMEM],
        out_specs=(VMEM, VMEM),
        cost_estimate=pl.CostEstimate(
            flops=2 * length * width * lanes,
            bytes_accessed=4 * width * lanes + 2 * members * length * lanes,
            transcendentals=0,
        ),
        compiler_params=pltpu.CompilerParams(vmem_limit_bytes=12 * 2**20),
        name="project",
    )(arrived, weight)


def spread_kernel(dispatched, out, rows, block, sems):
    planes, lines, _ = dispatched.shape
    members = out.shape[0]
    for plane in range(planes):
        rows[plane * lines : (plane + 1) * lines, :] = dispatched[plane].astype(jnp.float32)
    copies = [
        pltpu.make_async_copy(
            block.at[served_side(t) * 2 + served_rank(t)], out.at[t], sems.at[t]
        )
        for t in range(members)
    ]
    for side in range(2):
        for at in range(lines // 2):
            group = rows[pl.ds(side * (lines // 2) + at, planes, stride=lines), :]
            token, rank = at // 2, at % 2
            block[side * 2 + rank, token * planes : (token + 1) * planes, :] = group.astype(
                jnp.bfloat16
            )
        for t in range(members):
            if served_side(t) == side:
                copies[t].start()
    for copy in copies:
        copy.wait()


def spread(dispatched, members):
    planes, lines, lanes = dispatched.shape
    return pl.pallas_call(
        spread_kernel,
        out_shape=pltpu.HBM((members, planes * lines // 4, lanes), jnp.bfloat16),
        in_specs=[VMEM],
        out_specs=ANYWHERE,
        scratch_shapes=[
            pltpu.VMEM((planes * lines, lanes), jnp.float32),
            pltpu.VMEM((4, planes * lines // 4, lanes), jnp.bfloat16),
            pltpu.SemaphoreType.DMA((members,)),
        ],
        cost_estimate=pl.CostEstimate(
            flops=planes * lines * lanes,
            bytes_accessed=members * planes * lines * lanes,
            transcendentals=0,
        ),
        compiler_params=pltpu.CompilerParams(vmem_limit_bytes=8 * 2**20),
        name="spread",
    )(dispatched)


def exchange(value, axis, groups=None):
    return lax.all_to_all(
        value, axis, split_axis=0, concat_axis=0, tiled=True, axis_index_groups=groups
    )


def pack_kernel(gate, up, down, first, second, held, sems):
    half = gate.shape[0]
    part = half // 2
    sources, outs = (gate, up, down), (first, second)
    loads = [
        pltpu.make_async_copy(source, held.at[i], sems.at[i]) for i, source in enumerate(sources)
    ]
    for copy in loads:
        copy.start()
    stores = []
    for i, copy in enumerate(loads):
        copy.wait()
        for k, out in enumerate(outs):
            stores.append(
                pltpu.make_async_copy(
                    held.at[i, pl.ds(k * part, part)],
                    out.at[pl.ds(i * part, part)],
                    sems.at[3 + 2 * i + k],
                )
            )
            stores[-1].start()
    for copy in stores:
        copy.wait()


def pack(owned):
    half, width = owned[0].shape
    return pl.pallas_call(
        pack_kernel,
        out_shape=tuple(pltpu.HBM((3 * half // 2, width), jnp.bfloat16) for _ in range(2)),
        in_specs=[ANYWHERE] * 3,
        out_specs=(ANYWHERE,) * 2,
        scratch_shapes=[
            pltpu.VMEM((3, half, width), jnp.bfloat16), pltpu.SemaphoreType.DMA((9,)),
        ],
        cost_estimate=pl.CostEstimate(
            flops=half * width, bytes_accessed=12 * half * width, transcendentals=0
        ),
        compiler_params=pltpu.CompilerParams(vmem_limit_bytes=8 * 2**20),
        name="pack",
    )(*in_hbm(owned))


def expert_kernel(
    serves, gathered, own, gain, gate_own, up_own, down_own,
    got_0, got_1, got_2, got_3, fwd_0, fwd_1, fwd_2, fwd_3,
    out, gate, up, down, normed, sems,
):
    half, width = gate_own.shape
    part = half // 2
    pairs, rows, piece = gathered.shape
    members = out.shape[0]
    each = rows // members
    tiles = width // 128
    targets = (gate, up, down)

    def placed(packed, start, base):
        return [
            pltpu.make_async_copy(
                packed.at[pl.ds(i * part, part)], target.at[pl.ds(start, part)], sems.at[base + i]
            )
            for i, target in enumerate(targets)
        ]

    received = [
        placed(packed, k * part, 3 * k) for k, packed in enumerate((got_0, got_1, got_2, got_3))
    ]
    received += [placed(fwd_0, 4 * part, 12), placed(fwd_1, 5 * part, 15)]
    forwarded = [placed(fwd_2, 6 * part, 18), placed(fwd_3, 7 * part, 18)]
    held = [
        pltpu.make_async_copy(source, target.at[pl.ds(3 * half, half)], sems.at[18 + i])
        for i, (source, target) in enumerate(zip((gate_own, up_own, down_own), targets))
    ]
    for copies in received:
        for copy in copies[:2]:
            copy.start()

    @pl.when(serves[0] == 1)
    def _():
        for copy in held:
            copy.start()

    @pl.when(serves[0] != 1)
    def _():
        for i in range(3):
            for copies in forwarded:
                copies[i].start()

    for copies in received:
        copies[2].start()

    total = jnp.zeros((rows, 1), jnp.float32)
    for k in range(pairs):
        block = gathered[k].astype(jnp.float32)
        total = total + jnp.sum(block * block, axis=-1, keepdims=True)
    inverse = lax.rsqrt(total * (1.0 / width) + EPS)
    for k in range(pairs):
        block = gathered[k].astype(jnp.float32)
        scaled = block * inverse * gain[:, k * piece : (k + 1) * piece]
        normed[:, k * piece : (k + 1) * piece] = scaled.astype(jnp.bfloat16)
    for t in range(members):
        out[t, each * tiles :, :] = own[t * 16 : (t + 1) * 16, :]
    contract = (((1,), (1,)), ((), ()))
    hidden = []
    arrived = 0
    for start in range(0, 4 * half, 256):
        size = 256
        while arrived < 6 and arrived * part < start + size:
            for copy in received[arrived][:2]:
                copy.wait()
            arrived += 1
        if arrived == 6 and start + size > 6 * part:
            for copy in held[:2]:
                copy.wait()
            arrived += 1
        g = lax.dot_general(
            normed[...], gate[pl.ds(start, size), :], contract, preferred_element_type=jnp.float32
        )
        u = lax.dot_general(
            normed[...], up[pl.ds(start, size), :], contract, preferred_element_type=jnp.float32
        )
        hidden.append((g / (1.0 + jnp.exp(-g)) * u).astype(jnp.bfloat16))
    hidden = jnp.concatenate(hidden, axis=1)
    for copy in (*(copies[2] for copies in received), held[2]):
        copy.wait()
    for chunk in range(width // 256):
        share = jnp.dot(
            hidden, down[:, pl.ds(chunk * 256, 256)], preferred_element_type=jnp.float32
        ).astype(jnp.bfloat16)
        for t in range(members):
            for side in range(2):
                tile = chunk * 2 + side
                out[t, tile * each : (tile + 1) * each, :] = share[
                    t * each : (t + 1) * each, side * 128 : (side + 1) * 128
                ]


def run_expert(serves, gathered, own, norm_gain, owned, moved):
    pairs, rows, _ = gathered.shape
    half, width = owned[0].shape
    members = pairs
    return pl.pallas_call(
        expert_kernel,
        out_shape=jax.ShapeDtypeStruct(
            (members, rows // members * (width // 128) + 16, 128), jnp.bfloat16
        ),
        in_specs=[SMEM, VMEM, VMEM, VMEM] + [ANYWHERE] * 11,
        out_specs=VMEM,
        scratch_shapes=[pltpu.VMEM((4 * half, width), jnp.bfloat16) for _ in range(3)]
        + [pltpu.VMEM((rows, width), jnp.bfloat16), pltpu.SemaphoreType.DMA((21,))],
        cost_estimate=pl.CostEstimate(
            flops=24 * rows * half * width,
            bytes_accessed=24 * half * width + 4 * rows * width,
            transcendentals=2 * rows * half,
        ),
        compiler_params=pltpu.CompilerParams(vmem_limit_bytes=28 * 2**20),
        name="expert",
    )(serves, gathered, own, norm_gain.reshape(1, -1), *in_hbm(owned), *in_hbm(moved))


def sum_kernel(shares, out, acc):
    members, rows, lanes = shares.shape
    planes = out.shape[0]
    tiles = (rows - 16) // planes
    for side in range(2):
        for rank in range(2):
            total = jnp.zeros((rows - 16, lanes), jnp.float32)
            for t in range(members):
                if served_side(t) == side and served_rank(t) == rank:
                    total = total + shares[t, pl.ds(0, rows - 16), :].astype(jnp.float32)
            acc[...] = total
            for plane in range(planes):
                rows_of = acc[pl.ds(plane, tiles, stride=planes), :]
                at = (side * 2 + rank) * tiles
                out[plane, at : at + tiles, :] = rows_of.astype(jnp.bfloat16)


def sum_shares(shares, planes):
    members, rows, lanes = shares.shape
    tiles = (rows - 16) // planes
    return pl.pallas_call(
        sum_kernel,
        out_shape=jax.ShapeDtypeStruct((planes, 4 * tiles, lanes), jnp.bfloat16),
        in_specs=[VMEM],
        out_specs=VMEM,
        scratch_shapes=[pltpu.VMEM((rows - 16, lanes), jnp.float32)],
        cost_estimate=pl.CostEstimate(
            flops=members * rows * lanes, bytes_accessed=2 * members * rows * lanes, transcendentals=0
        ),
        compiler_params=pltpu.CompilerParams(vmem_limit_bytes=8 * 2**20),
        name="shares",
    )(shares)


def local(
    queries,
    keys,
    values,
    sink_logit,
    out_weight,
    residual,
    norm_gain,
    routes,
    route_weights,
    gate_weight,
    up_weight,
    down_weight,
):
    n_sp, n_tp = lax.axis_size("sp"), lax.axis_size("tp")
    planes = n_sp // 2
    tok_rows, width = residual.shape
    length = queries.shape[0]
    same_core = [[plane * 2 + core for plane in range(planes)] for core in range(2)]

    steps = ((0, 1), (0, 3), (1, 0), (3, 0))
    diagonal = ((1, 1), (3, 3))
    moves, passes = [[] for _ in steps], [[] for _ in steps]
    for plane in range(planes):
        for core in range(2):
            for member in range(n_tp):
                base = (plane * 2 + core) * n_tp
                across = (plane * 2 + 1 - core) * n_tp
                y, x = member // 4, member % 4
                right = served_side(member) == core
                for k, (dy, dx) in enumerate(steps):
                    if right and k < 2:
                        dy, dx = diagonal[k]
                        target = across + (y + dy) % 4 * 4 + (x + dx) % 4
                    elif right:
                        target = across + member
                    else:
                        target = base + (y + dy) % 4 * 4 + (x + dx) % 4
                    moves[k].append((base + member, target))
                    if right or k < 2:
                        passes[k].append((base + member, across + member))
    core_index = lax.axis_index("sp") % 2
    serves = (core_index == served_side(lax.axis_index("tp"))).astype(jnp.int32).reshape(1)
    owned = (gate_weight[0].T, up_weight[0].T, down_weight[0])
    received, forwarded = [], []
    packed = pack(owned)
    for k, way in enumerate(moves):
        received.append(lax.ppermute(packed[k % 2], ("sp", "tp"), way))
        forwarded.append(lax.ppermute(received[-1], ("sp", "tp"), passes[k]))

    low, high, joined, asked, base, sinks, slot_rows = prepare(
        keys.T, values.T, queries, residual, sink_logit.reshape(1, -1), routes.T
    )
    forward = [(i, i + 1) for i in range(n_sp - 1)]
    backward = [(i + 1, i) for i in range(n_sp - 1)]
    low = lax.ppermute(low, "sp", forward)
    high = lax.ppermute(high, "sp", backward)
    where = jnp.stack([lax.axis_index("sp"), jnp.int32(n_sp)]).astype(jnp.int32)
    message = run_attention(where, sinks, asked, low, joined, high, base, slot_rows, n_tp)

    arrived = exchange(message, "tp")
    own, sending = project(arrived, out_weight, planes, length)

    dispatched = exchange(sending, "sp", same_core)
    to_servers = spread(dispatched, n_tp)
    gathered = exchange(to_servers, "tp")
    pieces = run_expert(serves, gathered, own, norm_gain, owned, (*received, *forwarded))

    shares = exchange(pieces, "tp")
    own_rows = shares[:, n_tp * planes :].transpose(1, 0, 2).reshape(tok_rows, width)
    returning = sum_shares(shares, planes)

    returned = exchange(returning, "sp", same_core)
    returned = returned.reshape(planes * 4, width)
    slots = slot_rows[:, :2].astype(jnp.int32)
    place = (slots[:, :, None] == jnp.arange(2 * n_sp)[None, None, :]).astype(jnp.bfloat16)
    first = jnp.dot(place[:, 0], returned, preferred_element_type=jnp.float32)
    second = jnp.dot(place[:, 1], returned, preferred_element_type=jnp.float32)
    mixture = route_weights[:, 0:1] * first + route_weights[:, 1:2] * second
    hidden_state = residual.astype(jnp.float32) + own_rows.astype(jnp.float32)
    return (hidden_state + mixture).astype(jnp.bfloat16)


def solution(mesh):
    in_specs = (
        P("sp", "tp"),
        P("sp", "tp"),
        P("sp", "tp"),
        P("tp"),
        P(None, "tp"),
        P(("sp", "tp"), None),
        P(),
        P(("sp", "tp"), None),
        P(("sp", "tp"), None),
        P("sp", None, "tp"),
        P("sp", None, "tp"),
        P("sp", "tp", None),
    )
    out_specs = P(("sp", "tp"), None)

    return jax.shard_map(local, mesh=mesh, in_specs=in_specs, out_specs=out_specs, check_vma=False)
```

```python
import jax
import jax.numpy as jnp
from jax import lax
from jax.experimental import pallas as pl
from jax.experimental.pallas import tpu as pltpu
from jax.sharding import PartitionSpec as P


HEAD = 64
WINDOW = 128

EPS = 1e-06
NEGATIVE = -1e30


VMEM = pl.BlockSpec(memory_space=pltpu.VMEM)
SMEM = pl.BlockSpec(memory_space=pltpu.SMEM)
ANYWHERE = pl.BlockSpec(memory_space=pltpu.HBM)


def in_hbm(values):
    return [pltpu.with_memory_space_constraint(value, pltpu.HBM) for value in values]


def served_side(member):
    return (member + member // 4) % 2


def served_rank(member):
    return member // 4 % 2


def prep_kernel(
    keys, values, queries, residual, sink, routes, low, high, own, asked, base, sinks, slots,
    named, sems,
):
    head, length = keys.shape
    copies = [
        pltpu.make_async_copy(source, target, sems.at[i])
        for i, (source, target) in enumerate(
            (
                (keys, own.at[pl.ds(0, head)]),
                (values, own.at[pl.ds(head, head)]),
                (queries, asked),
                (residual, base),
                (sink, sinks),
                (routes, named),
            )
        )
    ]
    for copy in copies:
        copy.start()
    for copy in copies:
        copy.wait()
    low[...] = own[:, length - WINDOW :]
    high[...] = own[:, :WINDOW]
    ways, count = named.shape
    flat = named[...].astype(jnp.float32)
    row = lax.broadcasted_iota(jnp.int32, (count, count), 0)
    col = lax.broadcasted_iota(jnp.int32, (count, count), 1)
    eye = jnp.where(row == col, 1.0, 0.0)
    upright = lax.dot_general(
        eye, flat, (((1,), (1,)), ((), ())), preferred_element_type=jnp.float32
    )
    lane = lax.broadcasted_iota(jnp.int32, slots.shape, 1)
    result = jnp.zeros(slots.shape, jnp.float32)
    for way in range(ways):
        mine = upright[:, way : way + 1]
        rank = jnp.zeros((count, 1), jnp.float32)
        for other in range(ways):
            same = (flat[other : other + 1, :] == mine) & (col < row)
            rank = rank + jnp.sum(jnp.where(same, 1.0, 0.0), axis=1, keepdims=True)
        result = jnp.where(lane == way, mine * 2.0 + rank, result)
    slots[...] = result.astype(jnp.bfloat16)


def prepare(keys, values, queries, residual, sink, routes):
    head, length = keys.shape
    tok_rows = residual.shape[0]
    bf16 = jnp.bfloat16
    return pl.pallas_call(
        prep_kernel,
        out_shape=(
            jax.ShapeDtypeStruct((2 * head, WINDOW), bf16),
            jax.ShapeDtypeStruct((2 * head, WINDOW), bf16),
            jax.ShapeDtypeStruct((2 * head, length), bf16),
            jax.ShapeDtypeStruct(queries.shape, bf16),
            jax.ShapeDtypeStruct(residual.shape, bf16),
            jax.ShapeDtypeStruct(sink.shape, jnp.float32),
            jax.ShapeDtypeStruct((tok_rows, 128), bf16),
        ),
        in_specs=[ANYWHERE] * 6,
        out_specs=(VMEM,) * 7,
        scratch_shapes=[pltpu.VMEM(routes.shape, jnp.int32), pltpu.SemaphoreType.DMA((6,))],
        compiler_params=pltpu.CompilerParams(vmem_limit_bytes=4 * 2**20),
        name="prepare",
    )(*in_hbm((keys, values, queries, residual, sink, routes)))


def attend_kernel(place, sink, queries, low, own, high, residual, slots, out):
    members = out.shape[0]
    length, both = queries.shape
    tok_rows = residual.shape[0]
    total = place[1] * length
    band = jnp.concatenate([low[...], own[...], high[...]], axis=1)
    row = lax.broadcasted_iota(jnp.int32, (WINDOW, 3 * WINDOW), 0)
    col = lax.broadcasted_iota(jnp.int32, (WINDOW, 3 * WINDOW), 1)
    near = jnp.abs(row + WINDOW - col) <= WINDOW
    for block in range(length // WINDOW):
        position = place[0] * length + (block - 1) * WINDOW + col
        valid = near & (position >= 0) & (position < total)
        keys = band[:HEAD, block * WINDOW : (block + 3) * WINDOW]
        values = band[HEAD:, block * WINDOW : (block + 3) * WINDOW]
        heads = []
        for head in range(both // HEAD):
            asked = queries[block * WINDOW : (block + 1) * WINDOW, head * HEAD : (head + 1) * HEAD]
            scores = jnp.dot(asked, keys, preferred_element_type=jnp.float32) * HEAD ** (-0.5)
            masked = jnp.where(valid, scores, NEGATIVE)
            bound = sink[:, head : head + 1]
            top = jnp.maximum(jnp.max(masked, axis=-1, keepdims=True), bound)
            probs = jnp.exp(masked - top)
            denom = jnp.sum(probs, axis=-1, keepdims=True) + jnp.exp(bound - top)
            weights = (probs / denom).astype(jnp.bfloat16)
            heads.append(
                lax.dot_general(
                    weights, values, (((1,), (1,)), ((), ())), preferred_element_type=jnp.float32
                )
            )
        attended = jnp.concatenate(heads, axis=1).astype(jnp.bfloat16)
        for t in range(members):
            out[t, block * WINDOW : (block + 1) * WINDOW, :] = attended
    for t in range(members):
        out[t, length : length + tok_rows, :] = residual[:, t * 128 : (t + 1) * 128]
        out[t, length + tok_rows :, :] = slots[...]


def run_attention(place, sink, queries, low, own, high, residual, slots, members):
    length, both = queries.shape
    tok_rows = residual.shape[0]
    return pl.pallas_call(
        attend_kernel,
        out_shape=jax.ShapeDtypeStruct((members, length + 2 * tok_rows, 128), jnp.bfloat16),
        in_specs=[SMEM] + [VMEM] * 7,
        out_specs=VMEM,
        cost_estimate=pl.CostEstimate(
            flops=4 * length * both * 3 * WINDOW,
            bytes_accessed=4 * members * length * 128,
            transcendentals=6 * length * WINDOW,
        ),
        compiler_params=pltpu.CompilerParams(vmem_limit_bytes=10 * 2**20),
        name="attend",
    )(place, sink, queries, low, own, high, residual, slots)


def project_kernel(arrived, weight, projected, sending):
    members = arrived.shape[0]
    length = projected.shape[0]
    tok_rows = length // members
    planes, per_plane, lanes = sending.shape
    total = jnp.zeros((length, lanes), jnp.float32)
    for k in range(members // 2):
        part = jnp.concatenate(
            [arrived[2 * k, :length, :], arrived[2 * k + 1, :length, :]], axis=1
        )
        total = total + jnp.dot(
            part, weight[k * 256 : (k + 1) * 256, :], preferred_element_type=jnp.float32
        )
    rounded = total.astype(jnp.bfloat16)
    projected[...] = rounded
    base = jnp.concatenate(
        [arrived[t, length : length + tok_rows, :] for t in range(members)], axis=0
    )
    hidden = (base.astype(jnp.float32) + rounded.astype(jnp.float32)).astype(jnp.bfloat16)
    slots = jnp.concatenate([arrived[t, length + tok_rows :, :] for t in range(members)], axis=0)
    slots = slots.astype(jnp.float32)
    lines = planes * per_plane
    place = lax.broadcasted_iota(jnp.int32, (1, lines), 1)
    named = place // per_plane * 4 + place // (per_plane // 2) % 2 * 2 + place % 2
    wanted = (named + place // 2 % members * (4 * planes)).astype(jnp.float32)
    device = lax.broadcasted_iota(jnp.int32, (length, 1), 0) // tok_rows * (4 * planes)
    device = device.astype(jnp.float32)
    taken = (slots[:, 0:1] + device == wanted) | (slots[:, 1:2] + device == wanted)
    placing = jnp.where(taken, 1.0, 0.0).astype(jnp.bfloat16)
    rows = lax.dot_general(
        placing, hidden, (((0,), (0,)), ((), ())), preferred_element_type=jnp.float32
    ).astype(jnp.bfloat16)
    for plane in range(planes):
        sending[plane] = rows[plane * per_plane : (plane + 1) * per_plane, :]


def project(arrived, weight, planes, length):
    members = arrived.shape[0]
    width, lanes = weight.shape
    return pl.pallas_call(
        project_kernel,
        out_shape=(
            jax.ShapeDtypeStruct((length, lanes), jnp.bfloat16),
            jax.ShapeDtypeStruct((planes, 4 * members, lanes), jnp.bfloat16),
        ),
        in_specs=[VMEM, VMEM],
        out_specs=(VMEM, VMEM),
        cost_estimate=pl.CostEstimate(
            flops=2 * length * width * lanes,
            bytes_accessed=4 * width * lanes + 2 * members * length * lanes,
            transcendentals=0,
        ),
        compiler_params=pltpu.CompilerParams(vmem_limit_bytes=12 * 2**20),
        name="project",
    )(arrived, weight)


def spread_kernel(dispatched, out, rows, block, sems):
    planes, lines, _ = dispatched.shape
    members = out.shape[0]
    for plane in range(planes):
        rows[plane * lines : (plane + 1) * lines, :] = dispatched[plane].astype(jnp.float32)
    copies = [
        pltpu.make_async_copy(
            block.at[served_side(t) * 2 + served_rank(t)], out.at[t], sems.at[t]
        )
        for t in range(members)
    ]
    for side in range(2):
        for at in range(lines // 2):
            group = rows[pl.ds(side * (lines // 2) + at, planes, stride=lines), :]
            token, rank = at // 2, at % 2
            block[side * 2 + rank, token * planes : (token + 1) * planes, :] = group.astype(
                jnp.bfloat16
            )
        for t in range(members):
            if served_side(t) == side:
                copies[t].start()
    for copy in copies:
        copy.wait()


def spread(dispatched, members):
    planes, lines, lanes = dispatched.shape
    return pl.pallas_call(
        spread_kernel,
        out_shape=pltpu.HBM((members, planes * lines // 4, lanes), jnp.bfloat16),
        in_specs=[VMEM],
        out_specs=ANYWHERE,
        scratch_shapes=[
            pltpu.VMEM((planes * lines, lanes), jnp.float32),
            pltpu.VMEM((4, planes * lines // 4, lanes), jnp.bfloat16),
            pltpu.SemaphoreType.DMA((members,)),
        ],
        cost_estimate=pl.CostEstimate(
            flops=planes * lines * lanes,
            bytes_accessed=members * planes * lines * lanes,
            transcendentals=0,
        ),
        compiler_params=pltpu.CompilerParams(vmem_limit_bytes=8 * 2**20),
        name="spread",
    )(dispatched)


def exchange(value, axis, groups=None):
    return lax.all_to_all(
        value, axis, split_axis=0, concat_axis=0, tiled=True, axis_index_groups=groups
    )


def pack_kernel(gate, up, down, first, second, held, sems):
    half = gate.shape[0]
    part = half // 2
    sources, outs = (gate, up, down), (first, second)
    loads = [
        pltpu.make_async_copy(source, held.at[i], sems.at[i]) for i, source in enumerate(sources)
    ]
    for copy in loads:
        copy.start()
    stores = []
    for i, copy in enumerate(loads):
        copy.wait()
        for k, out in enumerate(outs):
            stores.append(
                pltpu.make_async_copy(
                    held.at[i, pl.ds(k * part, part)],
                    out.at[pl.ds(i * part, part)],
                    sems.at[3 + 2 * i + k],
                )
            )
            stores[-1].start()
    for copy in stores:
        copy.wait()


def pack(owned):
    half, width = owned[0].shape
    return pl.pallas_call(
        pack_kernel,
        out_shape=tuple(pltpu.HBM((3 * half // 2, width), jnp.bfloat16) for _ in range(2)),
        in_specs=[ANYWHERE] * 3,
        out_specs=(ANYWHERE,) * 2,
        scratch_shapes=[
            pltpu.VMEM((3, half, width), jnp.bfloat16), pltpu.SemaphoreType.DMA((9,)),
        ],
        cost_estimate=pl.CostEstimate(
            flops=half * width, bytes_accessed=12 * half * width, transcendentals=0
        ),
        compiler_params=pltpu.CompilerParams(vmem_limit_bytes=8 * 2**20),
        name="pack",
    )(*in_hbm(owned))


def expert_kernel(
    serves, gathered, own, gain, gate_own, up_own, down_own,
    got_0, got_1, got_2, got_3, fwd_0, fwd_1, fwd_2, fwd_3,
    out, gate, up, down, normed, sems,
):
    half, width = gate_own.shape
    part = half // 2
    pairs, rows, piece = gathered.shape
    members = out.shape[0]
    each = rows // members
    tiles = width // 128
    targets = (gate, up, down)

    def placed(packed, start, base):
        return [
            pltpu.make_async_copy(
                packed.at[pl.ds(i * part, part)], target.at[pl.ds(start, part)], sems.at[base + i]
            )
            for i, target in enumerate(targets)
        ]

    received = [
        placed(packed, k * part, 3 * k) for k, packed in enumerate((got_0, got_1, got_2, got_3))
    ]
    received += [placed(fwd_0, 4 * part, 12), placed(fwd_1, 5 * part, 15)]
    forwarded = [placed(fwd_2, 6 * part, 18), placed(fwd_3, 7 * part, 18)]
    held = [
        pltpu.make_async_copy(source, target.at[pl.ds(3 * half, half)], sems.at[18 + i])
        for i, (source, target) in enumerate(zip((gate_own, up_own, down_own), targets))
    ]
    for copies in received:
        for copy in copies[:2]:
            copy.start()

    @pl.when(serves[0] == 1)
    def _():
        for copy in held:
            copy.start()

    @pl.when(serves[0] != 1)
    def _():
        for i in range(3):
            for copies in forwarded:
                copies[i].start()

    for copies in received:
        copies[2].start()

    total = jnp.zeros((rows, 1), jnp.float32)
    for k in range(pairs):
        block = gathered[k].astype(jnp.float32)
        total = total + jnp.sum(block * block, axis=-1, keepdims=True)
    inverse = lax.rsqrt(total * (1.0 / width) + EPS)
    for k in range(pairs):
        block = gathered[k].astype(jnp.float32)
        scaled = block * inverse * gain[:, k * piece : (k + 1) * piece]
        normed[:, k * piece : (k + 1) * piece] = scaled.astype(jnp.bfloat16)
    for t in range(members):
        out[t, each * tiles :, :] = own[t * 16 : (t + 1) * 16, :]
    contract = (((1,), (1,)), ((), ()))
    hidden = []
    arrived = 0
    for start in range(0, 4 * half, 256):
        size = 256
        while arrived < 6 and arrived * part < start + size:
            for copy in received[arrived][:2]:
                copy.wait()
            arrived += 1
        if arrived == 6 and start + size > 6 * part:
            for copy in held[:2]:
                copy.wait()
            arrived += 1
        g = lax.dot_general(
            normed[...], gate[pl.ds(start, size), :], contract, preferred_element_type=jnp.float32
        )
        u = lax.dot_general(
            normed[...], up[pl.ds(start, size), :], contract, preferred_element_type=jnp.float32
        )
        hidden.append((g / (1.0 + jnp.exp(-g)) * u).astype(jnp.bfloat16))
    hidden = jnp.concatenate(hidden, axis=1)
    for copy in (*(copies[2] for copies in received), held[2]):
        copy.wait()
    for chunk in range(width // 256):
        share = jnp.dot(
            hidden, down[:, pl.ds(chunk * 256, 256)], preferred_element_type=jnp.float32
        ).astype(jnp.bfloat16)
        for t in range(members):
            for side in range(2):
                tile = chunk * 2 + side
                out[t, tile * each : (tile + 1) * each, :] = share[
                    t * each : (t + 1) * each, side * 128 : (side + 1) * 128
                ]


def run_expert(serves, gathered, own, norm_gain, owned, moved):
    pairs, rows, _ = gathered.shape
    half, width = owned[0].shape
    members = pairs
    return pl.pallas_call(
        expert_kernel,
        out_shape=jax.ShapeDtypeStruct(
            (members, rows // members * (width // 128) + 16, 128), jnp.bfloat16
        ),
        in_specs=[SMEM, VMEM, VMEM, VMEM] + [ANYWHERE] * 11,
        out_specs=VMEM,
        scratch_shapes=[pltpu.VMEM((4 * half, width), jnp.bfloat16) for _ in range(3)]
        + [pltpu.VMEM((rows, width), jnp.bfloat16), pltpu.SemaphoreType.DMA((21,))],
        cost_estimate=pl.CostEstimate(
            flops=24 * rows * half * width,
            bytes_accessed=24 * half * width + 4 * rows * width,
            transcendentals=2 * rows * half,
        ),
        compiler_params=pltpu.CompilerParams(vmem_limit_bytes=28 * 2**20),
        name="expert",
    )(serves, gathered, own, norm_gain.reshape(1, -1), *in_hbm(owned), *in_hbm(moved))


def sum_kernel(shares, out, acc):
    members, rows, lanes = shares.shape
    planes = out.shape[0]
    tiles = (rows - 16) // planes
    for side in range(2):
        for rank in range(2):
            total = jnp.zeros((rows - 16, lanes), jnp.float32)
            for t in range(members):
                if served_side(t) == side and served_rank(t) == rank:
                    total = total + shares[t, pl.ds(0, rows - 16), :].astype(jnp.float32)
            acc[...] = total
            for plane in range(planes):
                rows_of = acc[pl.ds(plane, tiles, stride=planes), :]
                at = (side * 2 + rank) * tiles
                out[plane, at : at + tiles, :] = rows_of.astype(jnp.bfloat16)


def sum_shares(shares, planes):
    members, rows, lanes = shares.shape
    tiles = (rows - 16) // planes
    return pl.pallas_call(
        sum_kernel,
        out_shape=jax.ShapeDtypeStruct((planes, 4 * tiles, lanes), jnp.bfloat16),
        in_specs=[VMEM],
        out_specs=VMEM,
        scratch_shapes=[pltpu.VMEM((rows - 16, lanes), jnp.float32)],
        cost_estimate=pl.CostEstimate(
            flops=members * rows * lanes, bytes_accessed=2 * members * rows * lanes, transcendentals=0
        ),
        compiler_params=pltpu.CompilerParams(vmem_limit_bytes=8 * 2**20),
        name="shares",
    )(shares)


def local(
    queries,
    keys,
    values,
    sink_logit,
    out_weight,
    residual,
    norm_gain,
    routes,
    route_weights,
    gate_weight,
    up_weight,
    down_weight,
):
    n_sp, n_tp = lax.axis_size("sp"), lax.axis_size("tp")
    planes = n_sp // 2
    tok_rows, width = residual.shape
    length = queries.shape[0]
    same_core = [[plane * 2 + core for plane in range(planes)] for core in range(2)]

    steps = ((0, 1), (0, 3), (1, 0), (3, 0))
    diagonal = ((1, 1), (3, 3))
    moves, passes = [[] for _ in steps], [[] for _ in steps]
    for plane in range(planes):
        for core in range(2):
            for member in range(n_tp):
                base = (plane * 2 + core) * n_tp
                across = (plane * 2 + 1 - core) * n_tp
                y, x = member // 4, member % 4
                right = served_side(member) == core
                for k, (dy, dx) in enumerate(steps):
                    if right and k >= 2:
                        dy, dx = diagonal[k - 2]
                        target = across + (y + dy) % 4 * 4 + (x + dx) % 4
                    elif right:
                        target = across + member
                    else:
                        target = base + (y + dy) % 4 * 4 + (x + dx) % 4
                    moves[k].append((base + member, target))
                    if right or k >= 2:
                        passes[k].append((base + member, across + member))
    core_index = lax.axis_index("sp") % 2
    serves = (core_index == served_side(lax.axis_index("tp"))).astype(jnp.int32).reshape(1)
    owned = (gate_weight[0].T, up_weight[0].T, down_weight[0])
    received, forwarded = [], []
    packed = pack(owned)
    for k, way in enumerate(moves):
        received.append(lax.ppermute(packed[k % 2], ("sp", "tp"), way))
        forwarded.append(lax.ppermute(received[-1], ("sp", "tp"), passes[k]))

    low, high, joined, asked, base, sinks, slot_rows = prepare(
        keys.T, values.T, queries, residual, sink_logit.reshape(1, -1), routes.T
    )
    forward = [(i, i + 1) for i in range(n_sp - 1)]
    backward = [(i + 1, i) for i in range(n_sp - 1)]
    low = lax.ppermute(low, "sp", forward)
    high = lax.ppermute(high, "sp", backward)
    where = jnp.stack([lax.axis_index("sp"), jnp.int32(n_sp)]).astype(jnp.int32)
    message = run_attention(where, sinks, asked, low, joined, high, base, slot_rows, n_tp)

    arrived = exchange(message, "tp")
    own, sending = project(arrived, out_weight, planes, length)

    dispatched = exchange(sending, "sp", same_core)
    to_servers = spread(dispatched, n_tp)
    gathered = exchange(to_servers, "tp")
    pieces = run_expert(serves, gathered, own, norm_gain, owned, (*received, *forwarded[2:], *forwarded[:2]))

    shares = exchange(pieces, "tp")
    own_rows = shares[:, n_tp * planes :].transpose(1, 0, 2).reshape(tok_rows, width)
    returning = sum_shares(shares, planes)

    returned = exchange(returning, "sp", same_core)
    returned = returned.reshape(planes * 4, width)
    slots = slot_rows[:, :2].astype(jnp.int32)
    place = (slots[:, :, None] == jnp.arange(2 * n_sp)[None, None, :]).astype(jnp.bfloat16)
    first = jnp.dot(place[:, 0], returned, preferred_element_type=jnp.float32)
    second = jnp.dot(place[:, 1], returned, preferred_element_type=jnp.float32)
    mixture = route_weights[:, 0:1] * first + route_weights[:, 1:2] * second
    hidden_state = residual.astype(jnp.float32) + own_rows.astype(jnp.float32)
    return (hidden_state + mixture).astype(jnp.bfloat16)


def solution(mesh):
    in_specs = (
        P("sp", "tp"),
        P("sp", "tp"),
        P("sp", "tp"),
        P("tp"),
        P(None, "tp"),
        P(("sp", "tp"), None),
        P(),
        P(("sp", "tp"), None),
        P(("sp", "tp"), None),
        P("sp", None, "tp"),
        P("sp", None, "tp"),
        P("sp", "tp", None),
    )
    out_specs = P(("sp", "tp"), None)

    return jax.shard_map(local, mesh=mesh, in_specs=in_specs, out_specs=out_specs, check_vma=False)
```
